32 devices in a mesh: fs: 4 (over z), rep: 4 (over y, x), tp: 2 (over core).
Axes of the slice: x: 2, y: 2, z: 4, core: 2. Of those that a mesh axis runs over, the one named last changes fastest.
Arguments:
- mixer_out: bfloat16 [16384, 1536], P(('fs', 'rep')), may hold values from -6 to 6
- out_grad: bfloat16 [16384, 4096], P(('fs', 'rep'), 'tp'), may hold values from -0.046875 to 0.046875
- factors: bfloat16 [1536, 256], P(('fs', 'rep')), may hold values from -0.15625 to 0.15625
- weight: float32 [1536, 4096], P(('fs', 'rep'), 'tp'), may hold values from -0.15625 to 0.15625
- first_moment: float32 [256, 4096], P(('fs', 'rep'), 'tp'), may hold values from -6 to 6
- second_moment: float32 [256, 4096], P(('fs', 'rep'), 'tp'), may hold values from 0.05 to 2
Outputs:
- new_weight: float32 [1536, 4096], P(('fs', 'rep'), 'tp')
- update: float32 [1536, 4096], P(('fs', 'rep'), 'tp')
- new_first: float32 [256, 4096], P(('fs', 'rep'), 'tp')
- new_second: float32 [256, 4096], P(('fs', 'rep'), 'tp')
- weight_copy: bfloat16 [1536, 4096], P(None, 'tp')
The draws below stay inside these ranges and needn't reach their ends.
All inputs are finite; a program needn't handle non-finite values.
Results may differ from the reference program's by a relative error of at most 0.0034.
Values may be sent and summed in bfloat16 or wider, within the bound.
A program may use at most 64 MiB of HBM per device.

```python
import math
import jax
import jax.numpy as jnp

D = 4096
DH = 1536
RANK = 256
TOK_DEV = 1024
TOKENS = 16384
N_FS = 4
N_REP = 4


def raised(result, rng, source, target, shards_of, factor):
    owner, partner = [(jnp.arange(result.shape[dim]) // (result.shape[dim] // shards_of)).reshape([-1 if axis == dim else 1 for axis in range(result.ndim)]) for dim in (source, target)]
    chosen = jax.random.permutation(rng, shards_of)[partner]
    strong = (owner == chosen) | (owner == (partner + shards_of // 2) % shards_of)
    return jnp.where(strong, factor * result, result)


def block_levels(own_key, dims, cuts, smallest, high):
    def one(axis_at, blocks):
        draws = jax.random.uniform(jax.random.fold_in(jax.random.fold_in(own_key, 6), axis_at), (blocks,), jnp.float32, smallest / len(cuts), high / len(cuts))
        return jnp.repeat(jnp.exp(draws), dims[axis_at] // blocks).reshape((-1,) + (1,) * (len(dims) - axis_at - 1))

    level = one(*cuts[0])
    for cut in cuts[1:]:
        level = level * one(*cut)
    return level


def noise(own_key, dims, scale, limit, pieces=(), dtype=jnp.bfloat16):
    drawn = jax.random.normal(own_key, dims, jnp.float32) * scale
    if len(pieces) > 0:
        drawn = block_levels(own_key, dims, pieces, -0.22, 0.18) * drawn
    return jnp.clip(drawn, min=-limit, max=limit).astype(dtype)


def bell_draw_with(stream_key, dims, spread, most, pieces, heavy, kind=jnp.bfloat16):
    entries = spread * jax.random.normal(stream_key, dims, jnp.float32)
    if pieces:
        entries = entries * block_levels(stream_key, dims, pieces, -0.22, 0.18)
    return jnp.clip(raised(entries, jax.random.fold_in(stream_key, 3), *heavy), -most, most).astype(kind)


def setup_inputs(seed: int = 0) -> dict:
    arg_keys = jax.random.split(jax.random.key(seed), 7)
    return {
        "mixer_out": bell_draw_with(arg_keys[0], (TOKENS, DH), 1.0, 6.0, ((0, 16),), (0, 1, 16, 2.0)),
        "out_grad": noise(arg_keys[1], (TOKENS, D), ((TOK_DEV * N_FS * N_REP) ** -0.5), 0.046875, ((0, 16), (1, 2))),
        "factors": noise(arg_keys[2], (DH, RANK), DH ** -0.5, 0.15625, ((0, 16),)),
        "weight": noise(arg_keys[3], (DH, D), DH ** -0.5, 0.15625, ((0, 16), (1, 2)), jnp.float32),
        "first_moment": noise(arg_keys[4], (RANK, D), 1.0, 6.0, ((0, 16), (1, 2)), jnp.float32),
        "second_moment": jnp.clip(jnp.exp(math.log(2.0) - 3.6888794 * jax.random.uniform(arg_keys[5], (RANK, D), jnp.float32) ** block_levels(arg_keys[5], (RANK, D), ((0, 16), (1, 2)), -0.2, 0.2)), 0.05, 2.0),
    }


def reference(mixer_out, out_grad, factors, weight, first_moment, second_moment):
    gradient = jnp.dot(mixer_out.T, out_grad, preferred_element_type=jnp.float32)
    grad_low = gradient.astype(jnp.bfloat16)
    projected = jnp.dot(factors.T, grad_low, preferred_element_type=jnp.float32)
    new_first = 0.8 * first_moment + 0.2 * projected
    new_second = 0.9 * second_moment + 0.1 * projected * projected
    direction = new_first / (jnp.sqrt(new_second) + 1e-08)
    dir_low = direction.astype(jnp.bfloat16)
    proj_low = projected.astype(jnp.bfloat16)
    dir_wide = dir_low.astype(jnp.float32)
    proj_wide = proj_low.astype(jnp.float32)
    scale_ratio = jnp.sqrt(jnp.sum(dir_wide * dir_wide)) / jnp.sqrt(jnp.sum(proj_wide * proj_wide) + 1e-06)
    back_dir = jnp.dot(factors, dir_low, preferred_element_type=jnp.float32)
    back_proj = jnp.dot(factors, proj_low, preferred_element_type=jnp.float32)
    update = back_dir + scale_ratio * (gradient - back_proj)
    new_weight = weight - 0.01 * update
    weight_copy = new_weight.astype(jnp.bfloat16)
    return (new_weight, update, new_first, new_second, weight_copy)
```

```python
import functools

import jax
import jax.numpy as jnp
from jax import lax
from jax.experimental import pallas as pl
from jax.experimental.pallas import tpu as pltpu
from jax.sharding import PartitionSpec as P

MESH = pl.DeviceIdType.MESH
LANES = 128
TILE = 256


def contract_rows(left, right):
    return lax.dot_general(
        left, right, (((0,), (0,)), ((), ())), preferred_element_type=jnp.float32
    )


def fused_kernel(
    Z, R, T,
    m_ref, o_ref, f_ref, w_ref, m1_ref, m2_ref,
    nw_ref, upd_ref, nf_ref, ns_ref, wc_ref,
    mt, send1, recv1, own, send2, recv2, grad, f_all, m1_all, m2_all,
    nf_col, ns_col, upd_col, stat, stat_all,
    s1_send, s1_recv, s2_send, s2_recv,
    fa_send, fa_recv, ma_send, ma_recv, mb_send, mb_recv,
    st_send, st_recv, nf_send, nf_recv, ns_send, ns_recv, up_send, up_recv,
    gz_send, gz_recv, gr_send, gr_recv,
    recvd, d_send, d_recv, gh_send, gh_recv,
):
    N = Z * R
    z, r, t = lax.axis_index("fs"), lax.axis_index("rep"), lax.axis_index("tp")
    me = z * R + r
    every = me * T + t
    DH = m_ref.shape[1]
    FR = f_ref.shape[0]
    MR = m1_ref.shape[0]
    H, TH, FH = DH // 2, DH // TILE // 2, FR // 2
    xn, yn, dn = r + 1 - 2 * lax.rem(r, 2), lax.rem(r + 2, R), R - 1 - r

    def device(zz, rr, tt):
        return {"fs": zz, "rep": rr, "tp": tt}

    def peer(p):
        q = lax.rem(me + p, N)
        return q, q // R, lax.rem(q, R)

    def column(zz, rr):
        return pl.ds(pl.multiple_of((rr * Z + zz) * LANES, LANES), LANES)

    def rows(q, size):
        return pl.ds(pl.multiple_of(q * size, size), size)

    barrier = pltpu.get_barrier_semaphore()

    def greet(p, carry):
        q = lax.rem(every + p, N * T)
        d = q // T
        pl.semaphore_signal(
            barrier, inc=1, device_id=device(d // R, lax.rem(d, R), lax.rem(q, T)), device_id_type=MESH
        )
        return carry

    lax.fori_loop(1, N * T, greet, 0)

    def turn(i, carry):
        part = pl.ds(pl.multiple_of(i * TILE, TILE), TILE)
        mt[part, :] = m_ref[:, part].T
        return carry

    lax.fori_loop(0, DH // TILE, turn, 0)
    pl.semaphore_wait(barrier, N * T - 1)

    def product(zz, rr, store, lo=0, hi=None):
        cols = column(zz, rr)

        def tile(i, carry):
            part = pl.ds(pl.multiple_of(i * TILE, TILE), TILE)
            store(part, jnp.dot(mt[part, :], o_ref[:, cols], preferred_element_type=jnp.float32))
            return carry

        lax.fori_loop(lo, DH // TILE if hi is None else hi, tile, 0)

    def first(rr, zz, src):
        return pltpu.make_async_remote_copy(
            src_ref=send1.at[rr, zz], dst_ref=recv1.at[src, zz],
            send_sem=s1_send.at[rr, zz], recv_sem=s1_recv.at[src, zz],
            device_id=device(z, rr, t), device_id_type=MESH,
        )

    def second(zz, src):
        return pltpu.make_async_remote_copy(
            src_ref=send2.at[zz], dst_ref=recv2.at[src],
            send_sem=s2_send.at[zz], recv_sem=s2_recv.at[src],
            device_id=device(zz, r, t), device_id_type=MESH,
        )

    def via(h, zz):
        return pltpu.make_async_remote_copy(
            src_ref=send1.at[dn, zz, pl.ds(h * H, H), :], dst_ref=recvd.at[h, zz],
            send_sem=d_send.at[h, zz], recv_sem=d_recv.at[h, zz],
            device_id=device(z, yn if h else xn, t), device_id_type=MESH,
        )

    def across(e, carry):
        zz = lax.rem(z + 1 + e, Z)

        def store(part, value):
            send1[dn, zz, part, :] = value.astype(jnp.bfloat16)

        product(zz, dn, store)
        via(0, zz).start()
        via(1, zz).start()
        return carry

    lax.fori_loop(0, Z, across, 0)

    def beside(e, carry):
        zz = lax.rem(z + 1 + e, Z)
        for h, rr in ((1, xn), (0, yn)):

            def store(part, value):
                send1[rr, zz, part, :] = value.astype(jnp.bfloat16)

            def store_sum(part, value):
                inner = pl.ds(pl.multiple_of(part.start - h * H, TILE), TILE)
                total = value + recvd[h, zz, inner, :].astype(jnp.float32)
                send1[rr, zz, part, :] = total.astype(jnp.bfloat16)

            product(zz, rr, store, (1 - h) * TH, (2 - h) * TH)
            via(h, zz).wait_recv()
            product(zz, rr, store_sum, h * TH, (h + 1) * TH)
            first(rr, zz, r).start()
        return carry

    lax.fori_loop(0, Z, beside, 0)

    def f_copy(q, zz, rr, slot):
        return pltpu.make_async_remote_copy(
            src_ref=f_ref, dst_ref=f_all.at[rows(slot, FR), :],
            send_sem=fa_send.at[q], recv_sem=fa_recv.at[slot],
            device_id=device(zz, rr, t), device_id_type=MESH,
        )

    def m_copy(src, dst, ss, rs, q, zz, rr, slot):
        return pltpu.make_async_remote_copy(
            src_ref=src.at[:, column(zz, rr)], dst_ref=dst.at[rows(slot, MR), :],
            send_sem=ss.at[q], recv_sem=rs.at[slot],
            device_id=device(zz, rr, t), device_id_type=MESH,
        )

    def spread(p, carry):
        q, zz, rr = peer(p)
        f_copy(q, zz, rr, me).start()
        m_copy(m1_ref, m1_all, ma_send, ma_recv, q, zz, rr, me).start()
        m_copy(m2_ref, m2_all, mb_send, mb_recv, q, zz, rr, me).start()
        return carry

    lax.fori_loop(1, N, spread, 0)
    f_all[rows(me, FR), :] = f_ref[...]
    m1_all[rows(me, MR), :] = m1_ref[:, column(z, r)]
    m2_all[rows(me, MR), :] = m2_ref[:, column(z, r)]

    def own_block(i, carry):
        def store(part, value):
            own[i, part, :] = value

        product(i, r, store)
        return carry

    lax.fori_loop(0, Z, own_block, 0)

    def join(zz, store):
        for src in (xn, yn):
            first(src, zz, src).wait_recv()

        def tile(i, carry):
            part = pl.ds(pl.multiple_of(i * TILE, TILE), TILE)
            total = own[zz, part, :]
            for src in (xn, yn):
                total = total + recv1[src, zz, part, :].astype(jnp.float32)
            store(part, total)
            return carry

        lax.fori_loop(0, DH // TILE, tile, 0)

    def phase2(e, carry):
        zz = lax.rem(z + e, Z)

        def store(part, value):
            send2[zz, part, :] = value.astype(jnp.bfloat16)

        join(zz, store)
        second(zz, z).start()
        return carry

    lax.fori_loop(1, Z, phase2, 0)

    def store_own(part, value):
        grad[part, :] = value

    join(z, store_own)

    def wait_spread(p, carry):
        q, zz, rr = peer(p)
        f_copy(q, zz, rr, q).wait()
        m_copy(m1_ref, m1_all, ma_send, ma_recv, q, zz, rr, q).wait()
        m_copy(m2_ref, m2_all, mb_send, mb_recv, q, zz, rr, q).wait()
        return carry

    lax.fori_loop(1, N, wait_spread, 0)

    def wait_second(e, carry):
        src = lax.rem(z + e, Z)
        second(src, src).wait_recv()
        return carry

    lax.fori_loop(1, Z, wait_second, 0)

    def add_second(i, carry):
        part = pl.ds(pl.multiple_of(i * TILE, TILE), TILE)
        total = grad[part, :]
        for e in range(1, Z):
            total = total + recv2[lax.rem(z + e, Z), part, :].astype(jnp.float32)
        grad[part, :] = total
        return carry

    lax.fori_loop(0, DH // TILE, add_second, 0)

    projected = contract_rows(f_all[...], grad[...].astype(jnp.bfloat16))
    new_first = 0.8 * m1_all[...] + 0.2 * projected
    new_second = 0.9 * m2_all[...] + 0.1 * projected * projected
    nf_col[...] = new_first
    ns_col[...] = new_second
    dir_low = (new_first / (jnp.sqrt(new_second) + 1e-08)).astype(jnp.bfloat16)
    proj_low = projected.astype(jnp.bfloat16)
    dir_wide = dir_low.astype(jnp.float32)
    proj_wide = proj_low.astype(jnp.float32)
    stat[0] = jnp.broadcast_to(jnp.sum(dir_wide * dir_wide, axis=0, keepdims=True), (8, LANES))
    stat[1] = jnp.broadcast_to(jnp.sum(proj_wide * proj_wide, axis=0, keepdims=True), (8, LANES))
    stat_all[every] = stat[...]

    def s_copy(p, slot_of):
        q = lax.rem(every + p, N * T)
        d = q // T
        slot = slot_of(q)
        return pltpu.make_async_remote_copy(
            src_ref=stat, dst_ref=stat_all.at[slot],
            send_sem=st_send.at[q], recv_sem=st_recv.at[slot],
            device_id=device(d // R, lax.rem(d, R), lax.rem(q, T)), device_id_type=MESH,
        )

    def send_stat(p, carry):
        s_copy(p, lambda q: every).start()
        return carry

    lax.fori_loop(1, N * T, send_stat, 0)

    def back_copy(src, dst, size, ss, rs, q, zz, rr, sz, sr, slot):
        return pltpu.make_async_remote_copy(
            src_ref=src.at[rows(q, size), :], dst_ref=dst.at[:, column(sz, sr)],
            send_sem=ss.at[q], recv_sem=rs.at[slot],
            device_id=device(zz, rr, t), device_id_type=MESH,
        )

    def send_moments(p, carry):
        q, zz, rr = peer(p)
        back_copy(nf_col, nf_ref, MR, nf_send, nf_recv, q, zz, rr, z, r, me).start()
        back_copy(ns_col, ns_ref, MR, ns_send, ns_recv, q, zz, rr, z, r, me).start()
        return carry

    lax.fori_loop(1, N, send_moments, 0)
    nf_ref[:, column(z, r)] = nf_col[rows(me, MR), :]
    ns_ref[:, column(z, r)] = ns_col[rows(me, MR), :]

    upd_col[...] = jnp.dot(f_all[...], dir_low, preferred_element_type=jnp.float32)
    grad[...] = grad[...] - jnp.dot(f_all[...], proj_low, preferred_element_type=jnp.float32)

    def wait_stat(p, carry):
        s_copy(p, lambda q: q).wait()
        return carry

    lax.fori_loop(1, N * T, wait_stat, 0)
    totals = jnp.sum(stat_all[...], axis=0)
    dir_sum = jnp.sum(totals[0, 0:1, :], axis=1, keepdims=True)
    proj_sum = jnp.sum(totals[1, 0:1, :], axis=1, keepdims=True)
    scale_ratio = jnp.sqrt(dir_sum) / jnp.sqrt(proj_sum + 1e-06)
    upd_col[...] = upd_col[...] + scale_ratio * grad[...]

    def send_update(p, carry):
        q, zz, rr = peer(p)
        back_copy(upd_col, upd_ref, FR, up_send, up_recv, q, zz, rr, z, r, me).start()
        return carry

    lax.fori_loop(1, N, send_update, 0)
    upd_ref[:, column(z, r)] = upd_col[rows(me, FR), :]

    def wait_update(p, carry):
        q, zz, rr = peer(p)
        back_copy(upd_col, upd_ref, FR, up_send, up_recv, q, zz, rr, zz, rr, q).wait()
        return carry

    lax.fori_loop(1, N, wait_update, 0)

    new_weight = w_ref[...] - 0.01 * upd_ref[...]
    nw_ref[...] = new_weight
    wc_ref[rows(me, FR), :] = new_weight.astype(jnp.bfloat16)

    def along_z(zz, src):
        block = wc_ref.at[rows(src * R + r, FR), :]
        return pltpu.make_async_remote_copy(
            src_ref=block, dst_ref=block, send_sem=gz_send.at[zz], recv_sem=gz_recv.at[src],
            device_id=device(zz, r, t), device_id_type=MESH,
        )

    def along_r(rr, zz, src):
        block = wc_ref.at[rows(zz * R + src, FR), :]
        return pltpu.make_async_remote_copy(
            src_ref=block, dst_ref=block, send_sem=gr_send.at[rr, zz], recv_sem=gr_recv.at[src, zz],
            device_id=device(z, rr, t), device_id_type=MESH,
        )

    def start_z(e, carry):
        along_z(lax.rem(z + e, Z), z).start()
        return carry

    lax.fori_loop(1, Z, start_z, 0)

    def half(h, zz, src):
        block = wc_ref.at[pl.ds(pl.multiple_of((zz * R + src) * FR + h * FH, FH), FH), :]
        return pltpu.make_async_remote_copy(
            src_ref=block, dst_ref=block, send_sem=gh_send.at[h, zz], recv_sem=gh_recv.at[h, zz],
            device_id=device(z, xn if h else yn, t), device_id_type=MESH,
        )

    def relay(e, carry):
        zz = lax.rem(z + 2 * Z - e, Z)
        last = lax.rem(z + 2 * Z - e + 1, Z)

        @pl.when(e < Z)
        def _():
            @pl.when(e > 0)
            def _():
                along_z(zz, zz).wait_recv()

            along_r(xn, zz, r).start()
            along_r(yn, zz, r).start()

        @pl.when(e > 0)
        def _():
            along_r(xn, last, xn).wait_recv()
            half(0, last, xn).start()
            along_r(yn, last, yn).wait_recv()
            half(1, last, yn).start()

        return carry

    lax.fori_loop(0, Z + 1, relay, 0)

    def drain(zz, carry):
        for h, rr in ((0, xn), (1, yn)):
            along_r(rr, zz, r).wait_send()
            first(rr, zz, r).wait_send()
            via(h, zz).wait_send()
            half(h, zz, rr).wait_send()
            half(h, zz, dn).wait_recv()
        return carry

    lax.fori_loop(0, Z, drain, 0)

    def drain_z(e, carry):
        zz = lax.rem(z + e, Z)
        along_z(zz, z).wait_send()
        second(zz, z).wait_send()
        return carry

    lax.fori_loop(1, Z, drain_z, 0)

    def drain_moments(p, carry):
        q, zz, rr = peer(p)
        back_copy(nf_col, nf_ref, MR, nf_send, nf_recv, q, zz, rr, zz, rr, q).wait()
        back_copy(ns_col, ns_ref, MR, ns_send, ns_recv, q, zz, rr, zz, rr, q).wait()
        return carry

    lax.fori_loop(1, N, drain_moments, 0)


def drain_kernel(*refs):
    n = len(refs) // 2
    ins, outs, sem = refs[:n], refs[n:-1], refs[-1]
    copies = [pltpu.make_async_copy(a, b, sem.at[i]) for i, (a, b) in enumerate(zip(ins, outs))]
    for c in copies:
        c.start()
    for c in copies:
        c.wait()


def drain_out(*arrays):
    return pl.pallas_call(
        drain_kernel,
        out_shape=tuple(jax.ShapeDtypeStruct(a.shape, a.dtype) for a in arrays),
        in_specs=[pl.BlockSpec(memory_space=pltpu.VMEM)] * len(arrays),
        out_specs=(pl.BlockSpec(memory_space=pl.ANY),) * len(arrays),
        scratch_shapes=[pltpu.SemaphoreType.DMA((len(arrays),))],
        compiler_params=pltpu.CompilerParams(vmem_limit_bytes=4 * 1024 * 1024),
    )(*[pltpu.with_memory_space_constraint(a, pltpu.VMEM) for a in arrays])


def fused(Z, R, T, *args):
    mixer_out, out_grad, factors, weight, first_moment, second_moment = args
    N = Z * R
    DH = mixer_out.shape[1]
    rank = factors.shape[1]
    f32, bf16 = jnp.float32, jnp.bfloat16
    vmem = pl.BlockSpec(memory_space=pltpu.VMEM)
    dma = pltpu.SemaphoreType.DMA
    wide = lambda n: [dma((n,)), dma((n,))]
    return drain_out(*pl.pallas_call(
        functools.partial(fused_kernel, Z, R, T),
        out_shape=(
            pltpu.VMEM(weight.shape, f32),
            pltpu.VMEM(weight.shape, f32),
            pltpu.VMEM(first_moment.shape, f32),
            pltpu.VMEM(first_moment.shape, f32),
            pltpu.VMEM((DH, weight.shape[1]), bf16),
        ),
        in_specs=[vmem] * 6,
        out_specs=(vmem,) * 5,
        scratch_shapes=[
            pltpu.VMEM((DH, mixer_out.shape[0]), bf16),
            pltpu.VMEM((R, Z, DH, LANES), bf16),
            pltpu.VMEM((R, Z, DH, LANES), bf16),
            pltpu.VMEM((Z, DH, LANES), f32),
            pltpu.VMEM((Z, DH, LANES), bf16),
            pltpu.VMEM((Z, DH, LANES), bf16),
            pltpu.VMEM((DH, LANES), f32),
            pltpu.VMEM((DH, rank), bf16),
            pltpu.VMEM((rank, LANES), f32),
            pltpu.VMEM((rank, LANES), f32),
            pltpu.VMEM((rank, LANES), f32),
            pltpu.VMEM((rank, LANES), f32),
            pltpu.VMEM((DH, LANES), f32),
            pltpu.VMEM((2, 8, LANES), f32),
            pltpu.VMEM((N * T, 2, 8, LANES), f32),
            dma((R, Z)), dma((R, Z)), *wide(Z),
            *wide(N), *wide(N), *wide(N),
            *wide(N * T), *wide(N), *wide(N), *wide(N),
            *wide(Z), dma((R, Z)), dma((R, Z)),
            pltpu.VMEM((2, Z, DH // 2, LANES), bf16),
            dma((2, Z)), dma((2, Z)), dma((2, Z)), dma((2, Z)),
        ],
        compiler_params=pltpu.CompilerParams(
            collective_id=0, has_side_effects=True, vmem_limit_bytes=48 * 1024 * 1024
        ),
    )(*args))

def plain(mixer_out, out_grad, factors, weight, first_moment, second_moment):
    columns = mixer_out
    gradient = lax.psum_scatter(
        contract_rows(columns, out_grad), ("fs", "rep"), scatter_dimension=0, tiled=True
    )
    grad_low = gradient.astype(jnp.bfloat16)
    columns = factors
    projected = lax.psum_scatter(
        contract_rows(columns, grad_low), ("fs", "rep"), scatter_dimension=0, tiled=True
    )
    new_first = 0.8 * first_moment + 0.2 * projected
    new_second = 0.9 * second_moment + 0.1 * projected * projected
    direction = new_first / (jnp.sqrt(new_second) + 1e-08)
    dir_low = direction.astype(jnp.bfloat16)
    proj_low = projected.astype(jnp.bfloat16)
    dir_whole, proj_whole = (
        lax.all_gather(dir_low, ("fs", "rep"), axis=0, tiled=True),
        lax.all_gather(proj_low, ("fs", "rep"), axis=0, tiled=True),
    )
    dir_wide = dir_low.astype(jnp.float32)
    proj_wide = proj_low.astype(jnp.float32)
    dir_sum, proj_sum = lax.psum(
        (jnp.sum(dir_wide * dir_wide), jnp.sum(proj_wide * proj_wide)), ("fs", "rep", "tp")
    )
    back_dir = jnp.dot(factors, dir_whole, preferred_element_type=jnp.float32)
    back_proj = jnp.dot(factors, proj_whole, preferred_element_type=jnp.float32)
    scale_ratio = jnp.sqrt(dir_sum) / jnp.sqrt(proj_sum + 1e-06)
    update = back_dir + scale_ratio * (gradient - back_proj)
    new_weight = weight - 0.01 * update
    weight_copy = lax.all_gather(new_weight.astype(jnp.bfloat16), ("fs", "rep"), axis=0, tiled=True)
    return (new_weight, update, new_first, new_second, weight_copy)


def solution(mesh):
    Z, R, T = mesh.shape["fs"], mesh.shape["rep"], mesh.shape["tp"]

    def per_device(*args):
        mixer_out, out_grad, factors, weight, first_moment, second_moment = args
        fits = (
            out_grad.shape[1] == Z * R * LANES
            and mixer_out.shape[1] % (2 * TILE) == 0
            and weight.shape[0] % 32 == 0
            and first_moment.shape[0] % 8 == 0
            and R == 4
            and Z > 1
        )
        return fused(Z, R, T, *args) if fits else plain(*args)

    in_specs = (
        P(("fs", "rep"), None),
        P(("fs", "rep"), "tp"),
        P(("fs", "rep"), None),
        P(("fs", "rep"), "tp"),
        P(("fs", "rep"), "tp"),
        P(("fs", "rep"), "tp"),
    )
    out_specs = (
        P(("fs", "rep"), "tp"),
        P(("fs", "rep"), "tp"),
        P(("fs", "rep"), "tp"),
        P(("fs", "rep"), "tp"),
        P(None, "tp"),
    )
    return jax.shard_map(
        per_device, mesh=mesh, in_specs=in_specs, out_specs=out_specs, check_vma=False
    )
```

```python
import functools

import jax
import jax.numpy as jnp
from jax import lax
from jax.experimental import pallas as pl
from jax.experimental.pallas import tpu as pltpu
from jax.sharding import PartitionSpec as P

MESH = pl.DeviceIdType.MESH
LANES = 128
PAIR = 2 * LANES
RING = 4
START_GATHER = 10
VMEM_GRANT = 52 * 1024 * 1024


def contract_rows(left, right):
    return lax.dot_general(
        left, right, (((0,), (0,)), ((), ())), preferred_element_type=jnp.float32
    )


def drain_kernel(*refs):
    n = len(refs) // 2
    ins, outs, sem = refs[:n], refs[n:-1], refs[-1]
    copies = [pltpu.make_async_copy(a, b, sem.at[i]) for i, (a, b) in enumerate(zip(ins, outs))]
    for c in copies:
        c.start()
    for c in copies:
        c.wait()


def drain_out(*arrays):
    return pl.pallas_call(
        drain_kernel,
        out_shape=tuple(jax.ShapeDtypeStruct(a.shape, a.dtype) for a in arrays),
        in_specs=[pl.BlockSpec(memory_space=pltpu.VMEM)] * len(arrays),
        out_specs=(pl.BlockSpec(memory_space=pl.ANY),) * len(arrays),
        scratch_shapes=[pltpu.SemaphoreType.DMA((len(arrays),))],
        compiler_params=pltpu.CompilerParams(vmem_limit_bytes=4 * 1024 * 1024),
    )(*[pltpu.with_memory_space_constraint(a, pltpu.VMEM) for a in arrays])


def fused_kernel(
    Z, R, T,
    m_ref, o_ref, f_ref, w_ref, m1_ref, m2_ref,
    nw_ref, upd_ref, nf_ref, ns_ref, wc_ref,
    mt, own, s1, r1, s2, r2, s3, r3,
    f_all, ft, yt, own_p, s1_p, r1_p, s2_p, r2_p, s3_p, r3_p, proj, q_all, q_own,
    stat, stat_all, ratio,
    t_send, t_recv, u_send, u_recv, v_send, v_recv,
    tp_send, tp_recv, up_send, up_recv, vp_send, vp_recv,
    gz_send, gz_recv, gx_send, gx_recv,
    st_send, st_recv,
):
    N = Z * R
    z, r, t = lax.axis_index("fs"), lax.axis_index("rep"), lax.axis_index("tp")
    every = (z * R + r) * T + t
    TOK, DH = m_ref.shape
    CW = o_ref.shape[1]
    FR, RK = f_ref.shape
    MR = m1_ref.shape[0]
    NP = CW // PAIR
    K = START_GATHER
    HALF = CW // 2
    xn, yn, dn = r + 1 - 2 * lax.rem(r, 2), lax.rem(r + 2, R), R - 1 - r
    near = ((xn, yn), (yn, xn))
    f32, bf16 = jnp.float32, jnp.bfloat16

    def device(zz, rr, tt):
        return {"fs": zz, "rep": rr, "tp": tt}

    def lanes(index, size):
        return pl.ds(pl.multiple_of(index * size, size), size)

    def other(e):
        return lax.rem(z + e, Z)

    def each_z(body):
        def step(e, carry):
            body(other(e))
            return carry

        lax.fori_loop(1, Z, step, 0)

    barrier = pltpu.get_barrier_semaphore()

    def greet(p, carry):
        q = lax.rem(every + p, N * T)
        d = q // T
        pl.semaphore_signal(
            barrier, inc=1, device_id=device(d // R, lax.rem(d, R), lax.rem(q, T)), device_id_type=MESH
        )
        return carry

    lax.fori_loop(1, N * T, greet, 0)

    def turn(i, carry):
        mt[lanes(i, PAIR), :] = m_ref[:, lanes(i, PAIR)].T
        return carry

    lax.fori_loop(0, DH // PAIR, turn, 0)

    def move(src, dst, ss, rs, where):
        return pltpu.make_async_remote_copy(
            src_ref=src, dst_ref=dst, send_sem=ss, recv_sem=rs, device_id=where, device_id_type=MESH
        )

    class Scatter:
        def __init__(self, c, h, slot, refs, sems):
            self.c, self.h, self.slot = c, h, slot
            self.own, self.s1, self.r1, self.s2, self.r2, self.s3, self.r3 = refs
            self.ts, self.tr, self.us, self.ur, self.vs, self.vr = sems
            self.n1, self.n2 = near[h]

        def first(self, k):
            rr = self.n1 if k else dn
            c = self.c
            return move(self.s1.at[c, rr], self.r1.at[c, k], self.ts.at[c, k], self.tr.at[c, k], device(z, self.n1, t))

        def second(self):
            c = self.c
            return move(self.s2.at[c], self.r2.at[c], self.us.at[c], self.ur.at[c], device(z, self.n2, t))

        def third(self, zz, src):
            c = self.c
            return move(
                self.s3.at[c, zz], self.r3.at[c, src], self.vs.at[c, zz], self.vr.at[c, src], device(zz, r, t)
            )

        def mine(self, rr, zz):
            return self.own[self.slot, self.h, rr, zz]

        def stage2(self):
            c = self.c
            self.first(0).wait_recv()

            def add(zz, carry):
                total = self.mine(self.n2, zz) + self.r1[c, 0, zz].astype(f32)
                self.s2[c, zz] = total.astype(bf16)
                return carry

            lax.fori_loop(0, Z, add, 0)
            self.second().start()

        def stage3(self, put):
            c = self.c
            self.first(1).wait_recv()
            self.second().wait_recv()

            def total(zz):
                return self.mine(r, zz) + self.r1[c, 1, zz].astype(f32) + self.r2[c, zz].astype(f32)

            def send(zz):
                self.s3[c, zz] = total(zz).astype(bf16)
                self.third(zz, z).start()

            each_z(send)
            put(total(z))

        def last(self, get, put):
            each_z(lambda zz: self.third(zz, zz).wait_recv())
            value = get()
            for e in range(1, Z):
                value = value + self.r3[self.c, other(e)].astype(f32)
            put(value)

        def sent(self):
            self.first(0).wait_send()
            self.first(1).wait_send()
            self.second().wait_send()
            each_z(lambda zz: self.third(zz, z).wait_send())

    class Gather:
        def __init__(self, g, h, ref, cols):
            self.g, self.ref, self.cols = g, ref, cols
            self.n1, self.n2 = near[h]

        def along(self, zz, src_z, block=None):
            place = self.ref.at[src_z, r, :, self.cols]
            return move(
                place if block is None else block, place,
                gz_send.at[self.g, zz], gz_recv.at[self.g, src_z], device(zz, r, t),
            )

        def beside(self, k, rr):
            place = self.ref.at[:, rr, :, self.cols]
            to = self.n2 if k == 0 else self.n1
            return move(place, place, gx_send.at[self.g, k], gx_recv.at[self.g, k], device(z, to, t))

        def stage1(self, block=None):
            each_z(lambda zz: self.along(zz, z, block).start())

        def stage2(self):
            each_z(lambda zz: self.along(zz, zz).wait_recv())
            self.beside(0, r).start()
            self.beside(1, r).start()

        def stage3(self):
            self.beside(0, self.n2).wait_recv()
            self.beside(2, self.n2).start()

        def done(self):
            self.beside(1, self.n1).wait_recv()
            self.beside(2, dn).wait_recv()
            each_z(lambda zz: self.along(zz, z).wait_send())
            self.beside(0, r).wait_send()
            self.beside(1, r).wait_send()
            self.beside(2, self.n2).wait_send()

    main_refs = (own, s1, r1, s2, r2, s3, r3)
    main_sems = (t_send, t_recv, u_send, u_recv, v_send, v_recv)
    proj_refs = (own_p, s1_p, r1_p, s2_p, r2_p, s3_p, r3_p)
    proj_sems = (tp_send, tp_recv, up_send, up_recv, vp_send, vp_recv)

    def scatter(p, h):
        return Scatter(2 * p + h, h, lax.rem(p, RING), main_refs, main_sems)

    def scatter_p(h):
        return Scatter(h, h, 0, proj_refs, proj_sems)

    def gather_w(p, h):
        return Gather(2 * p + h, h, wc_ref, lanes(2 * p + h, LANES))

    def gather_f(h):
        return Gather(2 * NP + h, h, f_all, pl.ds(h * (RK // 2), RK // 2))

    def gather_q(h):
        return Gather(2 * NP + 2 + h, h, q_all, pl.ds(h * HALF, HALF))

    f_all[z, r] = f_ref[...]
    pl.semaphore_wait(barrier, N * T - 1)
    for h in (0, 1):
        gather_f(h).stage1(f_ref.at[:, pl.ds(h * (RK // 2), RK // 2)])

    def product(p):
        cols = lanes(p, PAIR)
        slot = lax.rem(p, RING)
        G = R * FR

        def tile(zz, carry):
            part = pl.ds(pl.multiple_of(zz * G, G), G)
            value = jnp.dot(mt[part, :], o_ref[:, cols], preferred_element_type=f32)
            for h in (0, 1):
                for rr in range(R):
                    block = value[rr * FR : (rr + 1) * FR, h * LANES : (h + 1) * LANES]
                    own[slot, h, rr, zz] = block
                    s1[2 * p + h, rr, zz] = block.astype(bf16)
            return carry

        lax.fori_loop(0, Z, tile, 0)
        for k in (0, 1):
            for h in (0, 1):
                scatter(p, h).first(k).start()

    def project():
        ft[...] = f_all[...].reshape(DH, RK).T

        def low(i, carry):
            yt[:, lanes(i, PAIR)] = jnp.dot(
                ft[...], mt[:, lanes(i, PAIR)], preferred_element_type=f32
            ).astype(bf16)
            return carry

        lax.fori_loop(0, TOK // PAIR, low, 0)

        def tile(n, carry):
            value = jnp.dot(yt[...], o_ref[:, lanes(n, PAIR)], preferred_element_type=f32)
            h = n // (NP // 2)
            cols = lanes(lax.rem(n, NP // 2), PAIR)
            for zz in range(Z):
                for rr in range(R):
                    low_row = (zz * R + rr) * MR
                    block = value[low_row : low_row + MR, :]
                    own_p[0, h, rr, zz, :, cols] = block
                    s1_p[h, rr, zz, :, cols] = block.astype(bf16)
            return carry

        lax.fori_loop(0, NP, tile, 0)

    def s_copy(p, slot_of):
        q = lax.rem(every + p, N * T)
        d = q // T
        slot = slot_of(q)
        return move(
            stat, stat_all.at[slot], st_send.at[q], st_recv.at[slot],
            device(d // R, lax.rem(d, R), lax.rem(q, T)),
        )

    def fold(value):
        row = jnp.sum(value, axis=0, keepdims=True)
        total = row[:, :LANES]
        for j in range(1, CW // LANES):
            total = total + row[:, j * LANES : (j + 1) * LANES]
        return jnp.broadcast_to(total, (8, LANES))

    def moments():
        projected = proj[...]
        new_first = 0.8 * m1_ref[...] + 0.2 * projected
        new_second = 0.9 * m2_ref[...] + 0.1 * projected * projected
        nf_ref[...] = new_first
        ns_ref[...] = new_second
        dir_wide = (new_first / (jnp.sqrt(new_second) + 1e-08)).astype(bf16).astype(f32)
        proj_wide = projected.astype(bf16).astype(f32)
        stat[0] = fold(dir_wide * dir_wide)
        stat[1] = fold(proj_wide * proj_wide)
        stat_all[every] = stat[...]

        def send(p, carry):
            s_copy(p, lambda q: every).start()
            return carry

        lax.fori_loop(1, N * T, send, 0)

    def combine():
        def wait(p, carry):
            s_copy(p, lambda q: q).wait()
            return carry

        lax.fori_loop(1, N * T, wait, 0)
        totals = jnp.sum(stat_all[...], axis=0)
        dir_sum = jnp.sum(totals[0, 0:1, :], axis=1, keepdims=True)
        proj_sum = jnp.sum(totals[1, 0:1, :], axis=1, keepdims=True)
        scale_ratio = jnp.sqrt(dir_sum) / jnp.sqrt(proj_sum + 1e-06)
        ratio[...] = jnp.broadcast_to(scale_ratio, (8, PAIR))
        projected = proj[...]
        dir_wide = (nf_ref[...] / (jnp.sqrt(ns_ref[...]) + 1e-08)).astype(bf16).astype(f32)
        mixed = (dir_wide - scale_ratio * projected.astype(bf16).astype(f32)).astype(bf16)
        q_own[...] = mixed
        q_all[z, r] = mixed
        for h in (0, 1):
            gather_q(h).stage1(q_own.at[:, pl.ds(h * HALF, HALF)])

    def put_proj(h):
        def put(value):
            proj[:, h * HALF : (h + 1) * HALF] = value

        return put

    def get_proj(h):
        return lambda: proj[:, h * HALF : (h + 1) * HALF]

    def both(action):
        for h in (0, 1):
            action(h)

    def event_project():
        both(lambda h: gather_f(h).done())
        project()
        for k in (0, 1):
            both(lambda h: scatter_p(h).first(k).start())

    def event_moments():
        both(lambda h: scatter_p(h).last(get_proj(h), put_proj(h)))
        moments()

    events = {
        1: lambda: both(lambda h: gather_f(h).stage2()),
        2: lambda: both(lambda h: gather_f(h).stage3()),
        3: event_project,
        4: lambda: both(lambda h: scatter_p(h).stage2()),
        5: lambda: both(lambda h: scatter_p(h).stage3(put_proj(h))),
        6: event_moments,
        7: combine,
        8: lambda: both(lambda h: gather_q(h).stage2()),
        9: lambda: both(lambda h: gather_q(h).stage3()),
        10: lambda: both(lambda h: (gather_q(h).done(), scatter_p(h).sent())),
    }

    def put_grad(p, h):
        def put(value):
            upd_ref[:, lanes(2 * p + h, LANES)] = value

        return put

    def get_grad(p, h):
        return lambda: upd_ref[:, lanes(2 * p + h, LANES)]

    def update(p):
        cols = lanes(p, PAIR)
        mixed = q_all[:, :, :, cols].reshape(RK, PAIR)
        value = jnp.dot(f_ref[...], mixed, preferred_element_type=f32) + ratio[0:1, :] * upd_ref[:, cols]
        upd_ref[:, cols] = value
        new_weight = w_ref[:, cols] - 0.01 * value
        nw_ref[:, cols] = new_weight
        wc_ref[z, r, :, cols] = new_weight.astype(bf16)
        both(lambda h: gather_w(p, h).stage1())

    def tick(i, carry):
        def within(lag, action):
            @pl.when((i >= lag) & (i < lag + NP))
            def _():
                action(i - lag)

        for when, action in events.items():
            pl.when(i == when)(action)
        within(0, product)
        within(1, lambda p: both(lambda h: scatter(p, h).stage2()))
        within(2, lambda p: both(lambda h: scatter(p, h).stage3(put_grad(p, h))))
        within(3, lambda p: both(lambda h: scatter(p, h).last(get_grad(p, h), put_grad(p, h))))
        within(4, lambda p: both(lambda h: scatter(p, h).sent()))
        within(K, update)
        within(K + 1, lambda p: both(lambda h: gather_w(p, h).stage2()))
        within(K + 2, lambda p: both(lambda h: gather_w(p, h).stage3()))
        within(K + 3, lambda p: both(lambda h: gather_w(p, h).done()))
        return carry

    lax.fori_loop(0, NP + K + 3, tick, 0)


def fused(Z, R, T, *args):
    mixer_out, out_grad, factors, weight, first_moment, second_moment = args
    N = Z * R
    TOK, DH = mixer_out.shape
    FR, RK = factors.shape
    MR, CW = first_moment.shape
    NC, HALF = CW // LANES, CW // 2
    f32, bf16 = jnp.float32, jnp.bfloat16
    vmem = pl.BlockSpec(memory_space=pltpu.VMEM)
    dma = pltpu.SemaphoreType.DMA
    pair = lambda *shape: [dma(shape), dma(shape)]
    outs = pl.pallas_call(
        functools.partial(fused_kernel, Z, R, T),
        out_shape=(
            pltpu.VMEM(weight.shape, f32),
            pltpu.VMEM(weight.shape, f32),
            pltpu.VMEM(first_moment.shape, f32),
            pltpu.VMEM(first_moment.shape, f32),
            pltpu.VMEM((Z, R, FR, CW), bf16),
        ),
        in_specs=[vmem] * 6,
        out_specs=(vmem,) * 5,
        scratch_shapes=[
            pltpu.VMEM((DH, TOK), bf16),
            pltpu.VMEM((RING, 2, R, Z, FR, LANES), f32),
            pltpu.VMEM((NC, R, Z, FR, LANES), bf16),
            pltpu.VMEM((NC, 2, Z, FR, LANES), bf16),
            pltpu.VMEM((NC, Z, FR, LANES), bf16),
            pltpu.VMEM((NC, Z, FR, LANES), bf16),
            pltpu.VMEM((NC, Z, FR, LANES), bf16),
            pltpu.VMEM((NC, Z, FR, LANES), bf16),
            pltpu.VMEM((Z, R, FR, RK), bf16),
            pltpu.VMEM((RK, DH), bf16),
            pltpu.VMEM((RK, TOK), bf16),
            pltpu.VMEM((1, 2, R, Z, MR, HALF), f32),
            pltpu.VMEM((2, R, Z, MR, HALF), bf16),
            pltpu.VMEM((2, 2, Z, MR, HALF), bf16),
            pltpu.VMEM((2, Z, MR, HALF), bf16),
            pltpu.VMEM((2, Z, MR, HALF), bf16),
            pltpu.VMEM((2, Z, MR, HALF), bf16),
            pltpu.VMEM((2, Z, MR, HALF), bf16),
            pltpu.VMEM((MR, CW), f32),
            pltpu.VMEM((Z, R, MR, CW), bf16),
            pltpu.VMEM((MR, CW), bf16),
            pltpu.VMEM((2, 8, LANES), f32),
            pltpu.VMEM((N * T, 2, 8, LANES), f32),
            pltpu.VMEM((8, PAIR), f32),
            *pair(NC, 2), *pair(NC), *pair(NC, Z),
            *pair(2, 2), *pair(2), *pair(2, Z),
            *pair(NC + 4, Z), *pair(NC + 4, 3),
            *pair(N * T),
        ],
        compiler_params=pltpu.CompilerParams(
            collective_id=0, has_side_effects=True, vmem_limit_bytes=VMEM_GRANT
        ),
    )(*args)
    new_weight, update, new_first, new_second, copy = drain_out(*outs)
    return new_weight, update, new_first, new_second, copy.reshape(DH, CW)


def plain(mixer_out, out_grad, factors, weight, first_moment, second_moment):
    columns = mixer_out
    gradient = lax.psum_scatter(
        contract_rows(columns, out_grad), ("fs", "rep"), scatter_dimension=0, tiled=True
    )
    grad_low = gradient.astype(jnp.bfloat16)
    columns = factors
    projected = lax.psum_scatter(
        contract_rows(columns, grad_low), ("fs", "rep"), scatter_dimension=0, tiled=True
    )
    new_first = 0.8 * first_moment + 0.2 * projected
    new_second = 0.9 * second_moment + 0.1 * projected * projected
    direction = new_first / (jnp.sqrt(new_second) + 1e-08)
    dir_low = direction.astype(jnp.bfloat16)
    proj_low = projected.astype(jnp.bfloat16)
    dir_whole, proj_whole = (
        lax.all_gather(dir_low, ("fs", "rep"), axis=0, tiled=True),
        lax.all_gather(proj_low, ("fs", "rep"), axis=0, tiled=True),
    )
    dir_wide = dir_low.astype(jnp.float32)
    proj_wide = proj_low.astype(jnp.float32)
    dir_sum, proj_sum = lax.psum(
        (jnp.sum(dir_wide * dir_wide), jnp.sum(proj_wide * proj_wide)), ("fs", "rep", "tp")
    )
    back_dir = jnp.dot(factors, dir_whole, preferred_element_type=jnp.float32)
    back_proj = jnp.dot(factors, proj_whole, preferred_element_type=jnp.float32)
    scale_ratio = jnp.sqrt(dir_sum) / jnp.sqrt(proj_sum + 1e-06)
    update = back_dir + scale_ratio * (gradient - back_proj)
    new_weight = weight - 0.01 * update
    weight_copy = lax.all_gather(new_weight.astype(jnp.bfloat16), ("fs", "rep"), axis=0, tiled=True)
    return (new_weight, update, new_first, new_second, weight_copy)


def solution(mesh):
    Z, R, T = mesh.shape["fs"], mesh.shape["rep"], mesh.shape["tp"]

    def per_device(*args):
        mixer_out, out_grad, factors, weight, first_moment, second_moment = args
        fits = (
            out_grad.shape[1] % (4 * PAIR) == 0
            and mixer_out.shape[0] % PAIR == 0
            and mixer_out.shape[1] % PAIR == 0
            and weight.shape[0] % 16 == 0
            and first_moment.shape[0] % 16 == 0
            and factors.shape[1] == PAIR
            and R == 4
            and Z > 1
        )
        return fused(Z, R, T, *args) if fits else plain(*args)

    in_specs = (
        P(("fs", "rep"), None),
        P(("fs", "rep"), "tp"),
        P(("fs", "rep"), None),
        P(("fs", "rep"), "tp"),
        P(("fs", "rep"), "tp"),
        P(("fs", "rep"), "tp"),
    )
    out_specs = (
        P(("fs", "rep"), "tp"),
        P(("fs", "rep"), "tp"),
        P(("fs", "rep"), "tp"),
        P(("fs", "rep"), "tp"),
        P(None, "tp"),
    )
    return jax.shard_map(
        per_device, mesh=mesh, in_specs=in_specs, out_specs=out_specs, check_vma=False
    )
```

```python
import functools

import jax
import jax.numpy as jnp
from jax import lax
from jax.experimental import pallas as pl
from jax.experimental.pallas import tpu as pltpu
from jax.sharding import PartitionSpec as P

MESH = pl.DeviceIdType.MESH
LANES = 128
PAIR = 2 * LANES
VMEM_GRANT = 52 * 1024 * 1024


ORDER = (
    "F1 f1.6 f1.1 F2",
    "F3 f1.0 F4 PM",
    "P1.1 P1.0 P2.1 P2.0",
    "f1.2 f2.0 P3.1 f2.6",
    "f2.1 P3.0 f1.3 f3.0",
    "P4 f2.3 f3.6 f1.4",
    "f2.2 Q1 f2.4 f3.1",
    "f3.2 Q2 f4.0 f3.4",
    "f3.3 Q3 f4.2 f1.5",
    "Q4 g1.2 f2.5 f4.1",
    "g1.1 f1.7 f3.5 f4.4",
    "g1.4 g2.2 f2.7 g2.1",
    "g1.0 f3.7 f4.6 f4.5",
    "g2.4 g1.5 f4.3 g3.1",
    "g1.3 g1.6 f4.7 g3.4",
    "g2.5 g4.1 g2.0 g1.7",
    "g4.4 g2.3 g3.0 g3.2",
    "g2.6 g4.2 g2.7 g3.5",
    "g3.6 g3.3 g3.7 g4.3",
    "g4.5 g4.6 g4.7 g4.0",
)
Z_SCATTER = (1,)
Z_GATHER = (0,)


def order_for(NP):
    if NP == 8:
        return [(a[:2], int(a[3:])) if "." in a else (a,) for line in ORDER for a in line.split()]
    events = {
        1: "F2", 2: "F3", 3: "F4 PM P1.0 P1.1", 4: "P2.0 P2.1", 5: "P3.0 P3.1",
        6: "P4", 7: "Q1", 8: "Q2", 9: "Q3", 10: "Q4",
    }
    lags = {"f1": 0, "f2": 1, "f3": 2, "f4": 3, "g1": 10, "g2": 11, "g3": 12, "g4": 13}
    order = [("F1",)]
    for i in range(max(NP, 1) + 14):
        for a in events.get(i, "").split():
            order.append((a[:2], int(a[3:])) if "." in a else (a,))
        order += [(name, i - lag) for name, lag in lags.items() if 0 <= i - lag < NP]
    return order


def z_pairs(NP):
    return (Z_SCATTER, Z_GATHER) if NP == 8 else ((), ())


def live_pairs(NP):
    live, most = 0, 0
    z_scatter = z_pairs(NP)[0]
    for name, *p in order_for(NP):
        live += (name == "f1") - (name in ("f3", "f4") and (name == "f4") == (p[0] in z_scatter))
        most = max(most, live)
    return most


def contract_rows(left, right):
    return lax.dot_general(
        left, right, (((0,), (0,)), ((), ())), preferred_element_type=jnp.float32
    )


def drain_kernel(*refs):
    n = len(refs) // 2
    ins, outs, sem = refs[:n], refs[n:-1], refs[-1]
    copies = [pltpu.make_async_copy(a, b, sem.at[i]) for i, (a, b) in enumerate(zip(ins, outs))]
    for c in copies:
        c.start()
    for c in copies:
        c.wait()


def drain_out(*arrays):
    return pl.pallas_call(
        drain_kernel,
        out_shape=tuple(jax.ShapeDtypeStruct(a.shape, a.dtype) for a in arrays),
        in_specs=[pl.BlockSpec(memory_space=pltpu.VMEM)] * len(arrays),
        out_specs=(pl.BlockSpec(memory_space=pl.ANY),) * len(arrays),
        scratch_shapes=[pltpu.SemaphoreType.DMA((len(arrays),))],
        compiler_params=pltpu.CompilerParams(vmem_limit_bytes=4 * 1024 * 1024),
    )(*[pltpu.with_memory_space_constraint(a, pltpu.VMEM) for a in arrays])


def fused_kernel(
    Z, R, T,
    m_hbm, o_hbm, f_hbm, w_hbm, m1_hbm, m2_hbm,
    nw_ref, upd_ref, nf_ref, ns_ref, wc_ref,
    m_ref, o_ref, f_ref, w_ref, m1_ref, m2_ref, load,
    mt, own, s1, r1, s2, r2, s3, r3, rz,
    f_all, ft, yt, own_p, s1_p, r1_p, s2_p, r2_p, s3_p, r3_p, proj, q_all, q_own,
    stat, stat_all, ratio,
    t_send, t_recv, u_send, u_recv, v_send, v_recv,
    tp_send, tp_recv, up_send, up_recv, vp_send, vp_recv,
    gz_send, gz_recv, gx_send, gx_recv,
    st_send, st_recv, cross_send, cross_recv,
):
    N = Z * R
    z, r, t = lax.axis_index("fs"), lax.axis_index("rep"), lax.axis_index("tp")
    every = (z * R + r) * T + t
    TOK, DH = m_ref.shape
    CW = o_ref.shape[1]
    FR, RK = f_ref.shape
    MR = m1_ref.shape[0]
    NP = CW // PAIR
    HALF = CW // 2
    xn, yn, dn = r + 1 - 2 * lax.rem(r, 2), lax.rem(r + 2, R), R - 1 - r
    near = ((xn, yn), (yn, xn))
    f32, bf16 = jnp.float32, jnp.bfloat16

    def device(zz, rr, tt):
        return {"fs": zz, "rep": rr, "tp": tt}

    def lanes(index, size):
        return pl.ds(pl.multiple_of(index * size, size), size)

    def other(e):
        return lax.rem(z + e, Z)

    def each_z(body):
        def step(e, carry):
            body(other(e))
            return carry

        lax.fori_loop(1, Z, step, 0)

    def fetch(src, dst, index):
        return pltpu.make_async_copy(src, dst, load.at[index])

    loads = {"f": fetch(f_hbm, f_ref, 0)}
    for i in range(DH // PAIR):
        part = pl.ds(i * PAIR, PAIR)
        loads["m", i] = fetch(m_hbm.at[:, part], m_ref.at[:, part], len(loads))
    for i in range(NP):
        part = pl.ds(i * PAIR, PAIR)
        loads["o", i] = fetch(o_hbm.at[:, part], o_ref.at[:, part], len(loads))
    for name, src, dst in (("m1", m1_hbm, m1_ref), ("m2", m2_hbm, m2_ref), ("w", w_hbm, w_ref)):
        loads[name] = fetch(src, dst, len(loads))
    for copy in loads.values():
        copy.start()

    def need(*names):
        for name in names:
            if name in loads:
                loads.pop(name).wait()

    barrier = pltpu.get_barrier_semaphore()

    def greet(p, carry):
        q = lax.rem(every + p, N * T)
        d = q // T
        pl.semaphore_signal(
            barrier, inc=1, device_id=device(d // R, lax.rem(d, R), lax.rem(q, T)), device_id_type=MESH
        )
        return carry

    lax.fori_loop(1, N * T, greet, 0)

    for i in range(DH // PAIR):
        need(("m", i))
        mt[i * PAIR : (i + 1) * PAIR, :] = m_ref[:, i * PAIR : (i + 1) * PAIR].T
    need("f")

    def move(src, dst, ss, rs, where):
        return pltpu.make_async_remote_copy(
            src_ref=src, dst_ref=dst, send_sem=ss, recv_sem=rs, device_id=where, device_id_type=MESH
        )

    class Scatter:
        def __init__(self, c, h, slot, refs, sems):
            self.c, self.h, self.slot = c, h, slot
            self.own, self.s1, self.r1, self.s2, self.r2, self.s3, self.r3 = refs
            self.ts, self.tr, self.us, self.ur, self.vs, self.vr = sems
            self.n1, self.n2 = near[h]

        def first(self, k):
            rr = self.n1 if k else dn
            c = self.c
            return move(self.s1.at[c, rr], self.r1.at[c, k], self.ts.at[c, k], self.tr.at[c, k], device(z, self.n1, t))

        def second(self):
            c = self.c
            return move(self.s2.at[c], self.r2.at[c], self.us.at[c], self.ur.at[c], device(z, self.n2, t))

        def third(self, zz, src):
            c = self.c
            return move(
                self.s3.at[c, zz], self.r3.at[c, src], self.vs.at[c, zz], self.vr.at[c, src], device(zz, r, t)
            )

        def mine(self, rr, zz):
            return self.own[self.slot, self.h, rr, zz]

        def stage2(self):
            c = self.c
            self.first(0).wait_recv()

            def add(zz, carry):
                total = self.mine(self.n2, zz) + self.r1[c, 0, zz].astype(f32)
                self.s2[c, zz] = total.astype(bf16)
                return carry

            lax.fori_loop(0, Z, add, 0)
            self.second().start()

        def stage3(self, put):
            c = self.c
            self.first(1).wait_recv()
            self.second().wait_recv()

            def total(zz):
                return self.mine(r, zz) + self.r1[c, 1, zz].astype(f32) + self.r2[c, zz].astype(f32)

            def send(zz):
                self.s3[c, zz] = total(zz).astype(bf16)
                self.third(zz, z).start()

            each_z(send)
            put(total(z))

        def last(self, get, put):
            each_z(lambda zz: self.third(zz, zz).wait_recv())
            value = get()
            for e in range(1, Z):
                value = value + self.r3[self.c, other(e)].astype(f32)
            put(value)

        def sent(self):
            self.first(0).wait_send()
            self.first(1).wait_send()
            self.second().wait_send()
            each_z(lambda zz: self.third(zz, z).wait_send())

    class Gather:
        def __init__(self, g, h, ref, cols, rows=slice(None)):
            self.g, self.ref, self.cols, self.rows = g, ref, cols, rows
            self.n1, self.n2 = near[h]

        def along(self, zz, src_z, block=None):
            place = self.ref.at[src_z, r, self.rows, self.cols]
            return move(
                place if block is None else block, place,
                gz_send.at[self.g, zz], gz_recv.at[self.g, src_z], device(zz, r, t),
            )

        def beside(self, k, rr):
            place = self.ref.at[:, rr, self.rows, self.cols]
            to = self.n2 if k == 0 else self.n1
            return move(place, place, gx_send.at[self.g, k], gx_recv.at[self.g, k], device(z, to, t))

        def stage1(self, block=None):
            each_z(lambda zz: self.along(zz, z, block).start())

        def stage2(self):
            each_z(lambda zz: self.along(zz, zz).wait_recv())
            self.beside(0, r).start()
            self.beside(1, r).start()

        def stage3(self):
            self.beside(0, self.n2).wait_recv()
            self.beside(2, self.n2).start()

        def done(self):
            self.beside(1, self.n1).wait_recv()
            self.beside(2, dn).wait_recv()
            each_z(lambda zz: self.along(zz, z).wait_send())
            self.beside(0, r).wait_send()
            self.beside(1, r).wait_send()
            self.beside(2, self.n2).wait_send()

    class ScatterZ(Scatter):
        def far(self, zz, src):
            c = self.c
            return move(
                self.s1.at[c, :, zz], rz.at[along_z[c], src], self.vs.at[c, zz], self.vr.at[c, src], device(zz, r, t)
            )

        def first(self, k):
            rr = self.n1 if k else dn
            c = self.c
            return move(self.s2.at[c, rr], self.r2.at[c, k], self.ts.at[c, k], self.tr.at[c, k], device(z, self.n1, t))

        def second(self):
            c = self.c
            return move(self.s3.at[c, 0], self.r3.at[c, 0], self.us.at[c], self.ur.at[c], device(z, self.n2, t))

        def stage1(self):
            each_z(lambda zz: self.far(zz, z).start())

        def stage2(self):
            each_z(lambda zz: self.far(zz, zz).wait_recv())

            def add(rr, carry):
                total = self.mine(rr, z)
                for e in range(1, Z):
                    total = total + rz[along_z[self.c], other(e), rr].astype(f32)
                self.own[self.slot, self.h, rr, z] = total
                self.s2[self.c, rr] = total.astype(bf16)
                return carry

            lax.fori_loop(0, R, add, 0)
            self.first(0).start()
            self.first(1).start()

        def stage3(self, put):
            c = self.c
            self.first(0).wait_recv()
            self.s3[c, 0] = (self.mine(self.n2, z) + self.r2[c, 0].astype(f32)).astype(bf16)
            self.second().start()

        def last(self, get, put):
            c = self.c
            self.first(1).wait_recv()
            self.second().wait_recv()
            put(self.mine(r, z) + self.r2[c, 1].astype(f32) + self.r3[c, 0].astype(f32))

        def sent(self):
            self.first(0).wait_send()
            self.first(1).wait_send()
            self.second().wait_send()
            each_z(lambda zz: self.far(zz, z).wait_send())

    class GatherZ(Gather):
        def along(self, zz, src_z):
            place = self.ref.at[src_z, :, :, self.cols]
            return move(place, place, gz_send.at[self.g, zz], gz_recv.at[self.g, src_z], device(zz, r, t))

        def beside(self, k, rr):
            place = self.ref.at[z, rr, :, self.cols]
            to = self.n2 if k == 0 else self.n1
            return move(place, place, gx_send.at[self.g, k], gx_recv.at[self.g, k], device(z, to, t))

        def stage1(self):
            self.beside(0, r).start()
            self.beside(1, r).start()

        def stage2(self):
            self.beside(0, self.n2).wait_recv()
            self.beside(2, self.n2).start()

        def stage3(self):
            self.beside(1, self.n1).wait_recv()
            self.beside(2, dn).wait_recv()
            each_z(lambda zz: self.along(zz, z).start())

        def done(self):
            each_z(lambda zz: self.along(zz, zz).wait_recv())
            each_z(lambda zz: self.along(zz, z).wait_send())
            self.beside(0, r).wait_send()
            self.beside(1, r).wait_send()
            self.beside(2, self.n2).wait_send()

    main_refs = (own, s1, r1, s2, r2, s3, r3)
    main_sems = (t_send, t_recv, u_send, u_recv, v_send, v_recv)
    proj_refs = (own_p, s1_p, r1_p, s2_p, r2_p, s3_p, r3_p)
    proj_sems = (tp_send, tp_recv, up_send, up_recv, vp_send, vp_recv)

    slots = {}
    z_scatter, z_gather = z_pairs(NP)
    along_z = {2 * p + h: 2 * i + h for i, p in enumerate(z_scatter) for h in (0, 1)}

    def scatter(p, h):
        kind = ScatterZ if p in z_scatter else Scatter
        return kind(2 * p + h, h, slots[p], main_refs, main_sems)

    def scatter_p(h):
        return Scatter(h, h, 0, proj_refs, proj_sems)

    def gather_w(p, h):
        kind = GatherZ if p in z_gather else Gather
        return kind(2 * p + h, h, wc_ref, lanes(2 * p + h, LANES))

    def gather_f(h):
        return Gather(2 * NP + h, h, f_all, pl.ds(h * (RK // 2), RK // 2), share)

    def gather_q(h):
        return Gather(2 * NP + 2 + h, h, q_all, pl.ds(h * HALF, HALF))

    share = pl.ds(pl.multiple_of(t * (FR // T), FR // T), FR // T)
    f_all[z, r, share] = f_ref[share, :]
    pl.semaphore_wait(barrier, N * T - 1)

    def product(p):
        need(("o", p))
        cols = lanes(p, PAIR)
        slot = slots[p]
        G = R * FR

        def tile(zz, carry):
            part = pl.ds(pl.multiple_of(zz * G, G), G)
            value = jnp.dot(mt[part, :], o_ref[:, cols], preferred_element_type=f32)
            for h in (0, 1):
                for rr in range(R):
                    block = value[rr * FR : (rr + 1) * FR, h * LANES : (h + 1) * LANES]
                    own[slot, h, rr, zz] = block
                    s1[2 * p + h, rr, zz] = block.astype(bf16)
            return carry

        lax.fori_loop(0, Z, tile, 0)
        if p in z_scatter:
            both(lambda h: scatter(p, h).stage1())
            return
        for k in (0, 1):
            for h in (0, 1):
                scatter(p, h).first(k).start()

    def start_factors():
        for h in (0, 1):
            gather_f(h).stage1(f_ref.at[share, pl.ds(h * (RK // 2), RK // 2)])

    def swap_factors():
        place = f_all.at[:, :, share, :]
        return move(place, place, cross_send, cross_recv, device(z, r, 1 - t))

    def finish_factors():
        both(lambda h: gather_f(h).done())
        swap_factors().start()

    def low_rank():
        swap_factors().wait()
        ft[...] = f_all[...].reshape(DH, RK).T

        def low(i, carry):
            yt[:, lanes(i, PAIR)] = jnp.dot(
                ft[...], mt[:, lanes(i, PAIR)], preferred_element_type=f32
            ).astype(bf16)
            return carry

        lax.fori_loop(0, TOK // PAIR, low, 0)

    def project(h):
        need(*[("o", h * (NP // 2) + n) for n in range(NP // 2)])

        def tile(n, carry):
            value = jnp.dot(yt[...], o_ref[:, lanes(h * (NP // 2) + n, PAIR)], preferred_element_type=f32)
            cols = lanes(n, PAIR)
            for zz in range(Z):
                for rr in range(R):
                    low_row = (zz * R + rr) * MR
                    block = value[low_row : low_row + MR, :]
                    own_p[0, h, rr, zz, :, cols] = block
                    s1_p[h, rr, zz, :, cols] = block.astype(bf16)
            return carry

        lax.fori_loop(0, NP // 2, tile, 0)
        for k in (0, 1):
            scatter_p(h).first(k).start()

    def s_copy(p, slot_of):
        q = lax.rem(every + p, N * T)
        d = q // T
        slot = slot_of(q)
        return move(
            stat, stat_all.at[slot], st_send.at[q], st_recv.at[slot],
            device(d // R, lax.rem(d, R), lax.rem(q, T)),
        )

    def fold(value):
        row = jnp.sum(value, axis=0, keepdims=True)
        total = row[:, :LANES]
        for j in range(1, CW // LANES):
            total = total + row[:, j * LANES : (j + 1) * LANES]
        return jnp.broadcast_to(total, (8, LANES))

    def moments():
        need("m1", "m2")
        projected = proj[...]
        new_first = 0.8 * m1_ref[...] + 0.2 * projected
        new_second = 0.9 * m2_ref[...] + 0.1 * projected * projected
        nf_ref[...] = new_first
        ns_ref[...] = new_second
        dir_wide = (new_first / (jnp.sqrt(new_second) + 1e-08)).astype(bf16).astype(f32)
        proj_wide = projected.astype(bf16).astype(f32)
        stat[0] = fold(dir_wide * dir_wide)
        stat[1] = fold(proj_wide * proj_wide)
        stat_all[every] = stat[...]

        def send(p, carry):
            s_copy(p, lambda q: every).start()
            return carry

        lax.fori_loop(1, N * T, send, 0)

    def combine():
        def wait(p, carry):
            s_copy(p, lambda q: q).wait()
            return carry

        lax.fori_loop(1, N * T, wait, 0)
        totals = jnp.sum(stat_all[...], axis=0)
        dir_sum = jnp.sum(totals[0, 0:1, :], axis=1, keepdims=True)
        proj_sum = jnp.sum(totals[1, 0:1, :], axis=1, keepdims=True)
        scale_ratio = jnp.sqrt(dir_sum) / jnp.sqrt(proj_sum + 1e-06)
        ratio[...] = jnp.broadcast_to(scale_ratio, (8, PAIR))
        projected = proj[...]
        dir_wide = (nf_ref[...] / (jnp.sqrt(ns_ref[...]) + 1e-08)).astype(bf16).astype(f32)
        mixed = (dir_wide - scale_ratio * projected.astype(bf16).astype(f32)).astype(bf16)
        q_own[...] = mixed
        q_all[z, r] = mixed
        for h in (0, 1):
            gather_q(h).stage1(q_own.at[:, pl.ds(h * HALF, HALF)])

    def put_proj(h):
        def put(value):
            proj[:, h * HALF : (h + 1) * HALF] = value

        return put

    def get_proj(h):
        return lambda: proj[:, h * HALF : (h + 1) * HALF]

    def both(action):
        for h in (0, 1):
            action(h)

    def finish_moments():
        both(lambda h: scatter_p(h).last(get_proj(h), put_proj(h)))
        moments()

    def put_grad(p, h):
        def put(value):
            upd_ref[:, lanes(2 * p + h, LANES)] = value

        return put

    def get_grad(p, h):
        return lambda: upd_ref[:, lanes(2 * p + h, LANES)]

    def update(p):
        need("w")
        cols = lanes(p, PAIR)
        mixed = q_all[:, :, :, cols].reshape(RK, PAIR)
        value = jnp.dot(f_ref[...], mixed, preferred_element_type=f32) + ratio[0:1, :] * upd_ref[:, cols]
        upd_ref[:, cols] = value
        new_weight = w_ref[:, cols] - 0.01 * value
        nw_ref[:, cols] = new_weight
        wc_ref[z, r, :, cols] = new_weight.astype(bf16)
        both(lambda h: gather_w(p, h).stage1())

    single = {
        "F1": start_factors,
        "F2": lambda: both(lambda h: gather_f(h).stage2()),
        "F3": lambda: both(lambda h: gather_f(h).stage3()),
        "F4": finish_factors,
        "PM": low_rank,
        "P4": finish_moments,
        "Q1": combine,
        "Q2": lambda: both(lambda h: gather_q(h).stage2()),
        "Q3": lambda: both(lambda h: gather_q(h).stage3()),
        "Q4": lambda: both(lambda h: gather_q(h).done()),
    }
    indexed = {
        "P1": project,
        "P2": lambda h: scatter_p(h).stage2(),
        "P3": lambda h: scatter_p(h).stage3(put_proj(h)),
        "f1": product,
        "f2": lambda p: both(lambda h: scatter(p, h).stage2()),
        "f3": lambda p: both(lambda h: scatter(p, h).stage3(put_grad(p, h))),
        "f4": lambda p: both(lambda h: scatter(p, h).last(get_grad(p, h), put_grad(p, h))),
        "g1": update,
        "g2": lambda p: both(lambda h: gather_w(p, h).stage2()),
        "g3": lambda p: both(lambda h: gather_w(p, h).stage3()),
        "g4": lambda p: both(lambda h: gather_w(p, h).done()),
    }
    free, issued = list(range(own.shape[0])), []
    for name, *index in order_for(NP):
        if not index:
            single[name]()
            continue
        if name == "f1":
            slots[index[0]] = free.pop(0)
        indexed[name](index[0])
        if name == ("f4" if index[0] in z_scatter else "f3"):
            free.append(slots[index[0]])
            issued.append(index[0])
        if name == "g3" and issued:
            p = issued.pop(0)
            both(lambda h: scatter(p, h).sent())
    for p in issued:
        both(lambda h: scatter(p, h).sent())
    both(lambda h: scatter_p(h).sent())


def fused(Z, R, T, *args):
    mixer_out, out_grad, factors, weight, first_moment, second_moment = args
    N = Z * R
    TOK, DH = mixer_out.shape
    FR, RK = factors.shape
    MR, CW = first_moment.shape
    NC, HALF = CW // LANES, CW // 2
    f32, bf16 = jnp.float32, jnp.bfloat16
    vmem = pl.BlockSpec(memory_space=pltpu.VMEM)
    dma = pltpu.SemaphoreType.DMA
    pair = lambda *shape: [dma(shape), dma(shape)]
    outs = pl.pallas_call(
        functools.partial(fused_kernel, Z, R, T),
        out_shape=(
            pltpu.VMEM(weight.shape, f32),
            pltpu.VMEM(weight.shape, f32),
            pltpu.VMEM(first_moment.shape, f32),
            pltpu.VMEM(first_moment.shape, f32),
            pltpu.VMEM((Z, R, FR, CW), bf16),
        ),
        in_specs=[pl.BlockSpec(memory_space=pltpu.HBM)] * 6,
        out_specs=(vmem,) * 5,
        scratch_shapes=[
            *[pltpu.VMEM(a.shape, a.dtype) for a in args],
            dma((DH // PAIR + CW // PAIR + 4,)),
            pltpu.VMEM((DH, TOK), bf16),
            pltpu.VMEM((live_pairs(CW // PAIR), 2, R, Z, FR, LANES), f32),
            pltpu.VMEM((NC, R, Z, FR, LANES), bf16),
            pltpu.VMEM((NC, 2, Z, FR, LANES), bf16),
            pltpu.VMEM((NC, max(Z, R), FR, LANES), bf16),
            pltpu.VMEM((NC, max(Z, R), FR, LANES), bf16),
            pltpu.VMEM((NC, Z, FR, LANES), bf16),
            pltpu.VMEM((NC, Z, FR, LANES), bf16),
            pltpu.VMEM((max(1, 2 * len(z_pairs(CW // PAIR)[0])), Z, R, FR, LANES), bf16),
            pltpu.VMEM((Z, R, FR, RK), bf16),
            pltpu.VMEM((RK, DH), bf16),
            pltpu.VMEM((RK, TOK), bf16),
            pltpu.VMEM((1, 2, R, Z, MR, HALF), f32),
            pltpu.VMEM((2, R, Z, MR, HALF), bf16),
            pltpu.VMEM((2, 2, Z, MR, HALF), bf16),
            pltpu.VMEM((2, Z, MR, HALF), bf16),
            pltpu.VMEM((2, Z, MR, HALF), bf16),
            pltpu.VMEM((2, Z, MR, HALF), bf16),
            pltpu.VMEM((2, Z, MR, HALF), bf16),
            pltpu.VMEM((MR, CW), f32),
            pltpu.VMEM((Z, R, MR, CW), bf16),
            pltpu.VMEM((MR, CW), bf16),
            pltpu.VMEM((2, 8, LANES), f32),
            pltpu.VMEM((N * T, 2, 8, LANES), f32),
            pltpu.VMEM((8, PAIR), f32),
            *pair(NC, 2), *pair(NC), *pair(NC, Z),
            *pair(2, 2), *pair(2), *pair(2, Z),
            *pair(NC + 4, Z), *pair(NC + 4, 3),
            *pair(N * T), dma, dma,
        ],
        compiler_params=pltpu.CompilerParams(
            collective_id=0, has_side_effects=True, vmem_limit_bytes=VMEM_GRANT
        ),
    )(*args)
    new_weight, update, new_first, new_second, copy = drain_out(*outs)
    return new_weight, update, new_first, new_second, copy.reshape(DH, CW)


def plain(mixer_out, out_grad, factors, weight, first_moment, second_moment):
    columns = mixer_out
    gradient = lax.psum_scatter(
        contract_rows(columns, out_grad), ("fs", "rep"), scatter_dimension=0, tiled=True
    )
    grad_low = gradient.astype(jnp.bfloat16)
    columns = factors
    projected = lax.psum_scatter(
        contract_rows(columns, grad_low), ("fs", "rep"), scatter_dimension=0, tiled=True
    )
    new_first = 0.8 * first_moment + 0.2 * projected
    new_second = 0.9 * second_moment + 0.1 * projected * projected
    direction = new_first / (jnp.sqrt(new_second) + 1e-08)
    dir_low = direction.astype(jnp.bfloat16)
    proj_low = projected.astype(jnp.bfloat16)
    dir_whole, proj_whole = (
        lax.all_gather(dir_low, ("fs", "rep"), axis=0, tiled=True),
        lax.all_gather(proj_low, ("fs", "rep"), axis=0, tiled=True),
    )
    dir_wide = dir_low.astype(jnp.float32)
    proj_wide = proj_low.astype(jnp.float32)
    dir_sum, proj_sum = lax.psum(
        (jnp.sum(dir_wide * dir_wide), jnp.sum(proj_wide * proj_wide)), ("fs", "rep", "tp")
    )
    back_dir = jnp.dot(factors, dir_whole, preferred_element_type=jnp.float32)
    back_proj = jnp.dot(factors, proj_whole, preferred_element_type=jnp.float32)
    scale_ratio = jnp.sqrt(dir_sum) / jnp.sqrt(proj_sum + 1e-06)
    update = back_dir + scale_ratio * (gradient - back_proj)
    new_weight = weight - 0.01 * update
    weight_copy = lax.all_gather(new_weight.astype(jnp.bfloat16), ("fs", "rep"), axis=0, tiled=True)
    return (new_weight, update, new_first, new_second, weight_copy)


def solution(mesh):
    Z, R, T = mesh.shape["fs"], mesh.shape["rep"], mesh.shape["tp"]

    def per_device(*args):
        mixer_out, out_grad, factors, weight, first_moment, second_moment = args
        fits = (
            out_grad.shape[1] % (4 * PAIR) == 0
            and mixer_out.shape[0] % PAIR == 0
            and mixer_out.shape[1] % PAIR == 0
            and weight.shape[0] % 16 == 0
            and first_moment.shape[0] % 16 == 0
            and factors.shape[1] == PAIR
            and weight.shape[0] % (16 * T) == 0
            and R == 4
            and T == 2
            and Z == R
            and Z > 1
        )
        return fused(Z, R, T, *args) if fits else plain(*args)

    in_specs = (
        P(("fs", "rep"), None),
        P(("fs", "rep"), "tp"),
        P(("fs", "rep"), None),
        P(("fs", "rep"), "tp"),
        P(("fs", "rep"), "tp"),
        P(("fs", "rep"), "tp"),
    )
    out_specs = (
        P(("fs", "rep"), "tp"),
        P(("fs", "rep"), "tp"),
        P(("fs", "rep"), "tp"),
        P(("fs", "rep"), "tp"),
        P(None, "tp"),
    )
    return jax.shard_map(
        per_device, mesh=mesh, in_specs=in_specs, out_specs=out_specs, check_vma=False
    )
```

```python
import functools

import jax
import jax.numpy as jnp
from jax import lax
from jax.experimental import pallas as pl
from jax.experimental.pallas import tpu as pltpu
from jax.sharding import PartitionSpec as P

MESH = pl.DeviceIdType.MESH
LANES = 128
PAIR = 2 * LANES
VMEM_GRANT = 52 * 1024 * 1024


ORDER = (
    "F1 f1.0 f1.1 F2",
    "f2.0.1 f2.0.0 F3 f1.6",
    "F4 f1.4 PM P1.0",
    "P1.1 f3.0.1 f2.6.1 f3.0.0",
    "P2.0 P2.1 f1.2 P3.0",
    "f2.6.0 f4.0.0 f2.4.1 P3.1",
    "f2.1.1 f1.3 f3.6.1 f3.4.1",
    "f2.2.1 f2.4.0 P4 f4.0.1",
    "f3.1.1 f1.5 f3.4.0 f2.3.0",
    "f3.2.1 f2.2.0 f2.3.1 Q1",
    "f2.5.0 f1.7 f3.2.0 f2.5.1",
    "f4.2.1 f3.3.0 Q2.1 f3.6.0",
    "f4.6.1 f2.1.0 Q2.0 f3.3.1",
    "f4.1.1 f4.4.1 f3.5.1 f2.7.0",
    "f3.1.0 Q3.1 Q3.0 f3.5.0",
    "f3.7.0 f4.2.0 f2.7.1 f4.4.0",
    "f4.5.1 f4.3.0 f4.1.0 Q4",
    "g1.2 g1.1 g1.0 g1.4",
    "f4.6.0 ga.2 f4.5.0 f4.3.1",
    "g1.5 g2.0.1 g2.0.0 ga.1",
    "g1.3 g2.2.1 f3.7.1 g2.2.0",
    "ga.4 g2.3.0 g1.6 g2.1.1",
    "g2.1.0 ga.5 g2.4.0 g3.0.0",
    "g3.2.1 g2.3.1 f4.7.1 g2.4.1",
    "ga.6 g2.5.0 f4.7.0 g1.7",
    "g2.6.1 g3.3.0 g3.1.0 ga.0.0",
    "g4.2.1 g3.4.1 g2.5.1 g3.3.1",
    "g3.0.1 ga.7 g3.5.0 g4.1.0",
    "ga.3.0 g2.6.0 g3.5.1 g3.4.0",
    "g2.7.0 g2.7.1 g4.5.0 g3.1.1",
    "g3.6.0 ga.3.1 g3.6.1 g4.4.0",
    "g3.7.0 ga.0.1 g4.3.0 g4.0.0",
    "g3.2.0 g4.4.1 g3.7.1 g4.6.0",
    "g4.3.1 g4.7.0 g4.5.1 g4.1.1",
    "g4.6.1 g4.0.1 g4.2.0 g4.7.1",
)
Z_SCATTER = (1,)
Z_GATHER = (0, 3)


def token(text):
    name, *index = text.split(".")
    return (name, *map(int, index))


def order_for(NP):
    if NP == 8:
        return [token(a) for line in ORDER for a in line.split()]
    events = {
        1: "F2", 2: "F3", 3: "F4 PM P1.0 P1.1", 4: "P2.0 P2.1", 5: "P3.0 P3.1",
        6: "P4", 7: "Q1", 8: "Q2", 9: "Q3", 10: "Q4",
    }
    lags = {"f1": 0, "f2": 1, "f3": 2, "f4": 3, "g1": 10, "ga": 11, "g2": 11, "g3": 12, "g4": 13}
    order = [("F1",)]
    for i in range(max(NP, 1) + 14):
        for a in events.get(i, "").split():
            order.append(token(a))
        order += [(name, i - lag) for name, lag in lags.items() if 0 <= i - lag < NP]
    return order


def z_pairs(NP):
    return (Z_SCATTER, Z_GATHER) if NP == 8 else ((), ())


def live_pairs(NP):
    live, most, passed = 0, 0, {}
    z_scatter = z_pairs(NP)[0]
    for name, *index in order_for(NP):
        live += name == "f1"
        if index and name == ("f4" if index[0] in z_scatter else "f3"):
            p = index[0]
            passed[p] = passed.get(p, 0) + (1 if index[1:] else 2)
            live -= passed[p] == 2
        most = max(most, live)
    return most


def contract_rows(left, right):
    return lax.dot_general(
        left, right, (((0,), (0,)), ((), ())), preferred_element_type=jnp.float32
    )


def drain_kernel(*refs):
    n = len(refs) // 2
    ins, outs, sem = refs[:n], refs[n:-1], refs[-1]
    copies = [pltpu.make_async_copy(a, b, sem.at[i]) for i, (a, b) in enumerate(zip(ins, outs))]
    for c in copies:
        c.start()
    for c in copies:
        c.wait()


def drain_out(*arrays):
    return pl.pallas_call(
        drain_kernel,
        out_shape=tuple(jax.ShapeDtypeStruct(a.shape, a.dtype) for a in arrays),
        in_specs=[pl.BlockSpec(memory_space=pltpu.VMEM)] * len(arrays),
        out_specs=(pl.BlockSpec(memory_space=pl.ANY),) * len(arrays),
        scratch_shapes=[pltpu.SemaphoreType.DMA((len(arrays),))],
        compiler_params=pltpu.CompilerParams(vmem_limit_bytes=4 * 1024 * 1024),
    )(*[pltpu.with_memory_space_constraint(a, pltpu.VMEM) for a in arrays])


def fused_kernel(
    Z, R, T,
    m_hbm, o_hbm, f_hbm, w_hbm, m1_hbm, m2_hbm,
    nw_ref, upd_ref, nf_ref, ns_ref, wc_ref,
    m_ref, o_ref, f_ref, w_ref, m1_ref, m2_ref, load,
    mt, own, s1, r1, s2, r2, s3, r3, rz,
    f_all, ft, yt, own_p, s1_p, r1_p, s2_p, r2_p, s3_p, r3_p, proj, q_all, q_own,
    stat, stat_all, ratio,
    t_send, t_recv, u_send, u_recv, v_send, v_recv,
    tp_send, tp_recv, up_send, up_recv, vp_send, vp_recv,
    gz_send, gz_recv, gx_send, gx_recv, gf_send,
    st_send, st_recv, cross_send, cross_recv,
):
    N = Z * R
    z, r, t = lax.axis_index("fs"), lax.axis_index("rep"), lax.axis_index("tp")
    every = (z * R + r) * T + t
    TOK, DH = m_ref.shape
    CW = o_ref.shape[1]
    FR, RK = f_ref.shape
    MR = m1_ref.shape[0]
    NP = CW // PAIR
    HALF = CW // 2
    xn, yn, dn = r + 1 - 2 * lax.rem(r, 2), lax.rem(r + 2, R), R - 1 - r
    near = ((xn, yn), (yn, xn))
    low_half = z < 2
    twin = z + 1 - 2 * lax.rem(z, 2)
    cross = jnp.where(low_half, 2, 1)
    away = jnp.where(low_half, 2, 0)
    middle = (z == 1) | (z == 2)
    f32, bf16 = jnp.float32, jnp.bfloat16

    def device(zz, rr, tt):
        return {"fs": zz, "rep": rr, "tp": tt}

    def lanes(index, size):
        return pl.ds(pl.multiple_of(index * size, size), size)

    def other(e):
        return lax.rem(z + e, Z)

    def each_z(body):
        def step(e, carry):
            body(other(e))
            return carry

        lax.fori_loop(1, Z, step, 0)

    def fetch(src, dst, index):
        return pltpu.make_async_copy(src, dst, load.at[index])

    loads = {"f": fetch(f_hbm, f_ref, 0)}
    for i in range(DH // PAIR):
        part = pl.ds(i * PAIR, PAIR)
        loads["m", i] = fetch(m_hbm.at[:, part], m_ref.at[:, part], len(loads))
    for i in range(NP):
        part = pl.ds(i * PAIR, PAIR)
        loads["o", i] = fetch(o_hbm.at[:, part], o_ref.at[:, part], len(loads))
    for name, src, dst in (("m1", m1_hbm, m1_ref), ("m2", m2_hbm, m2_ref), ("w", w_hbm, w_ref)):
        loads[name] = fetch(src, dst, len(loads))
    for copy in loads.values():
        copy.start()

    def need(*names):
        for name in names:
            if name in loads:
                loads.pop(name).wait()

    barrier = pltpu.get_barrier_semaphore()

    def greet(zz, rr, tt):
        pl.semaphore_signal(barrier, inc=1, device_id=device(zz, rr, tt), device_id_type=MESH)

    each_z(lambda zz: greet(zz, r, t))
    greet(z, xn, t)
    greet(z, yn, t)
    greet(z, r, 1 - t)

    for i in range(DH // PAIR):
        need(("m", i))
        mt[i * PAIR : (i + 1) * PAIR, :] = m_ref[:, i * PAIR : (i + 1) * PAIR].T
    need("f")

    def move(src, dst, ss, rs, where):
        return pltpu.make_async_remote_copy(
            src_ref=src, dst_ref=dst, send_sem=ss, recv_sem=rs, device_id=where, device_id_type=MESH
        )

    class Scatter:
        def __init__(self, c, h, slot, refs, sems):
            self.c, self.h, self.slot = c, h, slot
            self.own, self.s1, self.r1, self.s2, self.r2, self.s3, self.r3 = refs
            self.ts, self.tr, self.us, self.ur, self.vs, self.vr = sems
            self.n1, self.n2 = near[h]

        def first(self, k):
            rr = self.n1 if k else dn
            c = self.c
            return move(self.s1.at[c, rr], self.r1.at[c, k], self.ts.at[c, k], self.tr.at[c, k], device(z, self.n1, t))

        def second(self):
            c = self.c
            return move(self.s2.at[c], self.r2.at[c], self.us.at[c], self.ur.at[c], device(z, self.n2, t))

        def third(self, zz, src):
            c = self.c
            return move(
                self.s3.at[c, zz], self.r3.at[c, src], self.vs.at[c, zz], self.vr.at[c, src], device(zz, r, t)
            )

        def mine(self, rr, zz):
            return self.own[self.slot, self.h, rr, zz]

        def stage2(self):
            c = self.c
            self.first(0).wait_recv()

            def add(zz, carry):
                total = self.mine(self.n2, zz) + self.r1[c, 0, zz].astype(f32)
                self.s2[c, zz] = total.astype(bf16)
                return carry

            lax.fori_loop(0, Z, add, 0)
            self.second().start()

        def stage3(self, put):
            c = self.c
            self.first(1).wait_recv()
            self.second().wait_recv()

            def total(zz):
                return self.mine(r, zz) + self.r1[c, 1, zz].astype(f32) + self.r2[c, zz].astype(f32)

            def send(zz):
                self.s3[c, zz] = total(zz).astype(bf16)
                self.third(zz, z).start()

            each_z(send)
            put(total(z))

        def last(self, get, put):
            each_z(lambda zz: self.third(zz, zz).wait_recv())
            value = get()
            for e in range(1, Z):
                value = value + self.r3[self.c, other(e)].astype(f32)
            put(value)

        def sent(self):
            self.first(0).wait_send()
            self.first(1).wait_send()
            self.second().wait_send()
            each_z(lambda zz: self.third(zz, z).wait_send())

    class Gather:
        def __init__(self, g, h, ref, cols, rows=slice(None)):
            self.g, self.ref, self.cols, self.rows = g, ref, cols, rows
            self.n1, self.n2 = near[h]

        def along(self, zz, src_z, block=None, sent=None):
            place = self.ref.at[src_z, r, self.rows, self.cols]
            return move(
                place if block is None else block, place,
                gz_send.at[self.g, zz] if sent is None else sent, gz_recv.at[self.g, src_z], device(zz, r, t),
            )

        def beside(self, k, rr):
            place = self.ref.at[:, rr, self.rows, self.cols]
            to = self.n2 if k == 0 else self.n1
            return move(place, place, gx_send.at[self.g, k], gx_recv.at[self.g, k], device(z, to, t))

        def stage1(self, block=None):
            each_z(lambda zz: self.along(zz, z, block).start())

        def spread(self):
            self.along(cross, z).start()
            self.along(twin, z).start()

        def onward(self, k):
            return self.along(twin, away + k, None, gf_send.at[self.g, k])

        def forward(self):
            @pl.when(middle)
            def _():
                for k in (0, 1):
                    self.along(twin, away + k).wait_recv()
                    self.onward(k).start()

        def gathered(self):
            self.along(twin, twin).wait_recv()

            @pl.when(jnp.logical_not(middle))
            def _():
                for k in (0, 1):
                    self.along(twin, away + k).wait_recv()

        def spread_sent(self):
            self.along(cross, z).wait_send()
            self.along(twin, z).wait_send()

            @pl.when(middle)
            def _():
                for k in (0, 1):
                    self.onward(k).wait_send()

        def stage2(self, spread=False):
            if spread:
                self.gathered()
            else:
                each_z(lambda zz: self.along(zz, zz).wait_recv())
            self.beside(0, r).start()
            self.beside(1, r).start()

        def stage3(self):
            self.beside(0, self.n2).wait_recv()
            self.beside(2, self.n2).start()

        def done(self, spread=False):
            self.beside(1, self.n1).wait_recv()
            self.beside(2, dn).wait_recv()
            if spread:
                self.spread_sent()
            else:
                each_z(lambda zz: self.along(zz, z).wait_send())
            self.beside(0, r).wait_send()
            self.beside(1, r).wait_send()
            self.beside(2, self.n2).wait_send()

    class ScatterZ(Scatter):
        def far(self, zz, src):
            c = self.c
            return move(
                self.s1.at[c, :, zz], rz.at[along_z[c], src], self.vs.at[c, zz], self.vr.at[c, src], device(zz, r, t)
            )

        def first(self, k):
            rr = self.n1 if k else dn
            c = self.c
            return move(self.s2.at[c, rr], self.r2.at[c, k], self.ts.at[c, k], self.tr.at[c, k], device(z, self.n1, t))

        def second(self):
            c = self.c
            return move(self.s3.at[c, 0], self.r3.at[c, 0], self.us.at[c], self.ur.at[c], device(z, self.n2, t))

        def stage1(self):
            each_z(lambda zz: self.far(zz, z).start())

        def stage2(self):
            each_z(lambda zz: self.far(zz, zz).wait_recv())

            def add(rr, carry):
                total = self.mine(rr, z)
                for e in range(1, Z):
                    total = total + rz[along_z[self.c], other(e), rr].astype(f32)
                self.own[self.slot, self.h, rr, z] = total
                self.s2[self.c, rr] = total.astype(bf16)
                return carry

            lax.fori_loop(0, R, add, 0)
            self.first(0).start()
            self.first(1).start()

        def stage3(self, put):
            c = self.c
            self.first(0).wait_recv()
            self.s3[c, 0] = (self.mine(self.n2, z) + self.r2[c, 0].astype(f32)).astype(bf16)
            self.second().start()

        def last(self, get, put):
            c = self.c
            self.first(1).wait_recv()
            self.second().wait_recv()
            put(self.mine(r, z) + self.r2[c, 1].astype(f32) + self.r3[c, 0].astype(f32))

        def sent(self):
            self.first(0).wait_send()
            self.first(1).wait_send()
            self.second().wait_send()
            each_z(lambda zz: self.far(zz, z).wait_send())

    class GatherZ(Gather):
        def along(self, zz, src_z, block=None, sent=None):
            place = self.ref.at[src_z, :, :, self.cols]
            return move(
                place, place, gz_send.at[self.g, zz] if sent is None else sent, gz_recv.at[self.g, src_z],
                device(zz, r, t),
            )

        def beside(self, k, rr):
            place = self.ref.at[z, rr, :, self.cols]
            to = self.n2 if k == 0 else self.n1
            return move(place, place, gx_send.at[self.g, k], gx_recv.at[self.g, k], device(z, to, t))

        def begin(self):
            self.beside(0, r).start()
            self.beside(1, r).start()

        def stage2(self, spread=True):
            self.beside(0, self.n2).wait_recv()
            self.beside(2, self.n2).start()

        def stage3(self):
            self.beside(1, self.n1).wait_recv()
            self.beside(2, dn).wait_recv()
            self.spread()

        def done(self, spread=True):
            self.gathered()
            self.spread_sent()
            self.beside(0, r).wait_send()
            self.beside(1, r).wait_send()
            self.beside(2, self.n2).wait_send()

    main_refs = (own, s1, r1, s2, r2, s3, r3)
    main_sems = (t_send, t_recv, u_send, u_recv, v_send, v_recv)
    proj_refs = (own_p, s1_p, r1_p, s2_p, r2_p, s3_p, r3_p)
    proj_sems = (tp_send, tp_recv, up_send, up_recv, vp_send, vp_recv)

    slots = {}
    z_scatter, z_gather = z_pairs(NP)
    along_z = {2 * p + h: 2 * i + h for i, p in enumerate(z_scatter) for h in (0, 1)}

    def scatter(p, h):
        kind = ScatterZ if p in z_scatter else Scatter
        return kind(2 * p + h, h, slots[p], main_refs, main_sems)

    def scatter_p(h):
        return Scatter(h, h, 0, proj_refs, proj_sems)

    def gather_w(p, h):
        kind = GatherZ if p in z_gather else Gather
        return kind(2 * p + h, h, wc_ref, lanes(2 * p + h, LANES))

    def gather_f(h):
        return Gather(2 * NP + h, h, f_all, pl.ds(h * (RK // 2), RK // 2), share)

    def gather_q(h):
        return Gather(2 * NP + 2 + h, h, q_all, pl.ds(h * HALF, HALF))

    share = pl.ds(pl.multiple_of(t * (FR // T), FR // T), FR // T)
    f_all[z, r, share] = f_ref[share, :]
    pl.semaphore_wait(barrier, Z + 2)

    def product(p):
        need(("o", p))
        cols = lanes(p, PAIR)
        slot = slots[p]
        G = R * FR

        def tile(zz, carry):
            part = pl.ds(pl.multiple_of(zz * G, G), G)
            value = jnp.dot(mt[part, :], o_ref[:, cols], preferred_element_type=f32)
            for h in (0, 1):
                for rr in range(R):
                    block = value[rr * FR : (rr + 1) * FR, h * LANES : (h + 1) * LANES]
                    own[slot, h, rr, zz] = block
                    s1[2 * p + h, rr, zz] = block.astype(bf16)
            return carry

        lax.fori_loop(0, Z, tile, 0)
        if p in z_scatter:
            both(lambda h: scatter(p, h).stage1())
            return
        for k in (0, 1):
            for h in (0, 1):
                scatter(p, h).first(k).start()

    def start_factors():
        for h in (0, 1):
            gather_f(h).stage1(f_ref.at[share, pl.ds(h * (RK // 2), RK // 2)])

    def swap_factors():
        place = f_all.at[:, :, share, :]
        return move(place, place, cross_send, cross_recv, device(z, r, 1 - t))

    def finish_factors():
        both(lambda h: gather_f(h).done())
        swap_factors().start()

    def low_rank():
        swap_factors().wait()
        ft[...] = f_all[...].reshape(DH, RK).T

        def low(i, carry):
            yt[:, lanes(i, PAIR)] = jnp.dot(
                ft[...], mt[:, lanes(i, PAIR)], preferred_element_type=f32
            ).astype(bf16)
            return carry

        lax.fori_loop(0, TOK // PAIR, low, 0)

    def project(h):
        need(*[("o", h * (NP // 2) + n) for n in range(NP // 2)])

        def tile(n, carry):
            value = jnp.dot(yt[...], o_ref[:, lanes(h * (NP // 2) + n, PAIR)], preferred_element_type=f32)
            cols = lanes(n, PAIR)
            for zz in range(Z):
                for rr in range(R):
                    low_row = (zz * R + rr) * MR
                    block = value[low_row : low_row + MR, :]
                    own_p[0, h, rr, zz, :, cols] = block
                    s1_p[h, rr, zz, :, cols] = block.astype(bf16)
            return carry

        lax.fori_loop(0, NP // 2, tile, 0)
        for k in (0, 1):
            scatter_p(h).first(k).start()

    def s_copy(p, slot_of):
        q = lax.rem(every + p, N * T)
        d = q // T
        slot = slot_of(q)
        return move(
            stat, stat_all.at[slot], st_send.at[q], st_recv.at[slot],
            device(d // R, lax.rem(d, R), lax.rem(q, T)),
        )

    def fold(value):
        row = jnp.sum(value, axis=0, keepdims=True)
        total = row[:, :LANES]
        for j in range(1, CW // LANES):
            total = total + row[:, j * LANES : (j + 1) * LANES]
        return total

    def moments():
        need("m1", "m2")
        projected = proj[...]
        new_first = 0.8 * m1_ref[...] + 0.2 * projected
        new_second = 0.9 * m2_ref[...] + 0.1 * projected * projected
        nf_ref[...] = new_first
        ns_ref[...] = new_second
        dir_wide = (new_first / (jnp.sqrt(new_second) + 1e-08)).astype(bf16).astype(f32)
        proj_wide = projected.astype(bf16).astype(f32)
        stat[0:1, :] = fold(dir_wide * dir_wide)
        stat[1:2, :] = fold(proj_wide * proj_wide)
        stat_all[every] = stat[...]

        def send(p, carry):
            s_copy(p, lambda q: every).start()
            return carry

        lax.fori_loop(1, N * T, send, 0)

    def combine():
        def wait(p, carry):
            s_copy(p, lambda q: q).wait()
            return carry

        lax.fori_loop(1, N * T, wait, 0)
        totals = jnp.sum(stat_all[...], axis=0)
        dir_sum = jnp.sum(totals[0:1, :], axis=1, keepdims=True)
        proj_sum = jnp.sum(totals[1:2, :], axis=1, keepdims=True)
        scale_ratio = jnp.sqrt(dir_sum) / jnp.sqrt(proj_sum + 1e-06)
        ratio[...] = jnp.broadcast_to(scale_ratio, (8, PAIR))
        projected = proj[...]
        dir_wide = (nf_ref[...] / (jnp.sqrt(ns_ref[...]) + 1e-08)).astype(bf16).astype(f32)
        mixed = (dir_wide - scale_ratio * projected.astype(bf16).astype(f32)).astype(bf16)
        q_own[...] = mixed
        q_all[z, r] = mixed
        for h in (0, 1):
            gather_q(h).stage1(q_own.at[:, pl.ds(h * HALF, HALF)])

    def put_proj(h):
        def put(value):
            proj[:, h * HALF : (h + 1) * HALF] = value

        return put

    def get_proj(h):
        return lambda: proj[:, h * HALF : (h + 1) * HALF]

    def both(action):
        for h in (0, 1):
            action(h)

    def finish_moments():
        both(lambda h: scatter_p(h).last(get_proj(h), put_proj(h)))
        moments()

    def put_grad(p, h):
        def put(value):
            upd_ref[:, lanes(2 * p + h, LANES)] = value

        return put

    def get_grad(p, h):
        return lambda: upd_ref[:, lanes(2 * p + h, LANES)]

    def update(p):
        need("w")
        cols = lanes(p, PAIR)
        mixed = q_all[:, :, :, cols].reshape(RK, PAIR)
        value = jnp.dot(f_ref[...], mixed, preferred_element_type=f32) + ratio[0:1, :] * upd_ref[:, cols]
        upd_ref[:, cols] = value
        new_weight = w_ref[:, cols] - 0.01 * value
        nw_ref[:, cols] = new_weight
        wc_ref[z, r, :, cols] = new_weight.astype(bf16)
        if p in z_gather:
            both(lambda h: gather_w(p, h).begin())
        else:
            both(lambda h: gather_w(p, h).spread())

    single = {
        "F1": start_factors,
        "F2": lambda: both(lambda h: gather_f(h).stage2()),
        "F3": lambda: both(lambda h: gather_f(h).stage3()),
        "F4": finish_factors,
        "PM": low_rank,
        "P4": finish_moments,
        "Q1": combine,
        "Q4": lambda: both(lambda h: gather_q(h).done()),
    }
    halves = {
        "P1": project,
        "P2": lambda h: scatter_p(h).stage2(),
        "P3": lambda h: scatter_p(h).stage3(put_proj(h)),
        "Q2": lambda h: gather_q(h).stage2(),
        "Q3": lambda h: gather_q(h).stage3(),
    }
    pairs = {"f1": product, "g1": update}
    chunks = {
        "f2": lambda p, h: scatter(p, h).stage2(),
        "f3": lambda p, h: scatter(p, h).stage3(put_grad(p, h)),
        "f4": lambda p, h: scatter(p, h).last(get_grad(p, h), put_grad(p, h)),
        "ga": lambda p, h: gather_w(p, h).forward(),
        "g2": lambda p, h: gather_w(p, h).stage2(True),
        "g3": lambda p, h: gather_w(p, h).stage3(),
        "g4": lambda p, h: gather_w(p, h).done(True),
    }
    free, issued, passed = list(range(own.shape[0])), [], {}
    for name, *index in order_for(NP):
        if name in single:
            single[name]()
        elif name in halves:
            for h in index or (0, 1):
                halves[name](h)
        elif name in pairs:
            p = index[0]
            if name == "f1":
                slots[p] = free.pop(0)
            pairs[name](p)
        else:
            p = index[0]
            for h in index[1:] or (0, 1):
                chunks[name](p, h)
                if name == ("f4" if p in z_scatter else "f3"):
                    passed[p] = passed.get(p, 0) + 1
                    if passed[p] == 2:
                        free.append(slots[p])
                        issued.append(p)
            if name == "g3" and issued:
                p = issued.pop(0)
                both(lambda h: scatter(p, h).sent())
    for p in issued:
        both(lambda h: scatter(p, h).sent())
    both(lambda h: scatter_p(h).sent())


def fused(Z, R, T, *args):
    mixer_out, out_grad, factors, weight, first_moment, second_moment = args
    N = Z * R
    TOK, DH = mixer_out.shape
    FR, RK = factors.shape
    MR, CW = first_moment.shape
    NC, HALF = CW // LANES, CW // 2
    f32, bf16 = jnp.float32, jnp.bfloat16
    vmem = pl.BlockSpec(memory_space=pltpu.VMEM)
    dma = pltpu.SemaphoreType.DMA
    pair = lambda *shape: [dma(shape), dma(shape)]
    outs = pl.pallas_call(
        functools.partial(fused_kernel, Z, R, T),
        out_shape=(
            pltpu.VMEM(weight.shape, f32),
            pltpu.VMEM(weight.shape, f32),
            pltpu.VMEM(first_moment.shape, f32),
            pltpu.VMEM(first_moment.shape, f32),
            pltpu.VMEM((Z, R, FR, CW), bf16),
        ),
        in_specs=[pl.BlockSpec(memory_space=pltpu.HBM)] * 6,
        out_specs=(vmem,) * 5,
        scratch_shapes=[
            *[pltpu.VMEM(a.shape, a.dtype) for a in args],
            dma((DH // PAIR + CW // PAIR + 4,)),
            pltpu.VMEM((DH, TOK), bf16),
            pltpu.VMEM((live_pairs(CW // PAIR), 2, R, Z, FR, LANES), f32),
            pltpu.VMEM((NC, R, Z, FR, LANES), bf16),
            pltpu.VMEM((NC, 2, Z, FR, LANES), bf16),
            pltpu.VMEM((NC, max(Z, R), FR, LANES), bf16),
            pltpu.VMEM((NC, max(Z, R), FR, LANES), bf16),
            pltpu.VMEM((NC, Z, FR, LANES), bf16),
            pltpu.VMEM((NC, Z, FR, LANES), bf16),
            pltpu.VMEM((max(1, 2 * len(z_pairs(CW // PAIR)[0])), Z, R, FR, LANES), bf16),
            pltpu.VMEM((Z, R, FR, RK), bf16),
            pltpu.VMEM((RK, DH), bf16),
            pltpu.VMEM((RK, TOK), bf16),
            pltpu.VMEM((1, 2, R, Z, MR, HALF), f32),
            pltpu.VMEM((2, R, Z, MR, HALF), bf16),
            pltpu.VMEM((2, 2, Z, MR, HALF), bf16),
            pltpu.VMEM((2, Z, MR, HALF), bf16),
            pltpu.VMEM((2, Z, MR, HALF), bf16),
            pltpu.VMEM((2, Z, MR, HALF), bf16),
            pltpu.VMEM((2, Z, MR, HALF), bf16),
            pltpu.VMEM((MR, CW), f32),
            pltpu.VMEM((Z, R, MR, CW), bf16),
            pltpu.VMEM((MR, CW), bf16),
            pltpu.VMEM((2, LANES), f32),
            pltpu.VMEM((N * T, 2, LANES), f32),
            pltpu.VMEM((8, PAIR), f32),
            *pair(NC, 2), *pair(NC), *pair(NC, Z),
            *pair(2, 2), *pair(2), *pair(2, Z),
            *pair(NC + 4, Z), *pair(NC + 4, 3), dma((NC + 4, 2)),
            *pair(N * T), dma, dma,
        ],
        compiler_params=pltpu.CompilerParams(
            collective_id=0, has_side_effects=True, vmem_limit_bytes=VMEM_GRANT
        ),
    )(*args)
    new_weight, update, new_first, new_second, copy = drain_out(*outs)
    return new_weight, update, new_first, new_second, copy.reshape(DH, CW)


def plain(mixer_out, out_grad, factors, weight, first_moment, second_moment):
    columns = mixer_out
    gradient = lax.psum_scatter(
        contract_rows(columns, out_grad), ("fs", "rep"), scatter_dimension=0, tiled=True
    )
    grad_low = gradient.astype(jnp.bfloat16)
    columns = factors
    projected = lax.psum_scatter(
        contract_rows(columns, grad_low), ("fs", "rep"), scatter_dimension=0, tiled=True
    )
    new_first = 0.8 * first_moment + 0.2 * projected
    new_second = 0.9 * second_moment + 0.1 * projected * projected
    direction = new_first / (jnp.sqrt(new_second) + 1e-08)
    dir_low = direction.astype(jnp.bfloat16)
    proj_low = projected.astype(jnp.bfloat16)
    dir_whole, proj_whole = (
        lax.all_gather(dir_low, ("fs", "rep"), axis=0, tiled=True),
        lax.all_gather(proj_low, ("fs", "rep"), axis=0, tiled=True),
    )
    dir_wide = dir_low.astype(jnp.float32)
    proj_wide = proj_low.astype(jnp.float32)
    dir_sum, proj_sum = lax.psum(
        (jnp.sum(dir_wide * dir_wide), jnp.sum(proj_wide * proj_wide)), ("fs", "rep", "tp")
    )
    back_dir = jnp.dot(factors, dir_whole, preferred_element_type=jnp.float32)
    back_proj = jnp.dot(factors, proj_whole, preferred_element_type=jnp.float32)
    scale_ratio = jnp.sqrt(dir_sum) / jnp.sqrt(proj_sum + 1e-06)
    update = back_dir + scale_ratio * (gradient - back_proj)
    new_weight = weight - 0.01 * update
    weight_copy = lax.all_gather(new_weight.astype(jnp.bfloat16), ("fs", "rep"), axis=0, tiled=True)
    return (new_weight, update, new_first, new_second, weight_copy)


def solution(mesh):
    Z, R, T = mesh.shape["fs"], mesh.shape["rep"], mesh.shape["tp"]

    def per_device(*args):
        mixer_out, out_grad, factors, weight, first_moment, second_moment = args
        fits = (
            out_grad.shape[1] % (4 * PAIR) == 0
            and mixer_out.shape[0] % PAIR == 0
            and mixer_out.shape[1] % PAIR == 0
            and weight.shape[0] % 16 == 0
            and first_moment.shape[0] % 16 == 0
            and factors.shape[1] == PAIR
            and weight.shape[0] % (16 * T) == 0
            and R == 4
            and T == 2
            and Z == R
            and Z > 1
        )
        return fused(Z, R, T, *args) if fits else plain(*args)

    in_specs = (
        P(("fs", "rep"), None),
        P(("fs", "rep"), "tp"),
        P(("fs", "rep"), None),
        P(("fs", "rep"), "tp"),
        P(("fs", "rep"), "tp"),
        P(("fs", "rep"), "tp"),
    )
    out_specs = (
        P(("fs", "rep"), "tp"),
        P(("fs", "rep"), "tp"),
        P(("fs", "rep"), "tp"),
        P(("fs", "rep"), "tp"),
        P(None, "tp"),
    )
    return jax.shard_map(
        per_device, mesh=mesh, in_specs=in_specs, out_specs=out_specs, check_vma=False
    )
```

```python
import functools

import jax
import jax.numpy as jnp
from jax import lax
from jax.experimental import pallas as pl
from jax.experimental.pallas import tpu as pltpu
from jax.sharding import PartitionSpec as P

MESH = pl.DeviceIdType.MESH
LANES = 128
PAIR = 2 * LANES
PARTS = 4
VMEM_GRANT = 52 * 1024 * 1024


ORDER = (
    "F1 f1.4 f1.1 F2",
    "f1.0 F3 f2.4.1 f1.6",
    "F4 f2.0.1 f2.0.0 f2.4.0",
    "f3.4.1 PM P1.3 P1.2",
    "P1.1 P1.0 f3.0.1 f3.0.0",
    "P2.3 P2.2 f1.2 f2.6.1",
    "P2.0 P3.2 P3.3 f2.6.0",
    "f3.4.0 f2.2.0 P2.1 f1.3",
    "f2.1.1 P3.0 P3.1 f2.1.0",
    "f3.6.1 f2.2.1 f3.2.0 f3.6.0",
    "f2.3.1 f2.3.0 P4 f1.7",
    "f3.3.0 f3.2.1 f1.5 Q1",
    "f4.3.0 f2.7.0 f3.1.1 f2.7.1",
    "f3.3.1 f4.4.1 f4.2.1 f4.6.1",
    "Q2.0 f3.1.0 f4.1.1 f4.2.0",
    "f4.4.0 Q2.1 f2.5.0 f3.7.1",
    "Q3.0 f2.5.1 f4.6.0 Q2.3",
    "f3.7.0 f4.0.1 Q3.1 f4.1.0",
    "Q4.0 g1.1 f4.7.1 f4.3.1",
    "Q2.2 f3.5.1 Q4.1 Q3.3",
    "g1.2 f4.0.0 g1.3 ga.1",
    "Q3.2 f4.7.0 Q4.3 g1.6",
    "g2.3.0 g2.1.1 f3.5.0 ga.2",
    "g1.0 g2.1.0 Q4.2 g1.4",
    "g2.3.1 ga.6 f4.5.1 g2.2.1",
    "g1.7 g2.2.0 f4.5.0 g1.5",
    "g2.0.0 g3.3.0 g2.0.1 g2.6.1",
    "ga.4 g3.2.1 g3.1.1 ga.7",
    "g3.1.0 g2.6.0 g2.4.0 g3.0.1",
    "ga.5 g3.6.1 g3.2.0 g2.7.0",
    "g3.0.0 g2.5.0 g2.5.1 g2.7.1",
    "g4.1.0 g3.3.1 g2.4.1 g3.6.0",
    "ga.3.0 ga.0.1 g4.2.1 ga.0.0",
    "g4.1.1 g4.3.0 g3.5.1 g3.4.0",
    "g3.7.1 ga.3.1 g3.4.1 g3.5.0",
    "g4.6.0 g3.7.0 g4.2.0 g4.6.1",
    "g4.5.1 g4.0.0 g4.4.0 g4.0.1",
    "g4.7.1 g4.5.0 g4.3.1 g4.7.0",
    "g4.4.1",
)
Z_SCATTER = (1,)
Z_GATHER = (0, 3)


def token(text):
    name, *index = text.split(".")
    return (name, *map(int, index))


def order_for(NP):
    if NP == 8:
        return [token(a) for line in ORDER for a in line.split()]
    events = {
        1: "F2", 2: "F3", 3: "F4 PM P1", 4: "P2", 5: "P3",
        6: "P4", 7: "Q1", 8: "Q2", 9: "Q3", 10: "Q4",
    }
    lags = {"f1": 0, "f2": 1, "f3": 2, "f4": 3, "g1": 10, "ga": 11, "g2": 11, "g3": 12, "g4": 13}
    order = [("F1",)]
    for i in range(max(NP, 1) + 14):
        for a in events.get(i, "").split():
            order.append(token(a))
        order += [(name, i - lag) for name, lag in lags.items() if 0 <= i - lag < NP]
    return order


def z_pairs(NP):
    return (Z_SCATTER, Z_GATHER) if NP == 8 else ((), ())


def live_pairs(NP):
    live, most, passed = 0, 0, {}
    z_scatter = z_pairs(NP)[0]
    for name, *index in order_for(NP):
        live += name == "f1"
        if index and name == ("f4" if index[0] in z_scatter else "f3"):
            p = index[0]
            passed[p] = passed.get(p, 0) + (1 if index[1:] else 2)
            live -= passed[p] == 2
        most = max(most, live)
    return most


def contract_rows(left, right):
    return lax.dot_general(
        left, right, (((0,), (0,)), ((), ())), preferred_element_type=jnp.float32
    )


def drain_kernel(*refs):
    n = len(refs) // 2
    ins, outs, sem = refs[:n], refs[n:-1], refs[-1]
    copies = [pltpu.make_async_copy(a, b, sem.at[i]) for i, (a, b) in enumerate(zip(ins, outs))]
    for c in copies:
        c.start()
    for c in copies:
        c.wait()


def drain_out(*arrays):
    return pl.pallas_call(
        drain_kernel,
        out_shape=tuple(jax.ShapeDtypeStruct(a.shape, a.dtype) for a in arrays),
        in_specs=[pl.BlockSpec(memory_space=pltpu.VMEM)] * len(arrays),
        out_specs=(pl.BlockSpec(memory_space=pl.ANY),) * len(arrays),
        scratch_shapes=[pltpu.SemaphoreType.DMA((len(arrays),))],
        compiler_params=pltpu.CompilerParams(vmem_limit_bytes=4 * 1024 * 1024),
    )(*[pltpu.with_memory_space_constraint(a, pltpu.VMEM) for a in arrays])


def fused_kernel(
    Z, R, T,
    m_hbm, o_hbm, f_hbm, w_hbm, m1_hbm, m2_hbm,
    nw_ref, upd_ref, nf_ref, ns_ref, wc_ref,
    m_ref, o_ref, f_ref, w_ref, m1_ref, m2_ref, load,
    mt, own, s1, r1, s2, r2, s3, r3, rz,
    f_all, ft, yt, own_p, s1_p, r1_p, s2_p, r2_p, s3_p, r3_p, proj, q_all, q_own,
    stat, stat_all, ratio,
    t_send, t_recv, u_send, u_recv, v_send, v_recv,
    tp_send, tp_recv, up_send, up_recv, vp_send, vp_recv,
    gz_send, gz_recv, gx_send, gx_recv, gf_send,
    st_send, st_recv, cross_send, cross_recv,
):
    N = Z * R
    z, r, t = lax.axis_index("fs"), lax.axis_index("rep"), lax.axis_index("tp")
    every = (z * R + r) * T + t
    TOK, DH = m_ref.shape
    CW = o_ref.shape[1]
    FR, RK = f_ref.shape
    MR = m1_ref.shape[0]
    NP = CW // PAIR
    PART = CW // PARTS
    xn, yn, dn = r + 1 - 2 * lax.rem(r, 2), lax.rem(r + 2, R), R - 1 - r
    near = ((xn, yn), (yn, xn))
    low_half = z < 2
    twin = z + 1 - 2 * lax.rem(z, 2)
    cross = jnp.where(low_half, 2, 1)
    away = jnp.where(low_half, 2, 0)
    middle = (z == 1) | (z == 2)
    f32, bf16 = jnp.float32, jnp.bfloat16

    def device(zz, rr, tt):
        return {"fs": zz, "rep": rr, "tp": tt}

    def lanes(index, size):
        return pl.ds(pl.multiple_of(index * size, size), size)

    def other(e):
        return lax.rem(z + e, Z)

    def each_z(body):
        def step(e, carry):
            body(other(e))
            return carry

        lax.fori_loop(1, Z, step, 0)

    def fetch(src, dst, index):
        return pltpu.make_async_copy(src, dst, load.at[index])

    loads = {"f": fetch(f_hbm, f_ref, 0)}
    for i in range(DH // PAIR):
        part = pl.ds(i * PAIR, PAIR)
        loads["m", i] = fetch(m_hbm.at[:, part], m_ref.at[:, part], len(loads))
    for i in range(NP):
        part = pl.ds(i * PAIR, PAIR)
        loads["o", i] = fetch(o_hbm.at[:, part], o_ref.at[:, part], len(loads))
    for name, src, dst in (("m1", m1_hbm, m1_ref), ("m2", m2_hbm, m2_ref), ("w", w_hbm, w_ref)):
        loads[name] = fetch(src, dst, len(loads))
    for copy in loads.values():
        copy.start()

    def need(*names):
        for name in names:
            if name in loads:
                loads.pop(name).wait()

    barrier = pltpu.get_barrier_semaphore()

    def greet(zz, rr, tt):
        pl.semaphore_signal(barrier, inc=1, device_id=device(zz, rr, tt), device_id_type=MESH)

    each_z(lambda zz: greet(zz, r, t))
    greet(z, xn, t)
    greet(z, yn, t)
    greet(z, r, 1 - t)

    for i in range(DH // PAIR):
        need(("m", i))
        mt[i * PAIR : (i + 1) * PAIR, :] = m_ref[:, i * PAIR : (i + 1) * PAIR].T
    need("f")

    def move(src, dst, ss, rs, where):
        return pltpu.make_async_remote_copy(
            src_ref=src, dst_ref=dst, send_sem=ss, recv_sem=rs, device_id=where, device_id_type=MESH
        )

    class Scatter:
        def __init__(self, c, h, slot, refs, sems):
            self.c, self.h, self.slot = c, h, slot
            self.own, self.s1, self.r1, self.s2, self.r2, self.s3, self.r3 = refs
            self.ts, self.tr, self.us, self.ur, self.vs, self.vr = sems
            self.n1, self.n2 = near[h]

        def first(self, k):
            rr = self.n1 if k else dn
            c = self.c
            return move(self.s1.at[c, rr], self.r1.at[c, k], self.ts.at[c, k], self.tr.at[c, k], device(z, self.n1, t))

        def second(self):
            c = self.c
            return move(self.s2.at[c], self.r2.at[c], self.us.at[c], self.ur.at[c], device(z, self.n2, t))

        def third(self, zz, src):
            c = self.c
            return move(
                self.s3.at[c, zz], self.r3.at[c, src], self.vs.at[c, zz], self.vr.at[c, src], device(zz, r, t)
            )

        def mine(self, rr, zz):
            return self.own[self.slot, self.h, rr, zz]

        def stage2(self):
            c = self.c
            self.first(0).wait_recv()

            def add(zz, carry):
                total = self.mine(self.n2, zz) + self.r1[c, 0, zz].astype(f32)
                self.s2[c, zz] = total.astype(bf16)
                return carry

            lax.fori_loop(0, Z, add, 0)
            self.second().start()

        def stage3(self, put):
            c = self.c
            self.first(1).wait_recv()
            self.second().wait_recv()

            def total(zz):
                return self.mine(r, zz) + self.r1[c, 1, zz].astype(f32) + self.r2[c, zz].astype(f32)

            def send(zz):
                self.s3[c, zz] = total(zz).astype(bf16)
                self.third(zz, z).start()

            each_z(send)
            put(total(z))

        def last(self, get, put):
            each_z(lambda zz: self.third(zz, zz).wait_recv())
            value = get()
            for e in range(1, Z):
                value = value + self.r3[self.c, other(e)].astype(f32)
            put(value)

        def sent(self):
            self.first(0).wait_send()
            self.first(1).wait_send()
            self.second().wait_send()
            each_z(lambda zz: self.third(zz, z).wait_send())

    class Gather:
        def __init__(self, g, h, ref, cols, rows=slice(None)):
            self.g, self.ref, self.cols, self.rows = g, ref, cols, rows
            self.n1, self.n2 = near[h]

        def along(self, zz, src_z, block=None, sent=None):
            place = self.ref.at[src_z, r, self.rows, self.cols]
            return move(
                place if block is None else block, place,
                gz_send.at[self.g, zz] if sent is None else sent, gz_recv.at[self.g, src_z], device(zz, r, t),
            )

        def beside(self, k, rr):
            place = self.ref.at[:, rr, self.rows, self.cols]
            to = self.n2 if k == 0 else self.n1
            return move(place, place, gx_send.at[self.g, k], gx_recv.at[self.g, k], device(z, to, t))

        def stage1(self, block=None):
            each_z(lambda zz: self.along(zz, z, block).start())

        def spread(self):
            self.along(cross, z).start()
            self.along(twin, z).start()

        def onward(self, k):
            return self.along(twin, away + k, None, gf_send.at[self.g, k])

        def forward(self):
            @pl.when(middle)
            def _():
                for k in (0, 1):
                    self.along(twin, away + k).wait_recv()
                    self.onward(k).start()

        def gathered(self):
            self.along(twin, twin).wait_recv()

            @pl.when(jnp.logical_not(middle))
            def _():
                for k in (0, 1):
                    self.along(twin, away + k).wait_recv()

        def spread_sent(self):
            self.along(cross, z).wait_send()
            self.along(twin, z).wait_send()

            @pl.when(middle)
            def _():
                for k in (0, 1):
                    self.onward(k).wait_send()

        def stage2(self, spread=False):
            if spread:
                self.gathered()
            else:
                each_z(lambda zz: self.along(zz, zz).wait_recv())
            self.beside(0, r).start()
            self.beside(1, r).start()

        def stage3(self):
            self.beside(0, self.n2).wait_recv()
            self.beside(2, self.n2).start()

        def done(self, spread=False):
            self.beside(1, self.n1).wait_recv()
            self.beside(2, dn).wait_recv()
            if spread:
                self.spread_sent()
            else:
                each_z(lambda zz: self.along(zz, z).wait_send())
            self.beside(0, r).wait_send()
            self.beside(1, r).wait_send()
            self.beside(2, self.n2).wait_send()

    class ScatterZ(Scatter):
        def far(self, zz, src):
            c = self.c
            return move(
                self.s1.at[c, :, zz], rz.at[along_z[c], src], self.vs.at[c, zz], self.vr.at[c, src], device(zz, r, t)
            )

        def first(self, k):
            rr = self.n1 if k else dn
            c = self.c
            return move(self.s2.at[c, rr], self.r2.at[c, k], self.ts.at[c, k], self.tr.at[c, k], device(z, self.n1, t))

        def second(self):
            c = self.c
            return move(self.s3.at[c, 0], self.r3.at[c, 0], self.us.at[c], self.ur.at[c], device(z, self.n2, t))

        def stage1(self):
            each_z(lambda zz: self.far(zz, z).start())

        def stage2(self):
            each_z(lambda zz: self.far(zz, zz).wait_recv())

            def add(rr, carry):
                total = self.mine(rr, z)
                for e in range(1, Z):
                    total = total + rz[along_z[self.c], other(e), rr].astype(f32)
                self.own[self.slot, self.h, rr, z] = total
                self.s2[self.c, rr] = total.astype(bf16)
                return carry

            lax.fori_loop(0, R, add, 0)
            self.first(0).start()
            self.first(1).start()

        def stage3(self, put):
            c = self.c
            self.first(0).wait_recv()
            self.s3[c, 0] = (self.mine(self.n2, z) + self.r2[c, 0].astype(f32)).astype(bf16)
            self.second().start()

        def last(self, get, put):
            c = self.c
            self.first(1).wait_recv()
            self.second().wait_recv()
            put(self.mine(r, z) + self.r2[c, 1].astype(f32) + self.r3[c, 0].astype(f32))

        def sent(self):
            self.first(0).wait_send()
            self.first(1).wait_send()
            self.second().wait_send()
            each_z(lambda zz: self.far(zz, z).wait_send())

    class GatherZ(Gather):
        def along(self, zz, src_z, block=None, sent=None):
            place = self.ref.at[src_z, :, :, self.cols]
            return move(
                place, place, gz_send.at[self.g, zz] if sent is None else sent, gz_recv.at[self.g, src_z],
                device(zz, r, t),
            )

        def beside(self, k, rr):
            place = self.ref.at[z, rr, :, self.cols]
            to = self.n2 if k == 0 else self.n1
            return move(place, place, gx_send.at[self.g, k], gx_recv.at[self.g, k], device(z, to, t))

        def begin(self):
            self.beside(0, r).start()
            self.beside(1, r).start()

        def stage2(self, spread=True):
            self.beside(0, self.n2).wait_recv()
            self.beside(2, self.n2).start()

        def stage3(self):
            self.beside(1, self.n1).wait_recv()
            self.beside(2, dn).wait_recv()
            self.spread()

        def done(self, spread=True):
            self.gathered()
            self.spread_sent()
            self.beside(0, r).wait_send()
            self.beside(1, r).wait_send()
            self.beside(2, self.n2).wait_send()

    main_refs = (own, s1, r1, s2, r2, s3, r3)
    main_sems = (t_send, t_recv, u_send, u_recv, v_send, v_recv)
    proj_refs = (own_p, s1_p, r1_p, s2_p, r2_p, s3_p, r3_p)
    proj_sems = (tp_send, tp_recv, up_send, up_recv, vp_send, vp_recv)

    slots = {}
    z_scatter, z_gather = z_pairs(NP)
    along_z = {2 * p + h: 2 * i + h for i, p in enumerate(z_scatter) for h in (0, 1)}

    def scatter(p, h):
        kind = ScatterZ if p in z_scatter else Scatter
        return kind(2 * p + h, h, slots[p], main_refs, main_sems)

    def scatter_p(c):
        return Scatter(c, c % 2, c, proj_refs, proj_sems)

    def gather_w(p, h):
        kind = GatherZ if p in z_gather else Gather
        return kind(2 * p + h, h, wc_ref, lanes(2 * p + h, LANES))

    def gather_f(h):
        return Gather(2 * NP + h, h, f_all, pl.ds(h * (RK // 2), RK // 2), share)

    def gather_q(c):
        return Gather(2 * NP + 2 + c, c % 2, q_all, pl.ds(c * PART, PART))

    share = pl.ds(pl.multiple_of(t * (FR // T), FR // T), FR // T)
    f_all[z, r, share] = f_ref[share, :]
    pl.semaphore_wait(barrier, Z + 2)

    def product(p):
        need(("o", p))
        cols = lanes(p, PAIR)
        slot = slots[p]
        G = R * FR

        def tile(zz, carry):
            part = pl.ds(pl.multiple_of(zz * G, G), G)
            value = jnp.dot(mt[part, :], o_ref[:, cols], preferred_element_type=f32)
            for h in (0, 1):
                for rr in range(R):
                    block = value[rr * FR : (rr + 1) * FR, h * LANES : (h + 1) * LANES]
                    own[slot, h, rr, zz] = block
                    s1[2 * p + h, rr, zz] = block.astype(bf16)
            return carry

        lax.fori_loop(0, Z, tile, 0)
        if p in z_scatter:
            both(lambda h: scatter(p, h).stage1())
            return
        for k in (0, 1):
            for h in (0, 1):
                scatter(p, h).first(k).start()

    def start_factors():
        for h in (0, 1):
            gather_f(h).stage1(f_ref.at[share, pl.ds(h * (RK // 2), RK // 2)])

    def swap_factors():
        place = f_all.at[:, :, share, :]
        return move(place, place, cross_send, cross_recv, device(z, r, 1 - t))

    def finish_factors():
        both(lambda h: gather_f(h).done())
        swap_factors().start()

    def low_rank():
        swap_factors().wait()
        ft[...] = f_all[...].reshape(DH, RK).T

        def low(i, carry):
            yt[:, lanes(i, PAIR)] = jnp.dot(
                ft[...], mt[:, lanes(i, PAIR)], preferred_element_type=f32
            ).astype(bf16)
            return carry

        lax.fori_loop(0, TOK // PAIR, low, 0)

    def project(c):
        tiles = PART // PAIR
        need(*[("o", c * tiles + n) for n in range(tiles)])

        def tile(n, carry):
            value = jnp.dot(yt[...], o_ref[:, lanes(c * tiles + n, PAIR)], preferred_element_type=f32)
            cols = lanes(n, PAIR)
            for zz in range(Z):
                for rr in range(R):
                    low_row = (zz * R + rr) * MR
                    block = value[low_row : low_row + MR, :]
                    own_p[c, c % 2, rr, zz, :, cols] = block
                    s1_p[c, rr, zz, :, cols] = block.astype(bf16)
            return carry

        lax.fori_loop(0, tiles, tile, 0)
        for k in (0, 1):
            scatter_p(c).first(k).start()

    def s_copy(p, slot_of):
        q = lax.rem(every + p, N * T)
        d = q // T
        slot = slot_of(q)
        return move(
            stat, stat_all.at[slot], st_send.at[q], st_recv.at[slot],
            device(d // R, lax.rem(d, R), lax.rem(q, T)),
        )

    def fold(value):
        row = jnp.sum(value, axis=0, keepdims=True)
        total = row[:, :LANES]
        for j in range(1, CW // LANES):
            total = total + row[:, j * LANES : (j + 1) * LANES]
        return total

    def moments():
        need("m1", "m2")
        projected = proj[...]
        new_first = 0.8 * m1_ref[...] + 0.2 * projected
        new_second = 0.9 * m2_ref[...] + 0.1 * projected * projected
        nf_ref[...] = new_first
        ns_ref[...] = new_second
        dir_wide = (new_first / (jnp.sqrt(new_second) + 1e-08)).astype(bf16).astype(f32)
        proj_wide = projected.astype(bf16).astype(f32)
        stat[0:1, :] = fold(dir_wide * dir_wide)
        stat[1:2, :] = fold(proj_wide * proj_wide)
        stat_all[every] = stat[...]

        def send(p, carry):
            s_copy(p, lambda q: every).start()
            return carry

        lax.fori_loop(1, N * T, send, 0)

    def combine():
        def wait(p, carry):
            s_copy(p, lambda q: q).wait()
            return carry

        lax.fori_loop(1, N * T, wait, 0)
        totals = jnp.sum(stat_all[...], axis=0)
        dir_sum = jnp.sum(totals[0:1, :], axis=1, keepdims=True)
        proj_sum = jnp.sum(totals[1:2, :], axis=1, keepdims=True)
        scale_ratio = jnp.sqrt(dir_sum) / jnp.sqrt(proj_sum + 1e-06)
        ratio[...] = jnp.broadcast_to(scale_ratio, (8, PAIR))
        projected = proj[...]
        dir_wide = (nf_ref[...] / (jnp.sqrt(ns_ref[...]) + 1e-08)).astype(bf16).astype(f32)
        mixed = (dir_wide - scale_ratio * projected.astype(bf16).astype(f32)).astype(bf16)
        q_own[...] = mixed
        q_all[z, r] = mixed
        for c in range(PARTS):
            gather_q(c).stage1(q_own.at[:, pl.ds(c * PART, PART)])

    def put_proj(c):
        def put(value):
            proj[:, c * PART : (c + 1) * PART] = value

        return put

    def get_proj(c):
        return lambda: proj[:, c * PART : (c + 1) * PART]

    def both(action):
        for h in (0, 1):
            action(h)

    def finish_moments():
        for c in range(PARTS):
            scatter_p(c).last(get_proj(c), put_proj(c))
        moments()

    def put_grad(p, h):
        def put(value):
            upd_ref[:, lanes(2 * p + h, LANES)] = value

        return put

    def get_grad(p, h):
        return lambda: upd_ref[:, lanes(2 * p + h, LANES)]

    def update(p):
        need("w")
        cols = lanes(p, PAIR)
        mixed = q_all[:, :, :, cols].reshape(RK, PAIR)
        value = jnp.dot(f_ref[...], mixed, preferred_element_type=f32) + ratio[0:1, :] * upd_ref[:, cols]
        upd_ref[:, cols] = value
        new_weight = w_ref[:, cols] - 0.01 * value
        nw_ref[:, cols] = new_weight
        wc_ref[z, r, :, cols] = new_weight.astype(bf16)
        if p in z_gather:
            both(lambda h: gather_w(p, h).begin())
        else:
            both(lambda h: gather_w(p, h).spread())

    single = {
        "F1": start_factors,
        "F2": lambda: both(lambda h: gather_f(h).stage2()),
        "F3": lambda: both(lambda h: gather_f(h).stage3()),
        "F4": finish_factors,
        "PM": low_rank,
        "P4": finish_moments,
        "Q1": combine,
    }
    parts = {
        "P1": project,
        "P2": lambda c: scatter_p(c).stage2(),
        "P3": lambda c: scatter_p(c).stage3(put_proj(c)),
        "Q2": lambda c: gather_q(c).stage2(),
        "Q3": lambda c: gather_q(c).stage3(),
        "Q4": lambda c: gather_q(c).done(),
    }
    pairs = {"f1": product, "g1": update}
    chunks = {
        "f2": lambda p, h: scatter(p, h).stage2(),
        "f3": lambda p, h: scatter(p, h).stage3(put_grad(p, h)),
        "f4": lambda p, h: scatter(p, h).last(get_grad(p, h), put_grad(p, h)),
        "ga": lambda p, h: gather_w(p, h).forward(),
        "g2": lambda p, h: gather_w(p, h).stage2(True),
        "g3": lambda p, h: gather_w(p, h).stage3(),
        "g4": lambda p, h: gather_w(p, h).done(True),
    }
    free, issued, passed = list(range(own.shape[0])), [], {}
    for name, *index in order_for(NP):
        if name in single:
            single[name]()
        elif name in parts:
            for c in index or range(PARTS):
                parts[name](c)
        elif name in pairs:
            p = index[0]
            if name == "f1":
                slots[p] = free.pop(0)
            pairs[name](p)
        else:
            p = index[0]
            for h in index[1:] or (0, 1):
                chunks[name](p, h)
                if name == ("f4" if p in z_scatter else "f3"):
                    passed[p] = passed.get(p, 0) + 1
                    if passed[p] == 2:
                        free.append(slots[p])
                        issued.append(p)
            if name == "g3" and issued:
                p = issued.pop(0)
                both(lambda h: scatter(p, h).sent())
    for p in issued:
        both(lambda h: scatter(p, h).sent())
    for c in range(PARTS):
        scatter_p(c).sent()


def fused(Z, R, T, *args):
    mixer_out, out_grad, factors, weight, first_moment, second_moment = args
    N = Z * R
    TOK, DH = mixer_out.shape
    FR, RK = factors.shape
    MR, CW = first_moment.shape
    NC, PART = CW // LANES, CW // PARTS
    f32, bf16 = jnp.float32, jnp.bfloat16
    vmem = pl.BlockSpec(memory_space=pltpu.VMEM)
    dma = pltpu.SemaphoreType.DMA
    pair = lambda *shape: [dma(shape), dma(shape)]
    outs = pl.pallas_call(
        functools.partial(fused_kernel, Z, R, T),
        out_shape=(
            pltpu.VMEM(weight.shape, f32),
            pltpu.VMEM(weight.shape, f32),
            pltpu.VMEM(first_moment.shape, f32),
            pltpu.VMEM(first_moment.shape, f32),
            pltpu.VMEM((Z, R, FR, CW), bf16),
        ),
        in_specs=[pl.BlockSpec(memory_space=pltpu.HBM)] * 6,
        out_specs=(vmem,) * 5,
        scratch_shapes=[
            *[pltpu.VMEM(a.shape, a.dtype) for a in args],
            dma((DH // PAIR + CW // PAIR + 4,)),
            pltpu.VMEM((DH, TOK), bf16),
            pltpu.VMEM((live_pairs(CW // PAIR), 2, R, Z, FR, LANES), f32),
            pltpu.VMEM((NC, R, Z, FR, LANES), bf16),
            pltpu.VMEM((NC, 2, Z, FR, LANES), bf16),
            pltpu.VMEM((NC, max(Z, R), FR, LANES), bf16),
            pltpu.VMEM((NC, max(Z, R), FR, LANES), bf16),
            pltpu.VMEM((NC, Z, FR, LANES), bf16),
            pltpu.VMEM((NC, Z, FR, LANES), bf16),
            pltpu.VMEM((max(1, 2 * len(z_pairs(CW // PAIR)[0])), Z, R, FR, LANES), bf16),
            pltpu.VMEM((Z, R, FR, RK), bf16),
            pltpu.VMEM((RK, DH), bf16),
            pltpu.VMEM((RK, TOK), bf16),
            pltpu.VMEM((PARTS, 2, R, Z, MR, PART), f32),
            pltpu.VMEM((PARTS, R, Z, MR, PART), bf16),
            pltpu.VMEM((PARTS, 2, Z, MR, PART), bf16),
            pltpu.VMEM((PARTS, Z, MR, PART), bf16),
            pltpu.VMEM((PARTS, Z, MR, PART), bf16),
            pltpu.VMEM((PARTS, Z, MR, PART), bf16),
            pltpu.VMEM((PARTS, Z, MR, PART), bf16),
            pltpu.VMEM((MR, CW), f32),
            pltpu.VMEM((Z, R, MR, CW), bf16),
            pltpu.VMEM((MR, CW), bf16),
            pltpu.VMEM((2, LANES), f32),
            pltpu.VMEM((N * T, 2, LANES), f32),
            pltpu.VMEM((8, PAIR), f32),
            *pair(NC, 2), *pair(NC), *pair(NC, Z),
            *pair(PARTS, 2), *pair(PARTS), *pair(PARTS, Z),
            *pair(NC + 2 + PARTS, Z), *pair(NC + 2 + PARTS, 3), dma((NC + 2 + PARTS, 2)),
            *pair(N * T), dma, dma,
        ],
        compiler_params=pltpu.CompilerParams(
            collective_id=0, has_side_effects=True, vmem_limit_bytes=VMEM_GRANT
        ),
    )(*args)
    new_weight, update, new_first, new_second, copy = drain_out(*outs)
    return new_weight, update, new_first, new_second, copy.reshape(DH, CW)


def plain(mixer_out, out_grad, factors, weight, first_moment, second_moment):
    columns = mixer_out
    gradient = lax.psum_scatter(
        contract_rows(columns, out_grad), ("fs", "rep"), scatter_dimension=0, tiled=True
    )
    grad_low = gradient.astype(jnp.bfloat16)
    columns = factors
    projected = lax.psum_scatter(
        contract_rows(columns, grad_low), ("fs", "rep"), scatter_dimension=0, tiled=True
    )
    new_first = 0.8 * first_moment + 0.2 * projected
    new_second = 0.9 * second_moment + 0.1 * projected * projected
    direction = new_first / (jnp.sqrt(new_second) + 1e-08)
    dir_low = direction.astype(jnp.bfloat16)
    proj_low = projected.astype(jnp.bfloat16)
    dir_whole, proj_whole = (
        lax.all_gather(dir_low, ("fs", "rep"), axis=0, tiled=True),
        lax.all_gather(proj_low, ("fs", "rep"), axis=0, tiled=True),
    )
    dir_wide = dir_low.astype(jnp.float32)
    proj_wide = proj_low.astype(jnp.float32)
    dir_sum, proj_sum = lax.psum(
        (jnp.sum(dir_wide * dir_wide), jnp.sum(proj_wide * proj_wide)), ("fs", "rep", "tp")
    )
    back_dir = jnp.dot(factors, dir_whole, preferred_element_type=jnp.float32)
    back_proj = jnp.dot(factors, proj_whole, preferred_element_type=jnp.float32)
    scale_ratio = jnp.sqrt(dir_sum) / jnp.sqrt(proj_sum + 1e-06)
    update = back_dir + scale_ratio * (gradient - back_proj)
    new_weight = weight - 0.01 * update
    weight_copy = lax.all_gather(new_weight.astype(jnp.bfloat16), ("fs", "rep"), axis=0, tiled=True)
    return (new_weight, update, new_first, new_second, weight_copy)


def solution(mesh):
    Z, R, T = mesh.shape["fs"], mesh.shape["rep"], mesh.shape["tp"]

    def per_device(*args):
        mixer_out, out_grad, factors, weight, first_moment, second_moment = args
        fits = (
            out_grad.shape[1] % (PARTS * PAIR) == 0
            and mixer_out.shape[0] % PAIR == 0
            and mixer_out.shape[1] % PAIR == 0
            and weight.shape[0] % 16 == 0
            and first_moment.shape[0] % 16 == 0
            and factors.shape[1] == PAIR
            and weight.shape[0] % (16 * T) == 0
            and R == 4
            and T == 2
            and Z == R
            and Z > 1
        )
        return fused(Z, R, T, *args) if fits else plain(*args)

    in_specs = (
        P(("fs", "rep"), None),
        P(("fs", "rep"), "tp"),
        P(("fs", "rep"), None),
        P(("fs", "rep"), "tp"),
        P(("fs", "rep"), "tp"),
        P(("fs", "rep"), "tp"),
    )
    out_specs = (
        P(("fs", "rep"), "tp"),
        P(("fs", "rep"), "tp"),
        P(("fs", "rep"), "tp"),
        P(("fs", "rep"), "tp"),
        P(None, "tp"),
    )
    return jax.shard_map(
        per_device, mesh=mesh, in_specs=in_specs, out_specs=out_specs, check_vma=False
    )
```

```python
import functools

import jax
import jax.numpy as jnp
from jax import lax
from jax.experimental import pallas as pl
from jax.experimental.pallas import tpu as pltpu
from jax.sharding import PartitionSpec as P

MESH = pl.DeviceIdType.MESH
LANES = 128
PAIR = 2 * LANES
PARTS = 4
VMEM_GRANT = 52 * 1024 * 1024


ORDER = (
    "F1 f1.4 f1.1 F2",
    "f1.0 F3 f2.4.1 f1.6",
    "F4 f2.0.1 f2.0.0 f2.4.0",
    "f3.4.1 PM P1.3 P1.2",
    "P1.1 P1.0 f3.0.1 f3.0.0",
    "P2.3 P2.2 f1.2 f2.6.1",
    "P2.0 P3.2 P3.3 f2.6.0",
    "f3.4.0 f2.2.0 P2.1 f1.3",
    "f2.1.1 P3.0 P3.1 f2.1.0",
    "f3.6.1 f2.2.1 f3.2.0 f3.6.0",
    "f2.3.1 f2.3.0 P4 f1.7",
    "f3.3.0 f3.2.1 f1.5 Q1",
    "f4.3.0 f2.7.0 f3.1.1 f2.7.1",
    "f3.3.1 f4.4.1 f4.2.1 f4.6.1",
    "Q2.0 f3.1.0 f4.1.1 f4.2.0",
    "f4.4.0 Q2.1 f2.5.0 f3.7.1",
    "Q3.0 f2.5.1 f4.6.0 Q2.3",
    "f3.7.0 f4.0.1 Q3.1 f4.1.0",
    "Q4.0 g1.1 f4.7.1 f4.3.1",
    "Q2.2 f3.5.1 Q4.1 Q3.3",
    "g1.2 f4.0.0 g1.3 ga.1",
    "Q3.2 f4.7.0 Q4.3 g1.6",
    "g2.3.0 g2.1.1 f3.5.0 ga.2",
    "g1.0 g2.1.0 Q4.2 g1.4",
    "g2.3.1 ga.6 f4.5.1 g2.2.1",
    "g1.7 g2.2.0 f4.5.0 g1.5",
    "g2.0.0 g3.3.0 g2.0.1 g2.6.1",
    "ga.4 g3.2.1 g3.1.1 ga.7",
    "g3.1.0 g2.6.0 g2.4.0 g3.0.1",
    "ga.5 g3.6.1 g3.2.0 g2.7.0",
    "g3.0.0 g2.5.0 g2.5.1 g2.7.1",
    "g4.1.0 g3.3.1 g2.4.1 g3.6.0",
    "ga.3.0 ga.0.1 g4.2.1 ga.0.0",
    "g4.1.1 g4.3.0 g3.5.1 g3.4.0",
    "g3.7.1 ga.3.1 g3.4.1 g3.5.0",
    "g4.6.0 g3.7.0 g4.2.0 g4.6.1",
    "g4.5.1 g4.0.0 g4.4.0 g4.0.1",
    "g4.7.1 g4.5.0 g4.3.1 g4.7.0",
    "g4.4.1",
)
Z_SCATTER = (1,)
Z_GATHER = (0, 3)


def token(text):
    name, *index = text.split(".")
    return (name, *map(int, index))


def order_for(NP):
    if NP == 8:
        return [token(a) for line in ORDER for a in line.split()]
    events = {
        1: "F2", 2: "F3", 3: "F4 PM P1", 4: "P2", 5: "P3",
        6: "P4", 7: "Q1", 8: "Q2", 9: "Q3", 10: "Q4",
    }
    lags = {"f1": 0, "f2": 1, "f3": 2, "f4": 3, "g1": 10, "ga": 11, "g2": 11, "g3": 12, "g4": 13}
    order = [("F1",)]
    for i in range(max(NP, 1) + 14):
        for a in events.get(i, "").split():
            order.append(token(a))
        order += [(name, i - lag) for name, lag in lags.items() if 0 <= i - lag < NP]
    return order


def z_pairs(NP):
    return (Z_SCATTER, Z_GATHER) if NP == 8 else ((), ())


def live_pairs(NP):
    live, most, passed = 0, 0, {}
    z_scatter = z_pairs(NP)[0]
    for name, *index in order_for(NP):
        live += name == "f1"
        if index and name == ("f4" if index[0] in z_scatter else "f3"):
            p = index[0]
            passed[p] = passed.get(p, 0) + (1 if index[1:] else 2)
            live -= passed[p] == 2
        most = max(most, live)
    return most


def contract_rows(left, right):
    return lax.dot_general(
        left, right, (((0,), (0,)), ((), ())), preferred_element_type=jnp.float32
    )


def drain_kernel(*refs):
    n = len(refs) // 2
    ins, outs, sem = refs[:n], refs[n:-1], refs[-1]
    copies = [pltpu.make_async_copy(a, b, sem.at[i]) for i, (a, b) in enumerate(zip(ins, outs))]
    for c in copies:
        c.start()
    for c in copies:
        c.wait()


def drain_out(*arrays):
    return pl.pallas_call(
        drain_kernel,
        out_shape=tuple(jax.ShapeDtypeStruct(a.shape, a.dtype) for a in arrays),
        in_specs=[pl.BlockSpec(memory_space=pltpu.VMEM)] * len(arrays),
        out_specs=(pl.BlockSpec(memory_space=pl.ANY),) * len(arrays),
        scratch_shapes=[pltpu.SemaphoreType.DMA((len(arrays),))],
        compiler_params=pltpu.CompilerParams(vmem_limit_bytes=4 * 1024 * 1024),
    )(*[pltpu.with_memory_space_constraint(a, pltpu.VMEM) for a in arrays])


def fused_kernel(
    Z, R, T,
    m_hbm, o_hbm, f_hbm, w_hbm, m1_hbm, m2_hbm,
    nw_ref, upd_ref, nf_ref, ns_ref, wc_ref,
    m_ref, o_ref, f_ref, w_ref, m1_ref, m2_ref, load,
    mt, own, s1, r1, s2, r2, s3, r3, rz,
    f_all, ft, yt, own_p, s1_p, r1_p, s2_p, r2_p, s3_p, r3_p, proj, q_all, q_own,
    stat, stat_all, ratio,
    t_send, t_recv, u_send, u_recv, v_send, v_recv,
    tp_send, tp_recv, up_send, up_recv, vp_send, vp_recv,
    gz_send, gz_recv, gx_send, gx_recv, gf_send,
    st_send, st_recv, cross_send, cross_recv,
):
    N = Z * R
    z, r, t = lax.axis_index("fs"), lax.axis_index("rep"), lax.axis_index("tp")
    every = (z * R + r) * T + t
    TOK, DH = m_ref.shape
    CW = o_ref.shape[1]
    FR, RK = f_ref.shape
    MR = m1_ref.shape[0]
    NP = CW // PAIR
    PART = CW // PARTS
    xn, yn, dn = r + 1 - 2 * lax.rem(r, 2), lax.rem(r + 2, R), R - 1 - r
    near = ((xn, yn), (yn, xn))
    low_half = z < 2
    twin = z + 1 - 2 * lax.rem(z, 2)
    cross = jnp.where(low_half, 2, 1)
    away = jnp.where(low_half, 2, 0)
    middle = (z == 1) | (z == 2)
    f32, bf16 = jnp.float32, jnp.bfloat16

    def device(zz, rr, tt):
        return {"fs": zz, "rep": rr, "tp": tt}

    def lanes(index, size):
        return pl.ds(pl.multiple_of(index * size, size), size)

    def other(e):
        return lax.rem(z + e, Z)

    def each_z(body):
        def step(e, carry):
            body(other(e))
            return carry

        lax.fori_loop(1, Z, step, 0)

    def fetch(src, dst, index):
        return pltpu.make_async_copy(src, dst, load.at[index])

    loads = {"f": fetch(f_hbm, f_ref, 0)}
    for i in range(DH // PAIR):
        part = pl.ds(i * PAIR, PAIR)
        loads["m", i] = fetch(m_hbm.at[:, part], m_ref.at[:, part], len(loads))
    for i in range(NP):
        part = pl.ds(i * PAIR, PAIR)
        loads["o", i] = fetch(o_hbm.at[:, part], o_ref.at[:, part], len(loads))
    for name, src, dst in (("m1", m1_hbm, m1_ref), ("m2", m2_hbm, m2_ref), ("w", w_hbm, w_ref)):
        loads[name] = fetch(src, dst, len(loads))
    for copy in loads.values():
        copy.start()

    def need(*names):
        for name in names:
            if name in loads:
                loads.pop(name).wait()

    barrier = pltpu.get_barrier_semaphore()

    def greet(zz, rr, tt):
        pl.semaphore_signal(barrier, inc=1, device_id=device(zz, rr, tt), device_id_type=MESH)

    each_z(lambda zz: greet(zz, r, t))
    greet(z, xn, t)
    greet(z, yn, t)
    greet(z, r, 1 - t)

    for i in range(DH // PAIR):
        need(("m", i))
        mt[i * PAIR : (i + 1) * PAIR, :] = m_ref[:, i * PAIR : (i + 1) * PAIR].T
    need("f")

    def move(src, dst, ss, rs, where):
        return pltpu.make_async_remote_copy(
            src_ref=src, dst_ref=dst, send_sem=ss, recv_sem=rs, device_id=where, device_id_type=MESH
        )

    class Scatter:
        def __init__(self, c, h, slot, refs, sems):
            self.c, self.h, self.slot = c, h, slot
            self.own, self.s1, self.r1, self.s2, self.r2, self.s3, self.r3 = refs
            self.ts, self.tr, self.us, self.ur, self.vs, self.vr = sems
            self.n1, self.n2 = near[h]

        def first(self, k):
            rr = self.n1 if k else dn
            c = self.c
            return move(self.s1.at[c, rr], self.r1.at[c, k], self.ts.at[c], self.tr.at[c, k], device(z, self.n1, t))

        def second(self):
            c = self.c
            return move(self.s2.at[c], self.r2.at[c], self.us.at[c], self.ur.at[c], device(z, self.n2, t))

        def third(self, zz, src):
            c = self.c
            return move(
                self.s3.at[c, zz], self.r3.at[c, src], self.vs.at[c], self.vr.at[c], device(zz, r, t)
            )

        def thirds(self):
            every_block = self.r3.at[self.c, pl.ds(0, Z - 1)]
            return move(every_block, every_block, self.vs.at[self.c], self.vr.at[self.c], device(other(1), r, t))

        def firsts(self):
            return move(
                self.r1.at[self.c], self.r1.at[self.c], self.ts.at[self.c], self.tr.at[self.c, 0],
                device(z, self.n1, t),
            )

        def mine(self, rr, zz):
            return self.own[self.slot, self.h, rr, zz]

        def stage2(self):
            c = self.c
            self.first(0).wait_recv()

            def add(zz, carry):
                total = self.mine(self.n2, zz) + self.r1[c, 0, zz].astype(f32)
                self.s2[c, zz] = total.astype(bf16)
                return carry

            lax.fori_loop(0, Z, add, 0)
            self.second().start()

        def stage3(self, put):
            c = self.c
            self.first(1).wait_recv()
            self.second().wait_recv()

            def total(zz):
                return self.mine(r, zz) + self.r1[c, 1, zz].astype(f32) + self.r2[c, zz].astype(f32)

            def send(zz):
                self.s3[c, zz] = total(zz).astype(bf16)
                self.third(zz, z).start()

            each_z(send)
            put(total(z))

        def last(self, get, put):
            self.thirds().wait_recv()
            value = get()
            for e in range(1, Z):
                value = value + self.r3[self.c, other(e)].astype(f32)
            put(value)

        def sent(self):
            self.firsts().wait_send()
            self.second().wait_send()
            self.thirds().wait_send()

    class Gather:
        def __init__(self, g, h, ref, cols, rows=slice(None)):
            self.g, self.ref, self.cols, self.rows = g, ref, cols, rows
            self.n1, self.n2 = near[h]

        def along(self, zz, src_z, block=None, sent=None):
            place = self.ref.at[src_z, r, self.rows, self.cols]
            return move(
                place if block is None else block, place,
                gz_send.at[self.g] if sent is None else sent, gz_recv.at[self.g, src_z], device(zz, r, t),
            )

        def beside(self, k, rr):
            place = self.ref.at[:, rr, self.rows, self.cols]
            to = self.n2 if k == 0 else self.n1
            return move(place, place, gx_send.at[self.g], gx_recv.at[self.g, k], device(z, to, t))

        def stage1(self, block=None):
            each_z(lambda zz: self.along(zz, z, block).start())

        def spread(self):
            self.along(cross, z).start()
            self.along(twin, z).start()

        def onward(self, k):
            return self.along(twin, away + k, None, gf_send.at[self.g])

        def forward(self):
            @pl.when(middle)
            def _():
                for k in (0, 1):
                    self.along(twin, away + k).wait_recv()
                    self.onward(k).start()

        def gathered(self):
            self.along(twin, twin).wait_recv()

            @pl.when(jnp.logical_not(middle))
            def _():
                for k in (0, 1):
                    self.along(twin, away + k).wait_recv()

        def along_sent(self, blocks, sem):
            place = self.ref.at[pl.ds(0, blocks), r, self.rows, self.cols]
            move(place, place, sem, gz_recv.at[self.g, twin], device(twin, r, t)).wait_send()

        def beside_sent(self):
            place = self.ref.at[:, pl.ds(0, 3), self.rows, self.cols]
            move(place, place, gx_send.at[self.g], gx_recv.at[self.g, 0], device(z, self.n1, t)).wait_send()

        def spread_sent(self):
            self.along_sent(2, gz_send.at[self.g])

            @pl.when(middle)
            def _():
                self.along_sent(2, gf_send.at[self.g])

        def stage2(self, spread=False):
            if spread:
                self.gathered()
            else:
                each_z(lambda zz: self.along(zz, zz).wait_recv())
            self.beside(0, r).start()
            self.beside(1, r).start()

        def stage3(self):
            self.beside(0, self.n2).wait_recv()
            self.beside(2, self.n2).start()

        def done(self, spread=False):
            self.beside(1, self.n1).wait_recv()
            self.beside(2, dn).wait_recv()
            if spread:
                self.spread_sent()
            else:
                self.along_sent(Z - 1, gz_send.at[self.g])
            self.beside_sent()

    class ScatterZ(Scatter):
        def far(self, zz, src):
            c = self.c
            return move(
                self.s1.at[c, :, zz], rz.at[along_z[c], src], self.vs.at[c], self.vr.at[c], device(zz, r, t)
            )

        def thirds(self):
            every_block = rz.at[along_z[self.c], pl.ds(0, Z - 1)]
            return move(every_block, every_block, self.vs.at[self.c], self.vr.at[self.c], device(other(1), r, t))

        def firsts(self):
            both_blocks = self.r2.at[self.c, pl.ds(0, 2)]
            return move(both_blocks, both_blocks, self.ts.at[self.c], self.tr.at[self.c, 0], device(z, self.n1, t))

        def first(self, k):
            rr = self.n1 if k else dn
            c = self.c
            return move(self.s2.at[c, rr], self.r2.at[c, k], self.ts.at[c], self.tr.at[c, k], device(z, self.n1, t))

        def second(self):
            c = self.c
            return move(self.s3.at[c, 0], self.r3.at[c, 0], self.us.at[c], self.ur.at[c], device(z, self.n2, t))

        def stage1(self):
            each_z(lambda zz: self.far(zz, z).start())

        def stage2(self):
            self.thirds().wait_recv()

            def add(rr, carry):
                total = self.mine(rr, z)
                for e in range(1, Z):
                    total = total + rz[along_z[self.c], other(e), rr].astype(f32)
                self.own[self.slot, self.h, rr, z] = total
                self.s2[self.c, rr] = total.astype(bf16)
                return carry

            lax.fori_loop(0, R, add, 0)
            self.first(0).start()
            self.first(1).start()

        def stage3(self, put):
            c = self.c
            self.first(0).wait_recv()
            self.s3[c, 0] = (self.mine(self.n2, z) + self.r2[c, 0].astype(f32)).astype(bf16)
            self.second().start()

        def last(self, get, put):
            c = self.c
            self.first(1).wait_recv()
            self.second().wait_recv()
            put(self.mine(r, z) + self.r2[c, 1].astype(f32) + self.r3[c, 0].astype(f32))

        def sent(self):
            self.firsts().wait_send()
            self.second().wait_send()
            self.thirds().wait_send()

    class GatherZ(Gather):
        def along(self, zz, src_z, block=None, sent=None):
            place = self.ref.at[src_z, :, :, self.cols]
            return move(
                place, place, gz_send.at[self.g] if sent is None else sent, gz_recv.at[self.g, src_z],
                device(zz, r, t),
            )

        def along_sent(self, blocks, sem):
            place = self.ref.at[pl.ds(0, blocks), :, :, self.cols]
            move(place, place, sem, gz_recv.at[self.g, twin], device(twin, r, t)).wait_send()

        def beside_sent(self):
            place = self.ref.at[z, pl.ds(0, 3), :, self.cols]
            move(place, place, gx_send.at[self.g], gx_recv.at[self.g, 0], device(z, self.n1, t)).wait_send()

        def beside(self, k, rr):
            place = self.ref.at[z, rr, :, self.cols]
            to = self.n2 if k == 0 else self.n1
            return move(place, place, gx_send.at[self.g], gx_recv.at[self.g, k], device(z, to, t))

        def begin(self):
            self.beside(0, r).start()
            self.beside(1, r).start()

        def stage2(self, spread=True):
            self.beside(0, self.n2).wait_recv()
            self.beside(2, self.n2).start()

        def stage3(self):
            self.beside(1, self.n1).wait_recv()
            self.beside(2, dn).wait_recv()
            self.spread()

        def done(self, spread=True):
            self.gathered()
            self.spread_sent()
            self.beside_sent()

    main_refs = (own, s1, r1, s2, r2, s3, r3)
    main_sems = (t_send, t_recv, u_send, u_recv, v_send, v_recv)
    proj_refs = (own_p, s1_p, r1_p, s2_p, r2_p, s3_p, r3_p)
    proj_sems = (tp_send, tp_recv, up_send, up_recv, vp_send, vp_recv)

    slots = {}
    z_scatter, z_gather = z_pairs(NP)
    along_z = {2 * p + h: 2 * i + h for i, p in enumerate(z_scatter) for h in (0, 1)}

    def scatter(p, h):
        kind = ScatterZ if p in z_scatter else Scatter
        return kind(2 * p + h, h, slots[p], main_refs, main_sems)

    def scatter_p(c):
        return Scatter(c, c % 2, c, proj_refs, proj_sems)

    def gather_w(p, h):
        kind = GatherZ if p in z_gather else Gather
        return kind(2 * p + h, h, wc_ref, lanes(2 * p + h, LANES))

    def gather_f(h):
        return Gather(2 * NP + h, h, f_all, pl.ds(h * (RK // 2), RK // 2), share)

    def gather_q(c):
        return Gather(2 * NP + 2 + c, c % 2, q_all, pl.ds(c * PART, PART))

    share = pl.ds(pl.multiple_of(t * (FR // T), FR // T), FR // T)
    f_all[z, r, share] = f_ref[share, :]
    pl.semaphore_wait(barrier, Z + 2)

    def product(p):
        need(("o", p))
        cols = lanes(p, PAIR)
        slot = slots[p]
        G = R * FR

        def tile(zz, carry):
            part = pl.ds(pl.multiple_of(zz * G, G), G)
            value = jnp.dot(mt[part, :], o_ref[:, cols], preferred_element_type=f32)
            for h in (0, 1):
                for rr in range(R):
                    block = value[rr * FR : (rr + 1) * FR, h * LANES : (h + 1) * LANES]
                    own[slot, h, rr, zz] = block
                    s1[2 * p + h, rr, zz] = block.astype(bf16)
            return carry

        lax.fori_loop(0, Z, tile, 0)
        if p in z_scatter:
            both(lambda h: scatter(p, h).stage1())
            return
        for k in (0, 1):
            for h in (0, 1):
                scatter(p, h).first(k).start()

    def start_factors():
        for h in (0, 1):
            gather_f(h).stage1(f_ref.at[share, pl.ds(h * (RK // 2), RK // 2)])

    def swap_factors():
        place = f_all.at[:, :, share, :]
        return move(place, place, cross_send, cross_recv, device(z, r, 1 - t))

    def finish_factors():
        both(lambda h: gather_f(h).done())
        swap_factors().start()

    def low_rank():
        swap_factors().wait()
        ft[...] = f_all[...].reshape(DH, RK).T

        def low(i, carry):
            yt[:, lanes(i, PAIR)] = jnp.dot(
                ft[...], mt[:, lanes(i, PAIR)], preferred_element_type=f32
            ).astype(bf16)
            return carry

        lax.fori_loop(0, TOK // PAIR, low, 0)

    def project(c):
        tiles = PART // PAIR
        need(*[("o", c * tiles + n) for n in range(tiles)])

        def tile(n, carry):
            value = jnp.dot(yt[...], o_ref[:, lanes(c * tiles + n, PAIR)], preferred_element_type=f32)
            cols = lanes(n, PAIR)
            for zz in range(Z):
                for rr in range(R):
                    low_row = (zz * R + rr) * MR
                    block = value[low_row : low_row + MR, :]
                    own_p[c, c % 2, rr, zz, :, cols] = block
                    s1_p[c, rr, zz, :, cols] = block.astype(bf16)
            return carry

        lax.fori_loop(0, tiles, tile, 0)
        for k in (0, 1):
            scatter_p(c).first(k).start()

    def s_copy(p):
        q = lax.rem(every + p, N * T)
        d = q // T
        return move(
            stat, stat_all.at[every], st_send, st_recv, device(d // R, lax.rem(d, R), lax.rem(q, T))
        )

    def fold(value):
        row = jnp.sum(value, axis=0, keepdims=True)
        total = row[:, :LANES]
        for j in range(1, CW // LANES):
            total = total + row[:, j * LANES : (j + 1) * LANES]
        return total

    def moments():
        need("m1", "m2")
        projected = proj[...]
        new_first = 0.8 * m1_ref[...] + 0.2 * projected
        new_second = 0.9 * m2_ref[...] + 0.1 * projected * projected
        nf_ref[...] = new_first
        ns_ref[...] = new_second
        dir_wide = (new_first / (jnp.sqrt(new_second) + 1e-08)).astype(bf16).astype(f32)
        proj_wide = projected.astype(bf16).astype(f32)
        stat[0:1, :] = fold(dir_wide * dir_wide)
        stat[1:2, :] = fold(proj_wide * proj_wide)
        stat_all[every] = stat[...]

        def send(p, carry):
            s_copy(p).start()
            return carry

        lax.fori_loop(1, N * T, send, 0)

    def combine():
        arrivals = stat_all.at[pl.ds(0, N * T - 1)]
        move(arrivals, arrivals, st_send, st_recv, device(z, r, 1 - t)).wait()
        totals = jnp.sum(stat_all[...], axis=0)
        dir_sum = jnp.sum(totals[0:1, :], axis=1, keepdims=True)
        proj_sum = jnp.sum(totals[1:2, :], axis=1, keepdims=True)
        scale_ratio = jnp.sqrt(dir_sum) / jnp.sqrt(proj_sum + 1e-06)
        ratio[...] = jnp.broadcast_to(scale_ratio, (8, PAIR))
        projected = proj[...]
        dir_wide = (nf_ref[...] / (jnp.sqrt(ns_ref[...]) + 1e-08)).astype(bf16).astype(f32)
        mixed = (dir_wide - scale_ratio * projected.astype(bf16).astype(f32)).astype(bf16)
        q_own[...] = mixed
        q_all[z, r] = mixed
        for c in range(PARTS):
            gather_q(c).stage1(q_own.at[:, pl.ds(c * PART, PART)])

    def put_proj(c):
        def put(value):
            proj[:, c * PART : (c + 1) * PART] = value

        return put

    def get_proj(c):
        return lambda: proj[:, c * PART : (c + 1) * PART]

    def both(action):
        for h in (0, 1):
            action(h)

    def finish_moments():
        for c in range(PARTS):
            scatter_p(c).last(get_proj(c), put_proj(c))
        moments()

    def put_grad(p, h):
        def put(value):
            upd_ref[:, lanes(2 * p + h, LANES)] = value

        return put

    def get_grad(p, h):
        return lambda: upd_ref[:, lanes(2 * p + h, LANES)]

    def update(p):
        need("w")
        cols = lanes(p, PAIR)
        mixed = q_all[:, :, :, cols].reshape(RK, PAIR)
        value = jnp.dot(f_ref[...], mixed, preferred_element_type=f32) + ratio[0:1, :] * upd_ref[:, cols]
        upd_ref[:, cols] = value
        new_weight = w_ref[:, cols] - 0.01 * value
        nw_ref[:, cols] = new_weight
        wc_ref[z, r, :, cols] = new_weight.astype(bf16)
        if p in z_gather:
            both(lambda h: gather_w(p, h).begin())
        else:
            both(lambda h: gather_w(p, h).spread())

    single = {
        "F1": start_factors,
        "F2": lambda: both(lambda h: gather_f(h).stage2()),
        "F3": lambda: both(lambda h: gather_f(h).stage3()),
        "F4": finish_factors,
        "PM": low_rank,
        "P4": finish_moments,
        "Q1": combine,
    }
    parts = {
        "P1": project,
        "P2": lambda c: scatter_p(c).stage2(),
        "P3": lambda c: scatter_p(c).stage3(put_proj(c)),
        "Q2": lambda c: gather_q(c).stage2(),
        "Q3": lambda c: gather_q(c).stage3(),
        "Q4": lambda c: gather_q(c).done(),
    }
    pairs = {"f1": product, "g1": update}
    chunks = {
        "f2": lambda p, h: scatter(p, h).stage2(),
        "f3": lambda p, h: scatter(p, h).stage3(put_grad(p, h)),
        "f4": lambda p, h: scatter(p, h).last(get_grad(p, h), put_grad(p, h)),
        "ga": lambda p, h: gather_w(p, h).forward(),
        "g2": lambda p, h: gather_w(p, h).stage2(True),
        "g3": lambda p, h: gather_w(p, h).stage3(),
        "g4": lambda p, h: gather_w(p, h).done(True),
    }
    free, issued, passed = list(range(own.shape[0])), [], {}
    for name, *index in order_for(NP):
        if name in single:
            single[name]()
        elif name in parts:
            for c in index or range(PARTS):
                parts[name](c)
        elif name in pairs:
            p = index[0]
            if name == "f1":
                slots[p] = free.pop(0)
            pairs[name](p)
        else:
            p = index[0]
            for h in index[1:] or (0, 1):
                chunks[name](p, h)
                if name == ("f4" if p in z_scatter else "f3"):
                    passed[p] = passed.get(p, 0) + 1
                    if passed[p] == 2:
                        free.append(slots[p])
                        issued.append(p)
            if name == "g3" and issued:
                p = issued.pop(0)
                both(lambda h: scatter(p, h).sent())
    for p in issued:
        both(lambda h: scatter(p, h).sent())
    for c in range(PARTS):
        scatter_p(c).sent()


def fused(Z, R, T, *args):
    mixer_out, out_grad, factors, weight, first_moment, second_moment = args
    N = Z * R
    TOK, DH = mixer_out.shape
    FR, RK = factors.shape
    MR, CW = first_moment.shape
    NC, PART = CW // LANES, CW // PARTS
    GC = NC + 2 + PARTS
    f32, bf16 = jnp.float32, jnp.bfloat16
    vmem = pl.BlockSpec(memory_space=pltpu.VMEM)
    dma = pltpu.SemaphoreType.DMA
    pair = lambda *shape: [dma(shape), dma(shape)]
    outs = pl.pallas_call(
        functools.partial(fused_kernel, Z, R, T),
        out_shape=(
            pltpu.VMEM(weight.shape, f32),
            pltpu.VMEM(weight.shape, f32),
            pltpu.VMEM(first_moment.shape, f32),
            pltpu.VMEM(first_moment.shape, f32),
            pltpu.VMEM((Z, R, FR, CW), bf16),
        ),
        in_specs=[pl.BlockSpec(memory_space=pltpu.HBM)] * 6,
        out_specs=(vmem,) * 5,
        scratch_shapes=[
            *[pltpu.VMEM(a.shape, a.dtype) for a in args],
            dma((DH // PAIR + CW // PAIR + 4,)),
            pltpu.VMEM((DH, TOK), bf16),
            pltpu.VMEM((live_pairs(CW // PAIR), 2, R, Z, FR, LANES), f32),
            pltpu.VMEM((NC, R, Z, FR, LANES), bf16),
            pltpu.VMEM((NC, 2, Z, FR, LANES), bf16),
            pltpu.VMEM((NC, max(Z, R), FR, LANES), bf16),
            pltpu.VMEM((NC, max(Z, R), FR, LANES), bf16),
            pltpu.VMEM((NC, Z, FR, LANES), bf16),
            pltpu.VMEM((NC, Z, FR, LANES), bf16),
            pltpu.VMEM((max(1, 2 * len(z_pairs(CW // PAIR)[0])), Z, R, FR, LANES), bf16),
            pltpu.VMEM((Z, R, FR, RK), bf16),
            pltpu.VMEM((RK, DH), bf16),
            pltpu.VMEM((RK, TOK), bf16),
            pltpu.VMEM((PARTS, 2, R, Z, MR, PART), f32),
            pltpu.VMEM((PARTS, R, Z, MR, PART), bf16),
            pltpu.VMEM((PARTS, 2, Z, MR, PART), bf16),
            pltpu.VMEM((PARTS, Z, MR, PART), bf16),
            pltpu.VMEM((PARTS, Z, MR, PART), bf16),
            pltpu.VMEM((PARTS, Z, MR, PART), bf16),
            pltpu.VMEM((PARTS, Z, MR, PART), bf16),
            pltpu.VMEM((MR, CW), f32),
            pltpu.VMEM((Z, R, MR, CW), bf16),
            pltpu.VMEM((MR, CW), bf16),
            pltpu.VMEM((2, LANES), f32),
            pltpu.VMEM((N * T, 2, LANES), f32),
            pltpu.VMEM((8, PAIR), f32),
            dma((NC,)), dma((NC, 2)), *pair(NC), *pair(NC),
            dma((PARTS,)), dma((PARTS, 2)), *pair(PARTS), *pair(PARTS),
            dma((GC,)), dma((GC, Z)), dma((GC,)), dma((GC, 3)), dma((GC,)),
            dma, dma, dma, dma,
        ],
        compiler_params=pltpu.CompilerParams(
            collective_id=0, has_side_effects=True, vmem_limit_bytes=VMEM_GRANT
        ),
    )(*args)
    new_weight, update, new_first, new_second, copy = drain_out(*outs)
    return new_weight, update, new_first, new_second, copy.reshape(DH, CW)


def plain(mixer_out, out_grad, factors, weight, first_moment, second_moment):
    columns = mixer_out
    gradient = lax.psum_scatter(
        contract_rows(columns, out_grad), ("fs", "rep"), scatter_dimension=0, tiled=True
    )
    grad_low = gradient.astype(jnp.bfloat16)
    columns = factors
    projected = lax.psum_scatter(
        contract_rows(columns, grad_low), ("fs", "rep"), scatter_dimension=0, tiled=True
    )
    new_first = 0.8 * first_moment + 0.2 * projected
    new_second = 0.9 * second_moment + 0.1 * projected * projected
    direction = new_first / (jnp.sqrt(new_second) + 1e-08)
    dir_low = direction.astype(jnp.bfloat16)
    proj_low = projected.astype(jnp.bfloat16)
    dir_whole, proj_whole = (
        lax.all_gather(dir_low, ("fs", "rep"), axis=0, tiled=True),
        lax.all_gather(proj_low, ("fs", "rep"), axis=0, tiled=True),
    )
    dir_wide = dir_low.astype(jnp.float32)
    proj_wide = proj_low.astype(jnp.float32)
    dir_sum, proj_sum = lax.psum(
        (jnp.sum(dir_wide * dir_wide), jnp.sum(proj_wide * proj_wide)), ("fs", "rep", "tp")
    )
    back_dir = jnp.dot(factors, dir_whole, preferred_element_type=jnp.float32)
    back_proj = jnp.dot(factors, proj_whole, preferred_element_type=jnp.float32)
    scale_ratio = jnp.sqrt(dir_sum) / jnp.sqrt(proj_sum + 1e-06)
    update = back_dir + scale_ratio * (gradient - back_proj)
    new_weight = weight - 0.01 * update
    weight_copy = lax.all_gather(new_weight.astype(jnp.bfloat16), ("fs", "rep"), axis=0, tiled=True)
    return (new_weight, update, new_first, new_second, weight_copy)


def solution(mesh):
    Z, R, T = mesh.shape["fs"], mesh.shape["rep"], mesh.shape["tp"]

    def per_device(*args):
        mixer_out, out_grad, factors, weight, first_moment, second_moment = args
        fits = (
            out_grad.shape[1] % (PARTS * PAIR) == 0
            and mixer_out.shape[0] % PAIR == 0
            and mixer_out.shape[1] % PAIR == 0
            and weight.shape[0] % 16 == 0
            and first_moment.shape[0] % 16 == 0
            and factors.shape[1] == PAIR
            and weight.shape[0] % (16 * T) == 0
            and R == 4
            and T == 2
            and Z == R
            and Z > 1
        )
        return fused(Z, R, T, *args) if fits else plain(*args)

    in_specs = (
        P(("fs", "rep"), None),
        P(("fs", "rep"), "tp"),
        P(("fs", "rep"), None),
        P(("fs", "rep"), "tp"),
        P(("fs", "rep"), "tp"),
        P(("fs", "rep"), "tp"),
    )
    out_specs = (
        P(("fs", "rep"), "tp"),
        P(("fs", "rep"), "tp"),
        P(("fs", "rep"), "tp"),
        P(("fs", "rep"), "tp"),
        P(None, "tp"),
    )
    return jax.shard_map(
        per_device, mesh=mesh, in_specs=in_specs, out_specs=out_specs, check_vma=False
    )
```

```python
import functools

import jax
import jax.numpy as jnp
from jax import lax
from jax.experimental import pallas as pl
from jax.experimental.pallas import tpu as pltpu
from jax.sharding import PartitionSpec as P

MESH = pl.DeviceIdType.MESH
LANES = 128
PAIR = 2 * LANES
PARTS = 4
VMEM_GRANT = 52 * 1024 * 1024


ORDER = (
    "F1 f1.4 f1.1 F2",
    "f1.0 F3 f2.4.1 f1.6",
    "F4 f2.0.1 f2.0.0 f2.4.0",
    "f3.4.1 PM P1.3 P1.2",
    "P1.1 P1.0 f3.0.1 f3.0.0",
    "P2.3 P2.2 f1.2 f2.6.1",
    "P2.0 P3.2 P3.3 f2.6.0",
    "f3.4.0 f2.2.0 P2.1 f1.3",
    "f2.1.1 P3.0 P3.1 f2.1.0",
    "f3.6.1 f2.2.1 f3.2.0 f3.6.0",
    "f2.3.1 f2.3.0 P4 f1.7",
    "f3.3.0 f3.2.1 f1.5 Q1",
    "f4.3.0 f2.7.0 f3.1.1 f2.7.1",
    "f3.3.1 f4.4.1 f4.2.1 f4.6.1",
    "Q2.0 f3.1.0 f4.1.1 f4.2.0",
    "f4.4.0 Q2.1 f2.5.0 f3.7.1",
    "Q3.0 f2.5.1 f4.6.0 Q2.3",
    "f3.7.0 f4.0.1 Q3.1 f4.1.0",
    "Q4.0 g1.1 f4.7.1 f4.3.1",
    "Q2.2 f3.5.1 Q4.1 Q3.3",
    "g1.2 f4.0.0 g1.3 ga.1",
    "Q3.2 f4.7.0 Q4.3 g1.6",
    "g2.3.0 g2.1.1 f3.5.0 ga.2",
    "g1.0 g2.1.0 Q4.2 g1.4",
    "g2.3.1 ga.6 f4.5.1 g2.2.1",
    "g1.7 g2.2.0 f4.5.0 g1.5",
    "g2.0.0 g3.3.0 g2.0.1 g2.6.1",
    "ga.4 g3.2.1 g3.1.1 ga.7",
    "g3.1.0 g2.6.0 g2.4.0 g3.0.1",
    "ga.5 g3.6.1 g3.2.0 g2.7.0",
    "g3.0.0 g2.5.0 g2.5.1 g2.7.1",
    "g4.1.0 g3.3.1 g2.4.1 g3.6.0",
    "ga.3.0 ga.0.1 g4.2.1 ga.0.0",
    "g4.1.1 g4.3.0 g3.5.1 g3.4.0",
    "g3.7.1 ga.3.1 g3.4.1 g3.5.0",
    "g4.6.0 g3.7.0 g4.2.0 g4.6.1",
    "g4.5.1 g4.0.0 g4.4.0 g4.0.1",
    "g4.7.1 g4.5.0 g4.3.1 g4.7.0",
    "g4.4.1",
)
Z_SCATTER = (1,)
Z_GATHER = (0, 3)


def token(text):
    name, *index = text.split(".")
    return (name, *map(int, index))


def order_for(NP):
    if NP == 8:
        return [token(a) for line in ORDER for a in line.split()]
    events = {
        1: "F2", 2: "F3", 3: "F4 PM P1", 4: "P2", 5: "P3",
        6: "P4", 7: "Q1", 8: "Q2", 9: "Q3", 10: "Q4",
    }
    lags = {"f1": 0, "f2": 1, "f3": 2, "f4": 3, "g1": 10, "ga": 11, "g2": 11, "g3": 12, "g4": 13}
    order = [("F1",)]
    for i in range(max(NP, 1) + 14):
        for a in events.get(i, "").split():
            order.append(token(a))
        order += [(name, i - lag) for name, lag in lags.items() if 0 <= i - lag < NP]
    return order


def z_pairs(NP):
    return (Z_SCATTER, Z_GATHER) if NP == 8 else ((), ())


def live_pairs(NP):
    live, most, passed = 0, 0, {}
    z_scatter = z_pairs(NP)[0]
    for name, *index in order_for(NP):
        live += name == "f1"
        if index and name == ("f4" if index[0] in z_scatter else "f3"):
            p = index[0]
            passed[p] = passed.get(p, 0) + (1 if index[1:] else 2)
            live -= passed[p] == 2
        most = max(most, live)
    return most


def contract_rows(left, right):
    return lax.dot_general(
        left, right, (((0,), (0,)), ((), ())), preferred_element_type=jnp.float32
    )


def drain_kernel(*refs):
    n = len(refs) // 2
    ins, outs, sem = refs[:n], refs[n:-1], refs[-1]
    copies = [pltpu.make_async_copy(a, b, sem.at[i]) for i, (a, b) in enumerate(zip(ins, outs))]
    for c in copies:
        c.start()
    for c in copies:
        c.wait()


def drain_out(*arrays):
    return pl.pallas_call(
        drain_kernel,
        out_shape=tuple(jax.ShapeDtypeStruct(a.shape, a.dtype) for a in arrays),
        in_specs=[pl.BlockSpec(memory_space=pltpu.VMEM)] * len(arrays),
        out_specs=(pl.BlockSpec(memory_space=pl.ANY),) * len(arrays),
        scratch_shapes=[pltpu.SemaphoreType.DMA((len(arrays),))],
        compiler_params=pltpu.CompilerParams(vmem_limit_bytes=4 * 1024 * 1024),
    )(*[pltpu.with_memory_space_constraint(a, pltpu.VMEM) for a in arrays])


def fused_kernel(
    Z, R, T,
    m_hbm, o_hbm, f_hbm, w_hbm, m1_hbm, m2_hbm,
    nw_ref, upd_ref, nf_ref, ns_ref, wc_ref,
    m_ref, o_ref, f_ref, w_ref, m1_ref, m2_ref, load,
    mt, own, s1, r1, s2, r2, s3, r3, rz,
    f_all, ft, yt, own_p, s1_p, r1_p, s2_p, r2_p, s3_p, r3_p, proj, q_all, q_own,
    stat, stat_all, ratio,
    t_send, t_recv, u_send, u_recv, v_send, v_recv,
    tp_send, tp_recv, up_send, up_recv, vp_send, vp_recv,
    gz_send, gz_recv, gx_send, gx_recv, gf_send,
    st_send, st_recv, cross_send, cross_recv,
):
    N = Z * R
    z, r, t = lax.axis_index("fs"), lax.axis_index("rep"), lax.axis_index("tp")
    every = (z * R + r) * T + t
    TOK, DH = m_ref.shape
    CW = o_ref.shape[1]
    FR, RK = f_ref.shape
    MR = m1_ref.shape[0]
    NP = CW // PAIR
    PART = CW // PARTS
    xn, yn, dn = r + 1 - 2 * lax.rem(r, 2), lax.rem(r + 2, R), R - 1 - r
    near = ((xn, yn), (yn, xn))
    low_half = z < 2
    twin = z + 1 - 2 * lax.rem(z, 2)
    cross = jnp.where(low_half, 2, 1)
    away = jnp.where(low_half, 2, 0)
    middle = (z == 1) | (z == 2)
    f32, bf16 = jnp.float32, jnp.bfloat16

    def device(zz, rr, tt):
        return {"fs": zz, "rep": rr, "tp": tt}

    def lanes(index, size):
        return pl.ds(pl.multiple_of(index * size, size), size)

    def other(e):
        return lax.rem(z + e, Z)

    def each_z(body):
        def step(e, carry):
            body(other(e))
            return carry

        lax.fori_loop(1, Z, step, 0)

    def fetch(src, dst, index):
        return pltpu.make_async_copy(src, dst, load.at[index])

    loads = {"f": fetch(f_hbm, f_ref, 0)}
    for i in range(DH // PAIR):
        part = pl.ds(i * PAIR, PAIR)
        loads["m", i] = fetch(m_hbm.at[:, part], m_ref.at[:, part], len(loads))
    for i in range(NP):
        part = pl.ds(i * PAIR, PAIR)
        loads["o", i] = fetch(o_hbm.at[:, part], o_ref.at[:, part], len(loads))
    for name, src, dst in (("m1", m1_hbm, m1_ref), ("m2", m2_hbm, m2_ref), ("w", w_hbm, w_ref)):
        loads[name] = fetch(src, dst, len(loads))
    for copy in loads.values():
        copy.start()

    def need(*names):
        for name in names:
            if name in loads:
                loads.pop(name).wait()

    barrier = pltpu.get_barrier_semaphore()

    def greet(zz, rr, tt):
        pl.semaphore_signal(barrier, inc=1, device_id=device(zz, rr, tt), device_id_type=MESH)

    each_z(lambda zz: greet(zz, r, t))
    greet(z, xn, t)
    greet(z, yn, t)
    greet(z, r, 1 - t)

    for i in range(DH // PAIR):
        need(("m", i))
        mt[i * PAIR : (i + 1) * PAIR, :] = m_ref[:, i * PAIR : (i + 1) * PAIR].T
    need("f")

    def move(src, dst, ss, rs, where):
        return pltpu.make_async_remote_copy(
            src_ref=src, dst_ref=dst, send_sem=ss, recv_sem=rs, device_id=where, device_id_type=MESH
        )

    class Scatter:
        def __init__(self, c, h, slot, refs, sems):
            self.c, self.h, self.slot = c, h, slot
            self.own, self.s1, self.r1, self.s2, self.r2, self.s3, self.r3 = refs
            self.ts, self.tr, self.us, self.ur, self.vs, self.vr = sems
            self.n1, self.n2 = near[h]

        def first(self, k):
            rr = self.n1 if k else dn
            c = self.c
            return move(self.s1.at[c, rr], self.r1.at[c, k], self.ts.at[c], self.tr.at[c, k], device(z, self.n1, t))

        def second(self):
            c = self.c
            return move(self.s2.at[c], self.r2.at[c], self.us.at[c], self.ur.at[c], device(z, self.n2, t))

        def third(self, zz, src):
            c = self.c
            return move(
                self.s3.at[c, zz], self.r3.at[c, src], self.vs.at[c], self.vr.at[c], device(zz, r, t)
            )

        def thirds(self):
            every_block = self.r3.at[self.c, pl.ds(0, Z - 1)]
            return move(every_block, every_block, self.vs.at[self.c], self.vr.at[self.c], device(other(1), r, t))

        def firsts(self):
            return move(
                self.r1.at[self.c], self.r1.at[self.c], self.ts.at[self.c], self.tr.at[self.c, 0],
                device(z, self.n1, t),
            )

        def mine(self, rr, zz):
            return self.own[self.slot, self.h, rr, zz]

        def stage2(self):
            c = self.c
            self.first(0).wait_recv()

            def add(zz, carry):
                total = self.mine(self.n2, zz) + self.r1[c, 0, zz].astype(f32)
                self.s2[c, zz] = total.astype(bf16)
                return carry

            lax.fori_loop(0, Z, add, 0)
            self.second().start()

        def stage3(self, put):
            c = self.c
            self.first(1).wait_recv()
            self.second().wait_recv()

            def total(zz):
                return self.mine(r, zz) + self.r1[c, 1, zz].astype(f32) + self.r2[c, zz].astype(f32)

            def send(zz):
                self.s3[c, zz] = total(zz).astype(bf16)
                self.third(zz, z).start()

            each_z(send)
            put(total(z))

        def last(self, get, put):
            self.thirds().wait_recv()
            value = get()
            for e in range(1, Z):
                value = value + self.r3[self.c, other(e)].astype(f32)
            put(value)

        def sent(self):
            self.firsts().wait_send()
            self.second().wait_send()
            self.thirds().wait_send()

    class Gather:
        def __init__(self, g, h, ref, cols, rows=slice(None)):
            self.g, self.ref, self.cols, self.rows = g, ref, cols, rows
            self.n1, self.n2 = near[h]

        def along(self, zz, src_z, block=None, sent=None, got=None):
            place = self.ref.at[src_z, r, self.rows, self.cols]
            return move(
                place if block is None else block, place,
                gz_send.at[self.g] if sent is None else sent, gz_recv.at[self.g, src_z if got is None else got], device(zz, r, t),
            )

        def beside(self, k, rr):
            place = self.ref.at[:, rr, self.rows, self.cols]
            to = self.n2 if k == 0 else self.n1
            return move(place, place, gx_send.at[self.g], gx_recv.at[self.g, k], device(z, to, t))

        def stage1(self, block=None):
            each_z(lambda zz: self.along(zz, z, block, None, 0).start())

        def spread(self):
            self.along(cross, z).start()
            self.along(twin, z).start()

        def onward(self, k):
            return self.along(twin, away + k, None, gf_send.at[self.g])

        def forward(self):
            @pl.when(middle)
            def _():
                for k in (0, 1):
                    self.along(twin, away + k).wait_recv()
                    self.onward(k).start()

        def gathered(self):
            self.along(twin, twin).wait_recv()

            @pl.when(jnp.logical_not(middle))
            def _():
                for k in (0, 1):
                    self.along(twin, away + k).wait_recv()

        def along_sent(self, blocks, sem):
            place = self.ref.at[pl.ds(0, blocks), r, self.rows, self.cols]
            move(place, place, sem, gz_recv.at[self.g, twin], device(twin, r, t)).wait_send()

        def beside_sent(self):
            place = self.ref.at[:, pl.ds(0, 3), self.rows, self.cols]
            move(place, place, gx_send.at[self.g], gx_recv.at[self.g, 0], device(z, self.n1, t)).wait_send()

        def spread_sent(self):
            self.along_sent(2, gz_send.at[self.g])

            @pl.when(middle)
            def _():
                self.along_sent(2, gf_send.at[self.g])

        def stage2(self, spread=False):
            if spread:
                self.gathered()
            else:
                place = self.ref.at[pl.ds(0, Z - 1), r, self.rows, self.cols]
                move(place, place, gz_send.at[self.g], gz_recv.at[self.g, 0], device(twin, r, t)).wait_recv()
            self.beside(0, r).start()
            self.beside(1, r).start()

        def stage3(self):
            self.beside(0, self.n2).wait_recv()
            self.beside(2, self.n2).start()

        def done(self, spread=False):
            self.beside(1, self.n1).wait_recv()
            self.beside(2, dn).wait_recv()
            if spread:
                self.spread_sent()
            else:
                self.along_sent(Z - 1, gz_send.at[self.g])
            self.beside_sent()

    class ScatterZ(Scatter):
        def far(self, zz, src):
            c = self.c
            return move(
                self.s1.at[c, :, zz], rz.at[along_z[c], src], self.vs.at[c], self.vr.at[c], device(zz, r, t)
            )

        def thirds(self):
            every_block = rz.at[along_z[self.c], pl.ds(0, Z - 1)]
            return move(every_block, every_block, self.vs.at[self.c], self.vr.at[self.c], device(other(1), r, t))

        def firsts(self):
            both_blocks = self.r2.at[self.c, pl.ds(0, 2)]
            return move(both_blocks, both_blocks, self.ts.at[self.c], self.tr.at[self.c, 0], device(z, self.n1, t))

        def first(self, k):
            rr = self.n1 if k else dn
            c = self.c
            return move(self.s2.at[c, rr], self.r2.at[c, k], self.ts.at[c], self.tr.at[c, k], device(z, self.n1, t))

        def second(self):
            c = self.c
            return move(self.s3.at[c, 0], self.r3.at[c, 0], self.us.at[c], self.ur.at[c], device(z, self.n2, t))

        def stage1(self):
            each_z(lambda zz: self.far(zz, z).start())

        def stage2(self):
            self.thirds().wait_recv()

            def add(rr, carry):
                total = self.mine(rr, z)
                for e in range(1, Z):
                    total = total + rz[along_z[self.c], other(e), rr].astype(f32)
                self.own[self.slot, self.h, rr, z] = total
                self.s2[self.c, rr] = total.astype(bf16)
                return carry

            lax.fori_loop(0, R, add, 0)
            self.first(0).start()
            self.first(1).start()

        def stage3(self, put):
            c = self.c
            self.first(0).wait_recv()
            self.s3[c, 0] = (self.mine(self.n2, z) + self.r2[c, 0].astype(f32)).astype(bf16)
            self.second().start()

        def last(self, get, put):
            c = self.c
            self.first(1).wait_recv()
            self.second().wait_recv()
            put(self.mine(r, z) + self.r2[c, 1].astype(f32) + self.r3[c, 0].astype(f32))

        def sent(self):
            self.firsts().wait_send()
            self.second().wait_send()
            self.thirds().wait_send()

    class GatherZ(Gather):
        def along(self, zz, src_z, block=None, sent=None):
            place = self.ref.at[src_z, :, :, self.cols]
            return move(
                place, place, gz_send.at[self.g] if sent is None else sent, gz_recv.at[self.g, src_z],
                device(zz, r, t),
            )

        def along_sent(self, blocks, sem):
            place = self.ref.at[pl.ds(0, blocks), :, :, self.cols]
            move(place, place, sem, gz_recv.at[self.g, twin], device(twin, r, t)).wait_send()

        def beside_sent(self):
            place = self.ref.at[z, pl.ds(0, 3), :, self.cols]
            move(place, place, gx_send.at[self.g], gx_recv.at[self.g, 0], device(z, self.n1, t)).wait_send()

        def beside(self, k, rr):
            place = self.ref.at[z, rr, :, self.cols]
            to = self.n2 if k == 0 else self.n1
            return move(place, place, gx_send.at[self.g], gx_recv.at[self.g, k], device(z, to, t))

        def begin(self):
            self.beside(0, r).start()
            self.beside(1, r).start()

        def stage2(self, spread=True):
            self.beside(0, self.n2).wait_recv()
            self.beside(2, self.n2).start()

        def stage3(self):
            self.beside(1, self.n1).wait_recv()
            self.beside(2, dn).wait_recv()
            self.spread()

        def done(self, spread=True):
            self.gathered()
            self.spread_sent()
            self.beside_sent()

    main_refs = (own, s1, r1, s2, r2, s3, r3)
    main_sems = (t_send, t_recv, u_send, u_recv, v_send, v_recv)
    proj_refs = (own_p, s1_p, r1_p, s2_p, r2_p, s3_p, r3_p)
    proj_sems = (tp_send, tp_recv, up_send, up_recv, vp_send, vp_recv)

    slots = {}
    z_scatter, z_gather = z_pairs(NP)
    along_z = {2 * p + h: 2 * i + h for i, p in enumerate(z_scatter) for h in (0, 1)}

    def scatter(p, h):
        kind = ScatterZ if p in z_scatter else Scatter
        return kind(2 * p + h, h, slots[p], main_refs, main_sems)

    def scatter_p(c):
        return Scatter(c, c % 2, c, proj_refs, proj_sems)

    def gather_w(p, h):
        kind = GatherZ if p in z_gather else Gather
        return kind(2 * p + h, h, wc_ref, lanes(2 * p + h, LANES))

    def gather_f(h):
        return Gather(2 * NP + h, h, f_all, pl.ds(h * (RK // 2), RK // 2), share)

    def gather_q(c):
        return Gather(2 * NP + 2 + c, c % 2, q_all, pl.ds(c * PART, PART))

    share = pl.ds(pl.multiple_of(t * (FR // T), FR // T), FR // T)
    f_all[z, r, share] = f_ref[share, :]
    pl.semaphore_wait(barrier, Z + 2)

    def product(p):
        need(("o", p))
        cols = lanes(p, PAIR)
        slot = slots[p]
        G = R * FR

        def tile(zz, carry):
            part = pl.ds(pl.multiple_of(zz * G, G), G)
            value = jnp.dot(mt[part, :], o_ref[:, cols], preferred_element_type=f32)
            for h in (0, 1):
                for rr in range(R):
                    block = value[rr * FR : (rr + 1) * FR, h * LANES : (h + 1) * LANES]
                    own[slot, h, rr, zz] = block
                    s1[2 * p + h, rr, zz] = block.astype(bf16)
            return carry

        lax.fori_loop(0, Z, tile, 0)
        if p in z_scatter:
            both(lambda h: scatter(p, h).stage1())
            return
        for k in (0, 1):
            for h in (0, 1):
                scatter(p, h).first(k).start()

    def start_factors():
        for h in (0, 1):
            gather_f(h).stage1(f_ref.at[share, pl.ds(h * (RK // 2), RK // 2)])

    def swap_factors():
        place = f_all.at[:, :, share, :]
        return move(place, place, cross_send, cross_recv, device(z, r, 1 - t))

    def finish_factors():
        both(lambda h: gather_f(h).done())
        swap_factors().start()

    def low_rank():
        swap_factors().wait()
        ft[...] = f_all[...].reshape(DH, RK).T

        def low(i, carry):
            yt[:, lanes(i, PAIR)] = jnp.dot(
                ft[...], mt[:, lanes(i, PAIR)], preferred_element_type=f32
            ).astype(bf16)
            return carry

        lax.fori_loop(0, TOK // PAIR, low, 0)

    def project(c):
        tiles = PART // PAIR
        need(*[("o", c * tiles + n) for n in range(tiles)])

        def tile(n, carry):
            value = jnp.dot(yt[...], o_ref[:, lanes(c * tiles + n, PAIR)], preferred_element_type=f32)
            cols = lanes(n, PAIR)
            for zz in range(Z):
                for rr in range(R):
                    low_row = (zz * R + rr) * MR
                    block = value[low_row : low_row + MR, :]
                    own_p[c, c % 2, rr, zz, :, cols] = block
                    s1_p[c, rr, zz, :, cols] = block.astype(bf16)
            return carry

        lax.fori_loop(0, tiles, tile, 0)
        for k in (0, 1):
            scatter_p(c).first(k).start()

    def s_copy(p):
        q = lax.rem(every + p, N * T)
        d = q // T
        return move(
            stat, stat_all.at[every], st_send, st_recv, device(d // R, lax.rem(d, R), lax.rem(q, T))
        )

    def fold(value):
        row = jnp.sum(value, axis=0, keepdims=True)
        total = row[:, :LANES]
        for j in range(1, CW // LANES):
            total = total + row[:, j * LANES : (j + 1) * LANES]
        return total

    def moments():
        need("m1", "m2")
        projected = proj[...]
        new_first = 0.8 * m1_ref[...] + 0.2 * projected
        new_second = 0.9 * m2_ref[...] + 0.1 * projected * projected
        nf_ref[...] = new_first
        ns_ref[...] = new_second
        dir_wide = (new_first / (jnp.sqrt(new_second) + 1e-08)).astype(bf16).astype(f32)
        proj_wide = projected.astype(bf16).astype(f32)
        stat[0:1, :] = fold(dir_wide * dir_wide)
        stat[1:2, :] = fold(proj_wide * proj_wide)
        stat_all[every] = stat[...]

        def send(p, carry):
            s_copy(p).start()
            return carry

        lax.fori_loop(1, N * T, send, 0)

    def combine():
        arrivals = stat_all.at[pl.ds(0, N * T - 1)]
        move(arrivals, arrivals, st_send, st_recv, device(z, r, 1 - t)).wait()
        totals = jnp.sum(stat_all[...], axis=0)
        dir_sum = jnp.sum(totals[0:1, :], axis=1, keepdims=True)
        proj_sum = jnp.sum(totals[1:2, :], axis=1, keepdims=True)
        scale_ratio = jnp.sqrt(dir_sum) / jnp.sqrt(proj_sum + 1e-06)
        ratio[...] = jnp.broadcast_to(scale_ratio, (8, PAIR))
        projected = proj[...]
        dir_wide = (nf_ref[...] / (jnp.sqrt(ns_ref[...]) + 1e-08)).astype(bf16).astype(f32)
        mixed = (dir_wide - scale_ratio * projected.astype(bf16).astype(f32)).astype(bf16)
        q_own[...] = mixed
        q_all[z, r] = mixed
        for c in range(PARTS):
            gather_q(c).stage1(q_own.at[:, pl.ds(c * PART, PART)])

    def put_proj(c):
        def put(value):
            proj[:, c * PART : (c + 1) * PART] = value

        return put

    def get_proj(c):
        return lambda: proj[:, c * PART : (c + 1) * PART]

    def both(action):
        for h in (0, 1):
            action(h)

    def finish_moments():
        for c in range(PARTS):
            scatter_p(c).last(get_proj(c), put_proj(c))
        moments()

    def put_grad(p, h):
        def put(value):
            upd_ref[:, lanes(2 * p + h, LANES)] = value

        return put

    def get_grad(p, h):
        return lambda: upd_ref[:, lanes(2 * p + h, LANES)]

    def update(p):
        need("w")
        cols = lanes(p, PAIR)
        mixed = q_all[:, :, :, cols].reshape(RK, PAIR)
        value = jnp.dot(f_ref[...], mixed, preferred_element_type=f32) + ratio[0:1, :] * upd_ref[:, cols]
        upd_ref[:, cols] = value
        new_weight = w_ref[:, cols] - 0.01 * value
        nw_ref[:, cols] = new_weight
        wc_ref[z, r, :, cols] = new_weight.astype(bf16)
        if p in z_gather:
            both(lambda h: gather_w(p, h).begin())
        else:
            both(lambda h: gather_w(p, h).spread())

    single = {
        "F1": start_factors,
        "F2": lambda: both(lambda h: gather_f(h).stage2()),
        "F3": lambda: both(lambda h: gather_f(h).stage3()),
        "F4": finish_factors,
        "PM": low_rank,
        "P4": finish_moments,
        "Q1": combine,
    }
    parts = {
        "P1": project,
        "P2": lambda c: scatter_p(c).stage2(),
        "P3": lambda c: scatter_p(c).stage3(put_proj(c)),
        "Q2": lambda c: gather_q(c).stage2(),
        "Q3": lambda c: gather_q(c).stage3(),
        "Q4": lambda c: gather_q(c).done(),
    }
    pairs = {"f1": product, "g1": update}
    chunks = {
        "f2": lambda p, h: scatter(p, h).stage2(),
        "f3": lambda p, h: scatter(p, h).stage3(put_grad(p, h)),
        "f4": lambda p, h: scatter(p, h).last(get_grad(p, h), put_grad(p, h)),
        "ga": lambda p, h: gather_w(p, h).forward(),
        "g2": lambda p, h: gather_w(p, h).stage2(True),
        "g3": lambda p, h: gather_w(p, h).stage3(),
        "g4": lambda p, h: gather_w(p, h).done(True),
    }
    free, issued, passed = list(range(own.shape[0])), [], {}
    for name, *index in order_for(NP):
        if name in single:
            single[name]()
        elif name in parts:
            for c in index or range(PARTS):
                parts[name](c)
        elif name in pairs:
            p = index[0]
            if name == "f1":
                slots[p] = free.pop(0)
            pairs[name](p)
        else:
            p = index[0]
            for h in index[1:] or (0, 1):
                chunks[name](p, h)
                if name == ("f4" if p in z_scatter else "f3"):
                    passed[p] = passed.get(p, 0) + 1
                    if passed[p] == 2:
                        free.append(slots[p])
                        issued.append(p)
            if name == "g3" and issued:
                p = issued.pop(0)
                both(lambda h: scatter(p, h).sent())
    for p in issued:
        both(lambda h: scatter(p, h).sent())
    for c in range(PARTS):
        scatter_p(c).sent()


def fused(Z, R, T, *args):
    mixer_out, out_grad, factors, weight, first_moment, second_moment = args
    N = Z * R
    TOK, DH = mixer_out.shape
    FR, RK = factors.shape
    MR, CW = first_moment.shape
    NC, PART = CW // LANES, CW // PARTS
    GC = NC + 2 + PARTS
    f32, bf16 = jnp.float32, jnp.bfloat16
    vmem = pl.BlockSpec(memory_space=pltpu.VMEM)
    dma = pltpu.SemaphoreType.DMA
    pair = lambda *shape: [dma(shape), dma(shape)]
    outs = pl.pallas_call(
        functools.partial(fused_kernel, Z, R, T),
        out_shape=(
            pltpu.VMEM(weight.shape, f32),
            pltpu.VMEM(weight.shape, f32),
            pltpu.VMEM(first_moment.shape, f32),
            pltpu.VMEM(first_moment.shape, f32),
            pltpu.VMEM((Z, R, FR, CW), bf16),
        ),
        in_specs=[pl.BlockSpec(memory_space=pltpu.HBM)] * 6,
        out_specs=(vmem,) * 5,
        scratch_shapes=[
            *[pltpu.VMEM(a.shape, a.dtype) for a in args],
            dma((DH // PAIR + CW // PAIR + 4,)),
            pltpu.VMEM((DH, TOK), bf16),
            pltpu.VMEM((live_pairs(CW // PAIR), 2, R, Z, FR, LANES), f32),
            pltpu.VMEM((NC, R, Z, FR, LANES), bf16),
            pltpu.VMEM((NC, 2, Z, FR, LANES), bf16),
            pltpu.VMEM((NC, max(Z, R), FR, LANES), bf16),
            pltpu.VMEM((NC, max(Z, R), FR, LANES), bf16),
            pltpu.VMEM((NC, Z, FR, LANES), bf16),
            pltpu.VMEM((NC, Z, FR, LANES), bf16),
            pltpu.VMEM((max(1, 2 * len(z_pairs(CW // PAIR)[0])), Z, R, FR, LANES), bf16),
            pltpu.VMEM((Z, R, FR, RK), bf16),
            pltpu.VMEM((RK, DH), bf16),
            pltpu.VMEM((RK, TOK), bf16),
            pltpu.VMEM((PARTS, 2, R, Z, MR, PART), f32),
            pltpu.VMEM((PARTS, R, Z, MR, PART), bf16),
            pltpu.VMEM((PARTS, 2, Z, MR, PART), bf16),
            pltpu.VMEM((PARTS, Z, MR, PART), bf16),
            pltpu.VMEM((PARTS, Z, MR, PART), bf16),
            pltpu.VMEM((PARTS, Z, MR, PART), bf16),
            pltpu.VMEM((PARTS, Z, MR, PART), bf16),
            pltpu.VMEM((MR, CW), f32),
            pltpu.VMEM((Z, R, MR, CW), bf16),
            pltpu.VMEM((MR, CW), bf16),
            pltpu.VMEM((2, LANES), f32),
            pltpu.VMEM((N * T, 2, LANES), f32),
            pltpu.VMEM((8, PAIR), f32),
            dma((NC,)), dma((NC, 2)), *pair(NC), *pair(NC),
            dma((PARTS,)), dma((PARTS, 2)), *pair(PARTS), *pair(PARTS),
            dma((GC,)), dma((GC, Z)), dma((GC,)), dma((GC, 3)), dma((GC,)),
            dma, dma, dma, dma,
        ],
        compiler_params=pltpu.CompilerParams(
            collective_id=0, has_side_effects=True, vmem_limit_bytes=VMEM_GRANT
        ),
    )(*args)
    new_weight, update, new_first, new_second, copy = drain_out(*outs)
    return new_weight, update, new_first, new_second, copy.reshape(DH, CW)


def plain(mixer_out, out_grad, factors, weight, first_moment, second_moment):
    columns = mixer_out
    gradient = lax.psum_scatter(
        contract_rows(columns, out_grad), ("fs", "rep"), scatter_dimension=0, tiled=True
    )
    grad_low = gradient.astype(jnp.bfloat16)
    columns = factors
    projected = lax.psum_scatter(
        contract_rows(columns, grad_low), ("fs", "rep"), scatter_dimension=0, tiled=True
    )
    new_first = 0.8 * first_moment + 0.2 * projected
    new_second = 0.9 * second_moment + 0.1 * projected * projected
    direction = new_first / (jnp.sqrt(new_second) + 1e-08)
    dir_low = direction.astype(jnp.bfloat16)
    proj_low = projected.astype(jnp.bfloat16)
    dir_whole, proj_whole = (
        lax.all_gather(dir_low, ("fs", "rep"), axis=0, tiled=True),
        lax.all_gather(proj_low, ("fs", "rep"), axis=0, tiled=True),
    )
    dir_wide = dir_low.astype(jnp.float32)
    proj_wide = proj_low.astype(jnp.float32)
    dir_sum, proj_sum = lax.psum(
        (jnp.sum(dir_wide * dir_wide), jnp.sum(proj_wide * proj_wide)), ("fs", "rep", "tp")
    )
    back_dir = jnp.dot(factors, dir_whole, preferred_element_type=jnp.float32)
    back_proj = jnp.dot(factors, proj_whole, preferred_element_type=jnp.float32)
    scale_ratio = jnp.sqrt(dir_sum) / jnp.sqrt(proj_sum + 1e-06)
    update = back_dir + scale_ratio * (gradient - back_proj)
    new_weight = weight - 0.01 * update
    weight_copy = lax.all_gather(new_weight.astype(jnp.bfloat16), ("fs", "rep"), axis=0, tiled=True)
    return (new_weight, update, new_first, new_second, weight_copy)


def solution(mesh):
    Z, R, T = mesh.shape["fs"], mesh.shape["rep"], mesh.shape["tp"]

    def per_device(*args):
        mixer_out, out_grad, factors, weight, first_moment, second_moment = args
        fits = (
            out_grad.shape[1] % (PARTS * PAIR) == 0
            and mixer_out.shape[0] % PAIR == 0
            and mixer_out.shape[1] % PAIR == 0
            and weight.shape[0] % 16 == 0
            and first_moment.shape[0] % 16 == 0
            and factors.shape[1] == PAIR
            and weight.shape[0] % (16 * T) == 0
            and R == 4
            and T == 2
            and Z == R
            and Z > 1
        )
        return fused(Z, R, T, *args) if fits else plain(*args)

    in_specs = (
        P(("fs", "rep"), None),
        P(("fs", "rep"), "tp"),
        P(("fs", "rep"), None),
        P(("fs", "rep"), "tp"),
        P(("fs", "rep"), "tp"),
        P(("fs", "rep"), "tp"),
    )
    out_specs = (
        P(("fs", "rep"), "tp"),
        P(("fs", "rep"), "tp"),
        P(("fs", "rep"), "tp"),
        P(("fs", "rep"), "tp"),
        P(None, "tp"),
    )
    return jax.shard_map(
        per_device, mesh=mesh, in_specs=in_specs, out_specs=out_specs, check_vma=False
    )
```
